128 devices in a mesh: rep: 2 (over z_hi), fs: 32 (over z_lo, y, x), tp: 2 (over core).
Axes of the slice: x: 4, y: 4, z: 4 (z_hi: 2, z_lo: 2; z = z_hi * 2 + z_lo), core: 2. Of those that a mesh axis runs over, the one named last changes fastest.
Arguments:
- tokens: bfloat16 [64, 256, 1024], P(('rep', 'fs'), None, 'tp'), may hold values from -6 to 6
- pre_gain: float32 [1024], replicated, may hold values from 0.1 to 1.9
- first_gate: bfloat16 [1024, 2560], P('fs', 'tp'), may hold values from -0.1875 to 0.1875
- first_up: bfloat16 [1024, 2560], P('fs', 'tp'), may hold values from -0.1875 to 0.1875
- first_down: bfloat16 [2560, 1024], P('tp', 'fs'), may hold values from -0.125 to 0.125
- mix_gain: float32 [1024], P('tp'), may hold values from 0.1 to 1.9
- pool_weight: bfloat16 [4, 256, 256], P('tp', None, 'fs'), may hold values from -0.375 to 0.375
- pool_scale: float32 [1024], P('tp'), may hold values from 0.1 to 1.9
- post_gain: float32 [1024], replicated, may hold values from 0.1 to 1.9
- second_gate: bfloat16 [1024, 2560], P('fs', 'tp'), may hold values from -0.1875 to 0.1875
- second_up: bfloat16 [1024, 2560], P('fs', 'tp'), may hold values from -0.1875 to 0.1875
- second_down: bfloat16 [2560, 1024], P('tp', 'fs'), may hold values from -0.125 to 0.125
Outputs:
- layer_out: bfloat16 [64, 256, 1024], P(('rep', 'fs'), None, 'tp')
The draws below stay inside these ranges and needn't reach their ends.
All inputs are finite; a program needn't handle non-finite values.
Results may differ from the reference program's by a relative error of at most 0.015.
Values may be sent and summed in bfloat16 or wider, within the bound.
A program may use at most 64 MiB of HBM per device.

```python
import jax
import jax.numpy as jnp
from jax import lax

D = 1024
FF = 2560
GROUPS = 4
GROUP = 256
SEQ = 256
BATCH = 64


def levels(stream_key, extent, cuts, least, high):
    loudness = 1.0
    for axis_at, shards_of in cuts:
        steps = jax.random.uniform(jax.random.fold_in(jax.random.fold_in(stream_key, 6), axis_at), (shards_of,), jnp.float32, least / len(cuts), high / len(cuts))
        loudness = loudness * jnp.repeat(jnp.exp(steps), extent[axis_at] // shards_of).reshape((-1,) + (1,) * (len(extent) - 1 - axis_at))
    return loudness


def scatter_about(own_key, shape, deviation, reach, shards=(), held_as=jnp.bfloat16):
    values = deviation * jax.random.normal(own_key, shape, jnp.float32)
    if shards:
        values = values * levels(own_key, shape, shards, -0.22, 0.18)
    return jnp.clip(values, -reach, reach).astype(held_as)


def setup_inputs(seed: int = 0) -> dict:
    key_of = jax.random.split(jax.random.key(seed), 13)
    tokens = scatter_about(key_of[0], (BATCH, SEQ, D), 1.0, 6.0, ((0, 64), (2, 2)))
    pre_gain = jnp.clip(1.0 + 0.18 * jax.random.normal(key_of[1], (D,), jnp.float32), 0.1, 1.9)
    first_gate = scatter_about(key_of[2], (D, FF), D ** -0.5, 0.1875, ((0, 32), (1, 2)))
    first_up = scatter_about(key_of[3], (D, FF), D ** -0.5, 0.1875, ((0, 32), (1, 2)))
    first_down = scatter_about(key_of[4], (FF, D), FF ** -0.5, 0.125, ((0, 2), (1, 32)))
    mix_gain = jnp.clip(1.0 + 0.18 * jax.random.normal(key_of[5], (D,), jnp.float32), 0.1, 1.9)
    pool_weight = scatter_about(key_of[6], (GROUPS, GROUP, GROUP), GROUP ** -0.5, 0.375, ((0, 2), (2, 32)))
    pool_scale = jnp.clip(1.0 + 0.18 * jax.random.normal(key_of[7], (D,), jnp.float32), 0.1, 1.9)
    post_gain = jnp.clip(1.0 + 0.18 * jax.random.normal(key_of[8], (D,), jnp.float32), 0.1, 1.9)
    second_gate = scatter_about(key_of[9], (D, FF), D ** -0.5, 0.1875, ((0, 32), (1, 2)))
    second_up = scatter_about(key_of[10], (D, FF), D ** -0.5, 0.1875, ((0, 32), (1, 2)))
    second_down = scatter_about(key_of[11], (FF, D), FF ** -0.5, 0.125, ((0, 2), (1, 32)))
    return dict(tokens=tokens, pre_gain=pre_gain, first_gate=first_gate, first_up=first_up, first_down=first_down, mix_gain=mix_gain, pool_weight=pool_weight, pool_scale=pool_scale, post_gain=post_gain, second_gate=second_gate, second_up=second_up, second_down=second_down)


epsilon = 1e-06

def normalize(values, gain_vec):
    floats = values.astype(jnp.float32)
    scaled = floats * lax.rsqrt(lax.optimization_barrier(jnp.mean(floats * floats, axis=-1, keepdims=True)) + epsilon)
    return (scaled * gain_vec.astype(jnp.float32)).astype(jnp.bfloat16)

def half_block(flat_rows, gain_vec, gate_w, up_w, down_w):
    normed = normalize(flat_rows, gain_vec)
    gate_sum = jnp.dot(normed, gate_w, preferred_element_type=jnp.float32)
    up_sum = jnp.dot(normed, up_w, preferred_element_type=jnp.float32)
    hidden = (jax.nn.silu(gate_sum) * up_sum).astype(jnp.bfloat16)
    return jnp.dot(hidden, down_w, preferred_element_type=jnp.float32)

def trailing(grouped, windows, widest):
    seq_length = grouped.shape[1]
    running = jnp.zeros_like(grouped)
    for back_step in range(widest):
        moved = jnp.pad(grouped, ((0, 0), (back_step, 0), (0, 0), (0, 0)))[:, :seq_length]
        running = running + jnp.where(back_step < windows[None, None, :, None], moved, 0.0)
    positions = jnp.arange(seq_length, dtype=jnp.int32)
    counts = jnp.minimum(positions[:, None] + 1, windows[None, :]).astype(jnp.float32)
    return running / counts[None, :, :, None]

def reference(tokens, pre_gain, first_gate, first_up, first_down, mix_gain, pool_weight, pool_scale, post_gain, second_gate, second_up, second_down):
    flat_rows = tokens.reshape(BATCH * SEQ, D)
    first_out = half_block(flat_rows, pre_gain, first_gate, first_up, first_down)
    after_first = (flat_rows.astype(jnp.float32) + 0.5 * first_out).astype(jnp.bfloat16)
    normed = normalize(after_first, mix_gain)
    grouped = normed.astype(jnp.float32).reshape(BATCH, SEQ, GROUPS, GROUP)
    windows = 2 ** (jnp.arange(GROUPS, dtype=jnp.int32) + 1)
    pooled = trailing(grouped, windows, 2 ** GROUPS)
    diff = (pooled - grouped).astype(jnp.bfloat16)
    mixed = jnp.einsum('bsgc,gcd->bsgd', diff.astype(jnp.float32), pool_weight.astype(jnp.float32))
    mixed = mixed.reshape(BATCH * SEQ, D)
    after_mix = (after_first.astype(jnp.float32) + mixed * pool_scale.astype(jnp.float32)).astype(jnp.bfloat16)
    second_out = half_block(after_mix, post_gain, second_gate, second_up, second_down)
    layer_out = (after_mix.astype(jnp.float32) + 0.5 * second_out).astype(jnp.bfloat16)
    return layer_out.reshape(BATCH, SEQ, D)
```

```python
import jax
import jax.numpy as jnp
from jax import lax
from jax.experimental import pallas as pl
from jax.experimental.pallas import tpu as pltpu
from jax.sharding import PartitionSpec as P

MESH = pl.DeviceIdType.MESH
BF16 = jnp.bfloat16
F32 = jnp.float32
EPS = 1e-06
D = 1024
HALF = 512
ROWS = 128
UNIT = 640
N_SEND = 224
N_RECV = 224
N_LOCAL = 16


class Net:
    def __init__(self, ss, rs, ls, here):
        self.ss, self.rs, self.ls, self.here = ss, rs, ls, here
        self.names = {}
        self.sends = 0
        self.locals = 0
        self.pending = []

    def name(self, key, width=1):
        if key not in self.names:
            self.names[key] = sum(w for _, w in self.names.values()), width
        return self.names[key][0]

    def send(self, key, make, cond=None, width=1, shift=None):
        base = self.name(key, width)
        slot = self.sends
        self.sends += 1

        def copy():
            src, dst, device = make()
            where = base if shift is None else base + shift
            return pltpu.make_async_remote_copy(
                src, dst, self.ss.at[slot], self.rs.at[where], device_id=device, device_id_type=MESH
            )

        def end():
            copy().wait_send()

        if cond is None:
            copy().start()
            self.pending.append(end)
        else:
            pl.when(cond)(lambda: copy().start())
            self.pending.append(lambda: pl.when(cond)(end))

    def recv(self, key, ref, offset=0, width=1):
        where = self.name(key, width) + offset
        pltpu.make_async_remote_copy(
            ref, ref, self.ss.at[0], self.rs.at[where], device_id=self.here, device_id_type=MESH
        ).wait_recv()

    def local(self, src, dst):
        copy = pltpu.make_async_copy(src, dst, self.ls.at[self.locals])
        self.locals += 1
        return copy

    def finish(self):
        assert self.sends <= N_SEND and self.locals <= N_LOCAL
        assert sum(w for _, w in self.names.values()) <= N_RECV
        for end in self.pending:
            end()


class Stream:
    def __init__(self, net, tag, piece, group, first, second, sibling):
        self.net, self.tag, self.piece, self.group = net, tag, piece, group
        self.a, self.ap, self.am, self.ao, self.to_ap, self.to_am = first
        self.b, self.bp, self.bm, self.bo, self.to_bp, self.to_bm = second
        self.sibling = sibling

    def send(self, what, a, b, device):
        self.net.send((self.tag, what), lambda: (self.piece(a, b), self.piece(a, b), device))

    def recv(self, what, a, b):
        self.net.recv((self.tag, what), self.piece(a, b))

    def both(self, k, a):
        self.send(f"2m{k}", a, self.b, self.to_bp)
        self.send(f"2p{k}", a, self.b, self.to_bm)

    def hand(self, what, b):
        self.net.send((self.tag, what), lambda: (self.group(b), self.group(b), self.sibling))

    def one(self):
        self.send("1m", self.a, self.b, self.to_ap)
        self.send("1p", self.a, self.b, self.to_am)
        self.both(0, self.a)

    def two(self):
        self.recv("1m", self.am, self.b)
        self.send("1o", self.am, self.b, self.to_ap)
        self.both(1, self.am)
        self.recv("1p", self.ap, self.b)
        self.both(2, self.ap)

    def three(self):
        self.recv("1o", self.ao, self.b)
        self.both(3, self.ao)
        self.hand("d0", self.b)

    def four(self):
        self.recv("2m0", self.a, self.bm)
        self.send("2o0", self.a, self.bm, self.to_bp)
        self.recv("2m1", self.am, self.bm)
        self.send("2o1", self.am, self.bm, self.to_bp)
        self.recv("2p2", self.ap, self.bp)
        self.send("2o2", self.ap, self.bp, self.to_bm)
        self.recv("2p3", self.ao, self.bp)
        self.send("2o3", self.ao, self.bp, self.to_bm)
        self.recv("2p0", self.a, self.bp)
        self.recv("2p1", self.am, self.bp)
        self.hand("dp", self.bp)
        self.recv("2m2", self.ap, self.bm)
        self.recv("2m3", self.ao, self.bm)
        self.hand("dm", self.bm)

    def five(self):
        self.recv("2o0", self.a, self.bo)
        self.recv("2o1", self.am, self.bo)
        self.recv("2o2", self.ap, self.bo)
        self.recv("2o3", self.ao, self.bo)
        self.hand("do", self.bo)

    def handed(self, other):
        for what, b in (("d0", self.b), ("dp", self.bp), ("dm", self.bm), ("do", self.bo)):
            self.net.recv((self.tag, what), other(b))


def normed(values, gain):
    floats = values.astype(F32)
    mean = jnp.mean(floats * floats, axis=-1, keepdims=True)
    return (floats * lax.rsqrt(mean + EPS) * gain).astype(BF16)


def kernel(
    tok, g1, gate1, up1, down1, mixg, pool, scale, g2, gate2, up2, down2, out,
    w, pw, xt, xq, n, h, acc, pm, pp, so, sm, sp, ra, rb, a1, hs, hr, mg, ob, sq, rq, oc, of, ss, rs, ls,
):
    rep = lax.axis_index("rep")
    fs = lax.axis_index("fs")
    c = lax.axis_index("tp")
    o = 1 - c
    j = lax.div(fs, 16)
    z = rep * 2 + j
    y = lax.rem(lax.div(fs, 4), 4)
    x = lax.rem(fs, 4)
    zp, zo, zm = (lax.rem(z + k, 4) for k in (1, 2, 3))
    yp, yo, ym = (lax.rem(y + k, 4) for k in (1, 2, 3))
    xp, xo, xm = (lax.rem(x + k, 4) for k in (1, 2, 3))

    def dev(z_, y_, x_, c_):
        return (lax.div(z_, 2), lax.rem(z_, 2) * 16 + y_ * 4 + x_, c_)

    sibling = dev(z, y, x, o)
    net = Net(ss, rs, ls, sibling)
    keeper = c == j
    taker = c != j
    zq = lax.rem(z + 1 + 2 * lax.rem(z + c, 2), 4)
    peer = dev(zq, y, x, c)

    def cols(k):
        return pl.ds(pl.multiple_of(k * UNIT, 128), UNIT)

    def feats(k):
        return pl.ds(pl.multiple_of(k * HALF, 128), HALF)

    def rows(k):
        return pl.ds(pl.multiple_of(k * ROWS, 128), ROWS)

    mats = ((gate1, up1, down1), (gate2, up2, down2), (gate2, up2, down2))
    subs = (lax.div(z, 2), 0, 1)

    own_tok = net.local(tok.at[rows(c), :], xt.at[z, :, feats(c)])
    own_tok.start()
    own_w = []
    for u in range(3):
        base = net.locals
        net.locals += 3
        own_w.append(base)

    def own_copy(u, m):
        return pltpu.make_async_copy(
            mats[u][m].at[:, cols(subs[u])], w.at[u, m, c, y, x], ls.at[own_w[u] + m]
        )

    base_pool = net.locals
    net.locals += 1

    def own_pool():
        return pltpu.make_async_copy(pool, pw.at[c, c, y, x], ls.at[base_pool])

    @pl.when(keeper)
    def _():
        for u in range(3):
            for m in range(3):
                own_copy(u, m).start()
        own_pool().start()

    own_mg = net.local(mixg, mg.at[0, c])
    own_sc = net.local(scale, mg.at[1, c])
    own_mg.start()
    own_sc.start()

    barrier = pltpu.get_barrier_semaphore()
    friends = [dev(z, y, xp, c), dev(z, y, xm, c), dev(z, yp, x, c), dev(z, ym, x, c), sibling]
    friends += [dev(z_, y, x, k) for z_ in (zp, zm) for k in range(2)]
    for friend in friends:
        pl.semaphore_signal(barrier, inc=1, device_id=friend, device_id_type=MESH)
    pl.semaphore_wait(barrier, len(friends))

    def exchange(u):
        for ab, z_ in ((0, zp), (1, zm)):
            sub = (lax.div(z_, 2), 0, 1)[u]
            part = pl.ds(16 * ab, 16)
            for m in range(3):
                net.send(
                    ("z", u, ab, m),
                    lambda m=m, part=part, sub=sub, z_=z_: (
                        mats[u][m].at[part, cols(sub)],
                        w.at[u, m, o, y, x, part, :],
                        dev(z_, y, x, o),
                    ),
                    cond=taker,
                )

    def own(u):
        @pl.when(keeper)
        def _():
            for m in range(3):
                own_copy(u, m).wait()

        @pl.when(taker)
        def _():
            for ab in range(2):
                for m in range(3):
                    net.recv(("z", u, ab, m), w.at[u, m, c, y, x, pl.ds(16 * ab, 16), :])

    in_x = (x, xp, xm, xo, dev(z, y, xp, c), dev(z, y, xm, c))
    in_y = (y, yp, ym, yo, dev(z, yp, x, c), dev(z, ym, x, c))

    def stream_a(u):
        return Stream(
            net, ("a", u),
            lambda a, b: w.at[u, :, c, b, a, pl.ds(0, 16), :],
            lambda b: w.at[u, :, c, b, :, pl.ds(0, 16), :],
            in_x, in_y, sibling,
        )

    def stream_b(u):
        return Stream(
            net, ("b", u),
            lambda a, b: w.at[u, :, c, a, b, pl.ds(16, 16), :],
            lambda b: w.at[u, :, c, :, b, pl.ds(16, 16), :],
            in_y, in_x, sibling,
        )

    sa = [stream_a(u) for u in range(3)]
    sb = [stream_b(u) for u in range(3)]
    spool = Stream(
        net, ("p",),
        lambda a, b: pw.at[:, c, b, a],
        lambda b: pw.at[:, c, b],
        in_x, in_y, sibling,
    )

    def handed(u):
        sa[u].handed(lambda b: w.at[u, :, o, b, :, pl.ds(0, 16), :])
        sb[u].handed(lambda b: w.at[u, :, o, :, b, pl.ds(16, 16), :])

    def spread_tokens():
        net.send("ts", lambda: (tok.at[rows(o), :], xt.at[z, :, feats(c)], sibling))
        for k in range(2):
            for key, z_ in (("tm", zp), ("tp", zm)):
                net.send(
                    key,
                    lambda k=k, z_=z_: (tok.at[rows(k), :], xt.at[z, :, feats(c)], dev(z_, y, x, k)),
                    width=2, shift=c,
                )

    def relay_tokens():
        net.recv("tm", xt.at[zm, :, feats(0)], 0, 2)
        net.send("to0", lambda: (xt.at[zm, :, feats(0)], xt.at[zm, :, feats(0)], dev(zp, y, x, c)))
        net.recv("tp", xt.at[zp, :, feats(1)], 1, 2)
        net.send("to1", lambda: (xt.at[zp, :, feats(1)], xt.at[zp, :, feats(1)], dev(zm, y, x, c)))
        net.recv("tm", xt.at[zm, :, feats(1)], 1, 2)
        net.recv("tp", xt.at[zp, :, feats(0)], 0, 2)

    def gate_up(u, count):
        def step(k, carry):
            part = pl.ds(pl.multiple_of(k * 128, 128), 128)
            wg = w[u, 0, :, :, :, :, part].reshape(D, 128)
            wu = w[u, 1, :, :, :, :, part].reshape(D, 128)
            both = jnp.dot(
                n[pl.ds(0, count), :], jnp.concatenate([wg, wu], axis=1), preferred_element_type=F32
            )
            gate, up = both[:, :128], both[:, 128:]
            h[pl.ds(0, count), part] = (gate * jax.nn.sigmoid(gate) * up).astype(BF16)
            return carry

        lax.fori_loop(0, UNIT // 128, step, 0)

    def down(u, start, count, put):
        def step(k, carry):
            wd = w[u, 2, lax.div(k, 2), pl.ds(lax.rem(k, 2) * 2, 2), :, :, :].reshape(256, UNIT)
            part = lax.dot_general(
                h[pl.ds(start, count), :], wd, (((1,), (1,)), ((), ())), preferred_element_type=F32
            )
            put(pl.ds(pl.multiple_of(k * 256, 256), 256), part)
            return carry

        lax.fori_loop(0, 4, step, 0)

    exchange(0)
    spread_tokens()
    own(0)
    sa[0].one()
    sb[0].one()
    exchange(1)
    exchange(2)
    net.send("ps", lambda: (pool, pw.at[c, o, y, x], sibling), cond=taker)
    net.send("pz", lambda: (pool, pw.at[c, j, y, x], dev(zp, y, x, j)), width=2, shift=c)
    own_mg.wait()
    own_sc.wait()
    net.send("mg", lambda: (mixg, mg.at[0, c], sibling))
    net.send("sc", lambda: (scale, mg.at[1, c], sibling))

    sa[0].two()
    sb[0].two()
    gain1 = g1[...]
    own_tok.wait()
    net.recv("ts", xt.at[z, :, feats(o)])
    n[pl.ds(0, ROWS), :] = normed(xt[z], gain1)
    sa[0].three()
    sb[0].three()
    relay_tokens()
    own(1)
    sa[1].one()
    sb[1].one()
    n[pl.ds(ROWS, ROWS), :] = normed(xt[zm], gain1)
    n[pl.ds(2 * ROWS, ROWS), :] = normed(xt[zp], gain1)
    sa[0].four()
    sb[0].four()
    sa[1].two()
    sb[1].two()

    @pl.when(keeper)
    def _():
        own_pool().wait()
        net.recv("ps", pw.at[o, c, y, x])

    @pl.when(taker)
    def _():
        net.recv("pz", pw.at[0, c, y, x], 0, 2)
        net.recv("pz", pw.at[1, c, y, x], 1, 2)

    spool.one()
    sa[1].three()
    sb[1].three()
    net.recv("to0", xt.at[zo, :, feats(0)])
    net.recv("to1", xt.at[zo, :, feats(1)])
    n[pl.ds(3 * ROWS, ROWS), :] = normed(xt[zo], gain1)
    sa[0].five()
    sb[0].five()
    own(2)
    sa[2].one()
    sb[2].one()
    spool.two()
    handed(0)

    gate_up(0, 4 * ROWS)
    spool.three()
    sa[1].four()
    sb[1].four()

    def put_opposite(part, value):
        so[:, part] = value.astype(BF16)

    down(0, 3 * ROWS, ROWS, put_opposite)
    net.send("r0", lambda: (so.at[:, feats(0)], ra.at[0], dev(zp, y, x, c)))
    net.send("r1", lambda: (so.at[:, feats(1)], ra.at[1], dev(zm, y, x, c)))

    def put_rest(part, value):
        acc[pl.ds(0, ROWS), part] = value[:ROWS]
        pm[:, part] = value[ROWS : 2 * ROWS]
        pp[:, part] = value[2 * ROWS :]

    down(0, 0, 3 * ROWS, put_rest)
    sp[:, HALF:] = pp[:, HALF:].astype(BF16)
    sm[:, :HALF] = pm[:, :HALF].astype(BF16)
    sa[2].two()
    sb[2].two()
    net.send("qm1", lambda: (sp.at[:, feats(1)], rb.at[0, :, feats(1)], dev(zp, y, x, c)))
    net.send("qp0", lambda: (sm.at[:, feats(0)], rb.at[1, :, feats(0)], dev(zm, y, x, c)))
    net.recv("r0", ra.at[0])
    sp[:, :HALF] = (pp[:, :HALF] + ra[0].astype(F32)).astype(BF16)
    net.recv("r1", ra.at[1])
    sm[:, HALF:] = (pm[:, HALF:] + ra[1].astype(F32)).astype(BF16)
    sa[2].three()
    net.send("qm0", lambda: (sp.at[:, feats(0)], rb.at[0, :, feats(0)], dev(zp, y, x, c)))
    net.send("qp1", lambda: (sm.at[:, feats(1)], rb.at[1, :, feats(1)], dev(zm, y, x, c)))
    sb[2].three()
    spool.four()
    sa[1].five()
    sb[1].five()
    spool.five()
    sa[2].four()
    sb[2].four()
    for key, k, half in (("qm", 0, 1), ("qp", 1, 0), ("qm", 0, 0), ("qp", 1, 1)):
        net.recv(f"{key}{half}", rb.at[k, :, feats(half)])
    block = acc[pl.ds(0, ROWS), :] + rb[0].astype(F32) + rb[1].astype(F32)
    a1[...] = (xt[z].astype(F32) + 0.5 * block).astype(BF16)

    net.recv("mg", mg.at[0, o])
    net.recv("sc", mg.at[1, o])
    mix_gain = jnp.concatenate([mg[0, 0], mg[0, 1]], axis=1)
    mix_scale = jnp.concatenate([mg[1, 0], mg[1, 1]], axis=1)
    hidden = normed(a1[...], mix_gain)
    hs[...] = hidden
    spool.handed(lambda b: pw.at[:, o, b])
    net.send("h", lambda: (hs.at[pl.ds(112, 16), :], hr, sibling))
    sa[2].five()
    sb[2].five()
    net.recv("h", hr)
    before = jnp.where(c == 1, hr[...].astype(F32), 0.0)
    floats = hs[...].astype(F32)
    longer = jnp.concatenate([before, floats], axis=0)
    positions = c * ROWS + lax.broadcasted_iota(jnp.int32, (ROWS, 256), 0)
    for g in range(4):
        lanes = slice(256 * g, 256 * g + 256)
        total = longer[:, lanes]
        for k in range(g + 1):
            total = total + pltpu.roll(total, 2**k, axis=0)
        counts = jnp.minimum(positions + 1, 2 ** (g + 1)).astype(F32)
        diff = (total[16:] / counts - floats[:, lanes]).astype(BF16)
        wide = pw[g // 2].reshape(32, 16, 256).astype(F32)
        maps = wide[:, 8 * (g % 2) : 8 * (g % 2) + 8, :].reshape(256, 256).astype(BF16)
        mixed = lax.dot_general(diff, maps, (((1,), (1,)), ((), ())), preferred_element_type=F32)
        after = a1[:, lanes].astype(F32) + mixed * mix_scale[:, lanes]
        ob[:, lanes] = after.astype(BF16)

    net.send("a", lambda: (ob, xq, peer))
    gain2 = g2[...]
    n[pl.ds(0, ROWS), :] = normed(ob[...], gain2)
    handed(1)
    net.recv("a", xq)
    n[pl.ds(ROWS, ROWS), :] = normed(xq[...], gain2)

    def put_first(part, value):
        acc[:, part] = value

    def put_second(part, value):
        acc[:, part] += value

    gate_up(1, 2 * ROWS)
    down(1, 0, 2 * ROWS, put_first)
    handed(2)
    gate_up(2, 2 * ROWS)
    down(2, 0, 2 * ROWS, put_second)
    sq[...] = acc[pl.ds(ROWS, ROWS), :].astype(BF16)
    net.send("b", lambda: (sq, rq, peer))
    net.recv("b", rq)
    block = acc[pl.ds(0, ROWS), :] + rq[...].astype(F32)
    oc[...] = (ob[...].astype(F32) + 0.5 * block).astype(BF16)
    net.send("f", lambda: (oc.at[:, feats(o)], of, sibling))
    out[rows(c), :] = oc[:, feats(c)]
    net.recv("f", of)
    out[rows(o), :] = of[...]
    net.finish()


def local(tok, g1, gate1, up1, down1, mixg, pool, scale, g2, gate2, up2, down2):
    hbm = pl.BlockSpec(memory_space=pl.ANY)
    vmem = pl.BlockSpec(memory_space=pltpu.VMEM)
    result = pl.pallas_call(
        kernel,
        out_shape=jax.ShapeDtypeStruct((256, HALF), BF16),
        in_specs=[hbm, vmem, hbm, hbm, hbm, hbm, hbm, hbm, vmem, hbm, hbm, hbm],
        out_specs=vmem,
        scratch_shapes=[
            pltpu.VMEM((3, 3, 2, 4, 4, 32, UNIT), BF16),
            pltpu.VMEM((2, 2, 4, 4, 16, 256), BF16),
            pltpu.VMEM((4, ROWS, D), BF16),
            pltpu.VMEM((ROWS, D), BF16),
            pltpu.VMEM((4 * ROWS, D), BF16),
            pltpu.VMEM((4 * ROWS, UNIT), BF16),
            pltpu.VMEM((2 * ROWS, D), F32),
            pltpu.VMEM((ROWS, D), F32),
            pltpu.VMEM((ROWS, D), F32),
            pltpu.VMEM((ROWS, D), BF16),
            pltpu.VMEM((ROWS, D), BF16),
            pltpu.VMEM((ROWS, D), BF16),
            pltpu.VMEM((2, ROWS, HALF), BF16),
            pltpu.VMEM((2, ROWS, D), BF16),
            pltpu.VMEM((ROWS, D), BF16),
            pltpu.VMEM((ROWS, D), BF16),
            pltpu.VMEM((16, D), BF16),
            pltpu.VMEM((2, 2, 1, HALF), F32),
            pltpu.VMEM((ROWS, D), BF16),
            pltpu.VMEM((ROWS, D), BF16),
            pltpu.VMEM((ROWS, D), BF16),
            pltpu.VMEM((ROWS, D), BF16),
            pltpu.VMEM((ROWS, HALF), BF16),
            pltpu.SemaphoreType.DMA((N_SEND,)),
            pltpu.SemaphoreType.DMA((N_RECV,)),
            pltpu.SemaphoreType.DMA((N_LOCAL,)),
        ],
        compiler_params=pltpu.CompilerParams(collective_id=0, has_side_effects=True, vmem_limit_bytes=48 * 2**20),
    )(
        tok.reshape(256, HALF), g1.reshape(1, D), gate1, up1, down1.T, mixg.reshape(1, HALF),
        pool.transpose(0, 2, 1).reshape(16, 256), scale.reshape(1, HALF), g2.reshape(1, D), gate2, up2, down2.T,
    )
    return result.reshape(1, 256, HALF)


def solution(mesh):
    placed = (
        P(("rep", "fs"), None, "tp"),
        P(),
        P("fs", "tp"),
        P("fs", "tp"),
        P("tp", "fs"),
        P("tp"),
        P("tp", None, "fs"),
        P("tp"),
        P(),
        P("fs", "tp"),
        P("fs", "tp"),
        P("tp", "fs"),
    )
    return jax.shard_map(
        local, mesh=mesh, in_specs=placed, out_specs=P(("rep", "fs"), None, "tp"), check_vma=False
    )
```

```python
import jax
import jax.numpy as jnp
from jax import lax
from jax.experimental import pallas as pl
from jax.experimental.pallas import tpu as pltpu
from jax.sharding import PartitionSpec as P

MESH = pl.DeviceIdType.MESH
BF16 = jnp.bfloat16
F32 = jnp.float32
EPS = 1e-06
D = 1024
HALF = 512
ROWS = 128
UNIT = 640
N_SEND = 224
N_RECV = 224
N_LOCAL = 16


class Net:
    def __init__(self, ss, rs, ls, here):
        self.ss, self.rs, self.ls, self.here = ss, rs, ls, here
        self.names = {}
        self.sends = 0
        self.locals = 0
        self.pending = []

    def name(self, key, width=1):
        if key not in self.names:
            self.names[key] = sum(w for _, w in self.names.values()), width
        return self.names[key][0]

    def send(self, key, make, cond=None, width=1, shift=None):
        base = self.name(key, width)
        slot = self.sends
        self.sends += 1

        def copy():
            src, dst, device = make()
            where = base if shift is None else base + shift
            return pltpu.make_async_remote_copy(
                src, dst, self.ss.at[slot], self.rs.at[where], device_id=device, device_id_type=MESH
            )

        def end():
            copy().wait_send()

        if cond is None:
            copy().start()
            self.pending.append(end)
        else:
            pl.when(cond)(lambda: copy().start())
            self.pending.append(lambda: pl.when(cond)(end))

    def recv(self, key, ref, offset=0, width=1):
        where = self.name(key, width) + offset
        pltpu.make_async_remote_copy(
            ref, ref, self.ss.at[0], self.rs.at[where], device_id=self.here, device_id_type=MESH
        ).wait_recv()

    def local(self, src, dst):
        copy = pltpu.make_async_copy(src, dst, self.ls.at[self.locals])
        self.locals += 1
        return copy

    def finish(self):
        assert self.sends <= N_SEND and self.locals <= N_LOCAL
        assert sum(w for _, w in self.names.values()) <= N_RECV
        for end in self.pending:
            end()


class Stream:
    def __init__(self, net, tag, piece, group, first, second, sibling):
        self.net, self.tag, self.piece, self.group = net, tag, piece, group
        self.a, self.ap, self.am, self.ao, self.to_ap, self.to_am = first
        self.b, self.bp, self.bm, self.bo, self.to_bp, self.to_bm = second
        self.sibling = sibling

    def send(self, what, a, b, device):
        self.net.send((self.tag, what), lambda: (self.piece(a, b), self.piece(a, b), device))

    def recv(self, what, a, b):
        self.net.recv((self.tag, what), self.piece(a, b))

    def both(self, k, a):
        self.send(f"2m{k}", a, self.b, self.to_bp)
        self.send(f"2p{k}", a, self.b, self.to_bm)

    def hand(self, what, b):
        self.net.send((self.tag, what), lambda: (self.group(b), self.group(b), self.sibling))

    def one(self):
        self.send("1m", self.a, self.b, self.to_ap)
        self.send("1p", self.a, self.b, self.to_am)
        self.both(0, self.a)

    def two(self):
        self.recv("1m", self.am, self.b)
        self.send("1o", self.am, self.b, self.to_ap)
        self.both(1, self.am)
        self.recv("1p", self.ap, self.b)
        self.both(2, self.ap)

    def three(self):
        self.recv("1o", self.ao, self.b)
        self.both(3, self.ao)
        self.hand("d0", self.b)

    def four(self):
        self.recv("2m0", self.a, self.bm)
        self.send("2o0", self.a, self.bm, self.to_bp)
        self.recv("2m1", self.am, self.bm)
        self.send("2o1", self.am, self.bm, self.to_bp)
        self.recv("2p2", self.ap, self.bp)
        self.send("2o2", self.ap, self.bp, self.to_bm)
        self.recv("2p3", self.ao, self.bp)
        self.send("2o3", self.ao, self.bp, self.to_bm)
        self.recv("2p0", self.a, self.bp)
        self.recv("2p1", self.am, self.bp)
        self.hand("dp", self.bp)
        self.recv("2m2", self.ap, self.bm)
        self.recv("2m3", self.ao, self.bm)
        self.hand("dm", self.bm)

    def five(self):
        self.recv("2o0", self.a, self.bo)
        self.recv("2o1", self.am, self.bo)
        self.recv("2o2", self.ap, self.bo)
        self.recv("2o3", self.ao, self.bo)
        self.hand("do", self.bo)

    def handed(self, other):
        for what, b in (("d0", self.b), ("dp", self.bp), ("dm", self.bm), ("do", self.bo)):
            self.net.recv((self.tag, what), other(b))


def normed(values, gain):
    floats = values.astype(F32)
    mean = jnp.mean(floats * floats, axis=-1, keepdims=True)
    return (floats * lax.rsqrt(mean + EPS) * gain).astype(BF16)


def kernel(
    tok, g1, gate1, up1, down1, mixg, pool, scale, g2, gate2, up2, down2, out,
    w, pw, xt, xq, n, h, acc, pm, pp, so, sm, sp, ra, rb, a1, hs, hr, mg, ob, sq, rq, oc, of, ss, rs, ls,
):
    rep = lax.axis_index("rep")
    fs = lax.axis_index("fs")
    c = lax.axis_index("tp")
    o = 1 - c
    j = lax.div(fs, 16)
    z = rep * 2 + j
    y = lax.rem(lax.div(fs, 4), 4)
    x = lax.rem(fs, 4)
    zp, zo, zm = (lax.rem(z + k, 4) for k in (1, 2, 3))
    yp, yo, ym = (lax.rem(y + k, 4) for k in (1, 2, 3))
    xp, xo, xm = (lax.rem(x + k, 4) for k in (1, 2, 3))

    def dev(z_, y_, x_, c_):
        return (lax.div(z_, 2), lax.rem(z_, 2) * 16 + y_ * 4 + x_, c_)

    sibling = dev(z, y, x, o)
    net = Net(ss, rs, ls, sibling)
    keeper = c == j
    taker = c != j
    zq = lax.rem(z + 1 + 2 * lax.rem(z + c, 2), 4)
    peer = dev(zq, y, x, c)

    def cols(k):
        return pl.ds(pl.multiple_of(k * UNIT, 128), UNIT)

    def feats(k):
        return pl.ds(pl.multiple_of(k * HALF, 128), HALF)

    def rows(k):
        return pl.ds(pl.multiple_of(k * ROWS, 128), ROWS)

    mats = ((gate1, up1, down1), (gate2, up2, down2), (gate2, up2, down2))
    subs = (lax.div(z, 2), 0, 1)

    own_tok = net.local(tok.at[rows(c), :], xt.at[z, :, feats(c)])
    own_tok.start()
    own_w = []
    for u in range(3):
        base = net.locals
        net.locals += 3
        own_w.append(base)

    def own_copy(u, m):
        return pltpu.make_async_copy(
            mats[u][m].at[:, cols(subs[u])], w.at[u, m, c, y, x], ls.at[own_w[u] + m]
        )

    base_pool = net.locals
    net.locals += 1

    def own_pool():
        return pltpu.make_async_copy(pool, pw.at[c, c, y, x], ls.at[base_pool])

    @pl.when(keeper)
    def _():
        for u in range(3):
            for m in range(3):
                own_copy(u, m).start()
        own_pool().start()

    own_mg = net.local(mixg, mg.at[0, c])
    own_sc = net.local(scale, mg.at[1, c])
    own_mg.start()
    own_sc.start()

    barrier = pltpu.get_barrier_semaphore()
    friends = [dev(z, y, xp, c), dev(z, y, xm, c), dev(z, yp, x, c), dev(z, ym, x, c), sibling]
    friends += [dev(z_, y, x, k) for z_ in (zp, zm) for k in range(2)]
    for friend in friends:
        pl.semaphore_signal(barrier, inc=1, device_id=friend, device_id_type=MESH)
    pl.semaphore_wait(barrier, len(friends))

    def exchange(u):
        for ab, z_ in ((0, zp), (1, zm)):
            sub = (lax.div(z_, 2), 0, 1)[u]
            part = pl.ds(16 * ab, 16)
            for m in range(3):
                net.send(
                    ("z", u, ab, m),
                    lambda m=m, part=part, sub=sub, z_=z_: (
                        mats[u][m].at[part, cols(sub)],
                        w.at[u, m, o, y, x, part, :],
                        dev(z_, y, x, o),
                    ),
                    cond=taker,
                )

    def own(u):
        @pl.when(keeper)
        def _():
            for m in range(3):
                own_copy(u, m).wait()

        @pl.when(taker)
        def _():
            for ab in range(2):
                for m in range(3):
                    net.recv(("z", u, ab, m), w.at[u, m, c, y, x, pl.ds(16 * ab, 16), :])

    in_x = (x, xp, xm, xo, dev(z, y, xp, c), dev(z, y, xm, c))
    in_y = (y, yp, ym, yo, dev(z, yp, x, c), dev(z, ym, x, c))

    def stream_a(u):
        return Stream(
            net, ("a", u),
            lambda a, b: w.at[u, :, c, b, a, pl.ds(0, 16), :],
            lambda b: w.at[u, :, c, b, :, pl.ds(0, 16), :],
            in_x, in_y, sibling,
        )

    def stream_b(u):
        return Stream(
            net, ("b", u),
            lambda a, b: w.at[u, :, c, a, b, pl.ds(16, 16), :],
            lambda b: w.at[u, :, c, :, b, pl.ds(16, 16), :],
            in_y, in_x, sibling,
        )

    sa = [stream_a(u) for u in range(3)]
    sb = [stream_b(u) for u in range(3)]
    spool = Stream(
        net, ("p",),
        lambda a, b: pw.at[:, c, b, a],
        lambda b: pw.at[:, c, b],
        in_x, in_y, sibling,
    )

    def handed(u):
        sa[u].handed(lambda b: w.at[u, :, o, b, :, pl.ds(0, 16), :])
        sb[u].handed(lambda b: w.at[u, :, o, :, b, pl.ds(16, 16), :])

    def spread_tokens():
        net.send("ts", lambda: (tok.at[rows(o), :], xt.at[z, :, feats(c)], sibling))
        for k in range(2):
            for key, z_ in (("tm", zp), ("tp", zm)):
                net.send(
                    key,
                    lambda k=k, z_=z_: (tok.at[rows(k), :], xt.at[z, :, feats(c)], dev(z_, y, x, k)),
                    width=2, shift=c,
                )

    def relay_tokens():
        net.recv("tm", xt.at[zm, :, feats(0)], 0, 2)
        net.send("to0", lambda: (xt.at[zm, :, feats(0)], xt.at[zm, :, feats(0)], dev(zp, y, x, c)))
        net.recv("tp", xt.at[zp, :, feats(1)], 1, 2)
        net.send("to1", lambda: (xt.at[zp, :, feats(1)], xt.at[zp, :, feats(1)], dev(zm, y, x, c)))
        net.recv("tm", xt.at[zm, :, feats(1)], 1, 2)
        net.recv("tp", xt.at[zp, :, feats(0)], 0, 2)

    def gate_up(u, count):
        def step(k, carry):
            part = pl.ds(pl.multiple_of(k * 128, 128), 128)
            wg = w[u, 0, :, :, :, :, part].reshape(D, 128)
            wu = w[u, 1, :, :, :, :, part].reshape(D, 128)
            both = jnp.dot(
                n[pl.ds(0, count), :], jnp.concatenate([wg, wu], axis=1), preferred_element_type=F32
            )
            gate, up = both[:, :128], both[:, 128:]
            h[pl.ds(0, count), part] = (gate * jax.nn.sigmoid(gate) * up).astype(BF16)
            return carry

        lax.fori_loop(0, UNIT // 128, step, 0)

    def down(u, start, count, put):
        def step(k, carry):
            wd = w[u, 2, lax.div(k, 2), pl.ds(lax.rem(k, 2) * 2, 2), :, :, :].reshape(256, UNIT)
            part = lax.dot_general(
                h[pl.ds(start, count), :], wd, (((1,), (1,)), ((), ())), preferred_element_type=F32
            )
            put(pl.ds(pl.multiple_of(k * 256, 256), 256), part)
            return carry

        lax.fori_loop(0, 4, step, 0)

    exchange(0)
    spread_tokens()
    own(0)
    sa[0].one()
    sb[0].one()
    exchange(1)
    exchange(2)
    net.send("ps", lambda: (pool, pw.at[c, o, y, x], sibling), cond=taker)
    net.send("pz", lambda: (pool, pw.at[c, j, y, x], dev(zp, y, x, j)), width=2, shift=c)
    own_mg.wait()
    own_sc.wait()
    net.send("mg", lambda: (mixg, mg.at[0, c], sibling))
    net.send("sc", lambda: (scale, mg.at[1, c], sibling))

    sa[0].two()
    sb[0].two()
    gain1 = g1[...]
    own_tok.wait()
    net.recv("ts", xt.at[z, :, feats(o)])
    n[pl.ds(0, ROWS), :] = normed(xt[z], gain1)
    sa[0].three()
    sb[0].three()
    relay_tokens()
    own(1)
    sa[1].one()
    sb[1].one()
    n[pl.ds(ROWS, ROWS), :] = normed(xt[zm], gain1)
    n[pl.ds(2 * ROWS, ROWS), :] = normed(xt[zp], gain1)
    sa[0].four()
    sb[0].four()
    sa[1].two()
    sb[1].two()

    @pl.when(keeper)
    def _():
        own_pool().wait()
        net.recv("ps", pw.at[o, c, y, x])

    @pl.when(taker)
    def _():
        net.recv("pz", pw.at[0, c, y, x], 0, 2)
        net.recv("pz", pw.at[1, c, y, x], 1, 2)

    spool.one()
    sa[1].three()
    sb[1].three()
    net.recv("to0", xt.at[zo, :, feats(0)])
    net.recv("to1", xt.at[zo, :, feats(1)])
    n[pl.ds(3 * ROWS, ROWS), :] = normed(xt[zo], gain1)
    sa[0].five()
    sb[0].five()
    own(2)
    sa[2].one()
    sb[2].one()
    spool.two()
    handed(0)

    gate_up(0, 4 * ROWS)
    spool.three()
    sa[1].four()
    sb[1].four()

    def put_opposite(part, value):
        so[:, part] = value.astype(BF16)

    down(0, 3 * ROWS, ROWS, put_opposite)
    net.send("r0", lambda: (so.at[:, feats(0)], ra.at[0], dev(zp, y, x, c)))
    net.send("r1", lambda: (so.at[:, feats(1)], ra.at[1], dev(zm, y, x, c)))

    def put_rest(part, value):
        acc[pl.ds(0, ROWS), part] = value[:ROWS]
        pm[:, part] = value[ROWS : 2 * ROWS]
        pp[:, part] = value[2 * ROWS :]

    down(0, 0, 3 * ROWS, put_rest)
    sp[:, HALF:] = pp[:, HALF:].astype(BF16)
    sm[:, :HALF] = pm[:, :HALF].astype(BF16)
    sa[2].two()
    sb[2].two()
    net.send("qm1", lambda: (sp.at[:, feats(1)], rb.at[0, :, feats(1)], dev(zp, y, x, c)))
    net.send("qp0", lambda: (sm.at[:, feats(0)], rb.at[1, :, feats(0)], dev(zm, y, x, c)))
    net.recv("r0", ra.at[0])
    sp[:, :HALF] = (pp[:, :HALF] + ra[0].astype(F32)).astype(BF16)
    net.recv("r1", ra.at[1])
    sm[:, HALF:] = (pm[:, HALF:] + ra[1].astype(F32)).astype(BF16)
    sa[2].three()
    net.send("qm0", lambda: (sp.at[:, feats(0)], rb.at[0, :, feats(0)], dev(zp, y, x, c)))
    net.send("qp1", lambda: (sm.at[:, feats(1)], rb.at[1, :, feats(1)], dev(zm, y, x, c)))
    sb[2].three()
    spool.four()
    sa[1].five()
    sb[1].five()
    spool.five()
    sa[2].four()
    sb[2].four()
    for key, k, half in (("qm", 0, 1), ("qp", 1, 0), ("qm", 0, 0), ("qp", 1, 1)):
        net.recv(f"{key}{half}", rb.at[k, :, feats(half)])
    block = acc[pl.ds(0, ROWS), :] + rb[0].astype(F32) + rb[1].astype(F32)
    a1[...] = (xt[z].astype(F32) + 0.5 * block).astype(BF16)

    net.recv("mg", mg.at[0, o])
    net.recv("sc", mg.at[1, o])
    mix_gain = jnp.concatenate([mg[0, 0], mg[0, 1]], axis=1)
    mix_scale = jnp.concatenate([mg[1, 0], mg[1, 1]], axis=1)
    hidden = normed(a1[...], mix_gain)
    hs[...] = hidden
    spool.handed(lambda b: pw.at[:, o, b])
    net.send("h", lambda: (hs.at[pl.ds(112, 16), :], hr, sibling))
    sa[2].five()
    sb[2].five()
    net.recv("h", hr)
    before = jnp.where(c == 1, hr[...].astype(F32), 0.0)
    floats = hs[...].astype(F32)
    longer = jnp.concatenate([before, floats], axis=0)
    positions = c * ROWS + lax.broadcasted_iota(jnp.int32, (ROWS, 256), 0)
    for g in range(4):
        lanes = slice(256 * g, 256 * g + 256)
        total = longer[:, lanes]
        for k in range(g + 1):
            total = total + pltpu.roll(total, 2**k, axis=0)
        counts = jnp.minimum(positions + 1, 2 ** (g + 1)).astype(F32)
        diff = (total[16:] / counts - floats[:, lanes]).astype(BF16)
        wide = pw[g // 2].reshape(32, 16, 256).astype(F32)
        maps = wide[:, 8 * (g % 2) : 8 * (g % 2) + 8, :].reshape(256, 256).astype(BF16)
        mixed = lax.dot_general(diff, maps, (((1,), (1,)), ((), ())), preferred_element_type=F32)
        after = a1[:, lanes].astype(F32) + mixed * mix_scale[:, lanes]
        ob[:, lanes] = after.astype(BF16)

    net.send("a", lambda: (ob, xq, peer))
    gain2 = g2[...]
    n[pl.ds(0, ROWS), :] = normed(ob[...], gain2)
    handed(1)
    net.recv("a", xq)
    n[pl.ds(ROWS, ROWS), :] = normed(xq[...], gain2)

    def put_first(part, value):
        acc[:, part] = value

    def put_second(part, value):
        acc[:, part] += value

    gate_up(1, 2 * ROWS)
    down(1, 0, 2 * ROWS, put_first)
    handed(2)
    gate_up(2, 2 * ROWS)
    down(2, 0, 2 * ROWS, put_second)
    sq[...] = acc[pl.ds(ROWS, ROWS), :].astype(BF16)
    net.send("b", lambda: (sq, rq, peer))
    net.recv("b", rq)
    block = acc[pl.ds(0, ROWS), :] + rq[...].astype(F32)
    oc[...] = (ob[...].astype(F32) + 0.5 * block).astype(BF16)
    net.send("f", lambda: (oc.at[:, feats(o)], of, sibling))
    out[rows(c), :] = oc[:, feats(c)]
    net.recv("f", of)
    out[rows(o), :] = of[...]
    net.finish()


def local(tok, g1, gate1, up1, down1, mixg, pool, scale, g2, gate2, up2, down2):
    hbm = pl.BlockSpec(memory_space=pl.ANY)
    vmem = pl.BlockSpec(memory_space=pltpu.VMEM)
    result = pl.pallas_call(
        kernel,
        out_shape=jax.ShapeDtypeStruct((256, HALF), BF16),
        in_specs=[hbm, vmem, hbm, hbm, hbm, hbm, hbm, hbm, vmem, hbm, hbm, hbm],
        out_specs=vmem,
        scratch_shapes=[
            pltpu.VMEM((3, 3, 2, 4, 4, 32, UNIT), BF16),
            pltpu.VMEM((2, 2, 4, 4, 16, 256), BF16),
            pltpu.VMEM((4, ROWS, D), BF16),
            pltpu.VMEM((ROWS, D), BF16),
            pltpu.VMEM((4 * ROWS, D), BF16),
            pltpu.VMEM((4 * ROWS, UNIT), BF16),
            pltpu.VMEM((2 * ROWS, D), F32),
            pltpu.VMEM((ROWS, D), F32),
            pltpu.VMEM((ROWS, D), F32),
            pltpu.VMEM((ROWS, D), BF16),
            pltpu.VMEM((ROWS, D), BF16),
            pltpu.VMEM((ROWS, D), BF16),
            pltpu.VMEM((2, ROWS, HALF), BF16),
            pltpu.VMEM((2, ROWS, D), BF16),
            pltpu.VMEM((ROWS, D), BF16),
            pltpu.VMEM((ROWS, D), BF16),
            pltpu.VMEM((16, D), BF16),
            pltpu.VMEM((2, 2, 1, HALF), F32),
            pltpu.VMEM((ROWS, D), BF16),
            pltpu.VMEM((ROWS, D), BF16),
            pltpu.VMEM((ROWS, D), BF16),
            pltpu.VMEM((ROWS, D), BF16),
            pltpu.VMEM((ROWS, HALF), BF16),
            pltpu.SemaphoreType.DMA((N_SEND,)),
            pltpu.SemaphoreType.DMA((N_RECV,)),
            pltpu.SemaphoreType.DMA((N_LOCAL,)),
        ],
        compiler_params=pltpu.CompilerParams(collective_id=0, has_side_effects=True, vmem_limit_bytes=67043328),
    )(
        tok.reshape(256, HALF), g1.reshape(1, D), gate1, up1, down1.T, mixg.reshape(1, HALF),
        pool.transpose(0, 2, 1).reshape(16, 256), scale.reshape(1, HALF), g2.reshape(1, D), gate2, up2, down2.T,
    )
    return result.reshape(1, 256, HALF)


def solution(mesh):
    placed = (
        P(("rep", "fs"), None, "tp"),
        P(),
        P("fs", "tp"),
        P("fs", "tp"),
        P("tp", "fs"),
        P("tp"),
        P("tp", None, "fs"),
        P("tp"),
        P(),
        P("fs", "tp"),
        P("fs", "tp"),
        P("tp", "fs"),
    )
    return jax.shard_map(
        local, mesh=mesh, in_specs=placed, out_specs=P(("rep", "fs"), None, "tp"), check_vma=False
    )
```

```python
import jax
import jax.numpy as jnp
from jax import lax
from jax.experimental import pallas as pl
from jax.experimental.pallas import tpu as pltpu
from jax.sharding import PartitionSpec as P

MESH = pl.DeviceIdType.MESH
BF16 = jnp.bfloat16
F32 = jnp.float32
EPS = 1e-06
D = 1024
HALF = 512
ROWS = 128
UNIT = 640
N_SEND = 35
N_RECV = 98
N_LOCAL = 7


class Net:
    def __init__(self, ss, rs, ls, here):
        self.ss, self.rs, self.ls, self.here = ss, rs, ls, here
        self.names = {}
        self.batches = {}
        self.locals = 0
        self.sends = 0
        self.pending = []

    def name(self, key, width=1):
        if key not in self.names:
            self.names[key] = sum(w for _, w in self.names.values()), width
        return self.names[key][0]

    def send(self, key, make, cond=None, width=1, shift=None, batch=None, total=None):
        base = self.name(key, width)
        first = batch is None or batch not in self.batches
        if first:
            slot = self.sends
            self.sends += 1
            if batch is not None:
                self.batches[batch] = slot
        else:
            slot = self.batches[batch]

        def copy(src, dst, device):
            where = base if shift is None else base + shift
            return pltpu.make_async_remote_copy(
                src, dst, self.ss.at[slot], self.rs.at[where], device_id=device, device_id_type=MESH
            )

        def end():
            ref = make()[0] if total is None else total()
            copy(ref, ref, self.here).wait_send()

        if cond is None:
            copy(*make()).start()
        else:
            pl.when(cond)(lambda: copy(*make()).start())
        if first:
            self.pending.append(end if cond is None else lambda: pl.when(cond)(end))

    def recv(self, key, ref, offset=0, width=1):
        where = self.name(key, width) + offset
        pltpu.make_async_remote_copy(
            ref, ref, self.ss.at[0], self.rs.at[where], device_id=self.here, device_id_type=MESH
        ).wait_recv()

    def slot(self):
        self.locals += 1
        return self.ls.at[self.locals - 1]

    def local(self, src, dst):
        return pltpu.make_async_copy(src, dst, self.slot())

    def finish(self):
        for end in self.pending:
            end()
        assert self.sends == N_SEND and self.locals == N_LOCAL
        assert sum(w for _, w in self.names.values()) == N_RECV


class Stream:
    def __init__(self, net, unit, tag, direct, piece, group, size, many, first, second, sibling):
        self.net, self.unit, self.tag, self.direct = net, unit, (unit, tag), direct
        self.piece, self.group, self.size, self.many = piece, group, size, many
        self.a, self.ap, self.am, self.ao, self.to_ap, self.to_am, self.to_ao = first
        self.b, self.bp, self.bm, self.bo, self.to_bp, self.to_bm, self.to_bo = second
        self.sibling = sibling

    def send(self, what, a, b, device, kind, count):
        self.net.send(
            (self.tag, what),
            lambda: (self.piece(a, b), self.piece(a, b), device),
            batch=(self.unit, kind),
            total=lambda: self.size(count * self.many),
        )

    def recv(self, what, a, b):
        self.net.recv((self.tag, what), self.piece(a, b))

    def both(self, k, a):
        late_m, late_p = ("2m23" if k >= 2 else f"2m{k}"), ("2p01" if k < 2 else f"2p{k}")
        self.send(late_m, a, self.b, self.to_bp, "both", 8)
        self.send(late_p, a, self.b, self.to_bm, "both", 8)

    def hand(self, b):
        self.net.send(
            (self.unit, "d"),
            lambda: (self.group(b), self.group(b), self.sibling),
            batch=(self.unit, "hand"),
            total=lambda: self.size(16 * self.many),
        )

    def one(self):
        self.send("1m", self.a, self.b, self.to_ap, "ring", 2)
        self.send("1p", self.a, self.b, self.to_am, "ring", 2)
        if self.direct:
            self.send("1o", self.a, self.b, self.to_ao, "far", 1)

    def then(self):
        self.both(0, self.a)

    def two(self):
        self.recv("1m", self.am, self.b)
        if not self.direct:
            self.send("1o", self.am, self.b, self.to_ap, "far", 1)
        self.both(1, self.am)
        self.recv("1p", self.ap, self.b)
        self.both(2, self.ap)

    def three(self):
        self.recv("1o", self.ao, self.b)
        self.both(3, self.ao)
        self.hand(self.b)

    def four(self):
        self.recv("2m0", self.a, self.bm)
        self.send("2o", self.a, self.bm, self.to_bp, "on", 4)
        self.recv("2m1", self.am, self.bm)
        self.send("2o", self.am, self.bm, self.to_bp, "on", 4)
        self.recv("2p2", self.ap, self.bp)
        self.send("2o", self.ap, self.bp, self.to_bm, "on", 4)
        self.recv("2p3", self.ao, self.bp)
        self.send("2o", self.ao, self.bp, self.to_bm, "on", 4)
        self.net.recv((self.tag, "2p01"), self.size(2))
        self.hand(self.bp)
        self.net.recv((self.tag, "2m23"), self.size(2))
        self.hand(self.bm)

    def five(self):
        self.net.recv((self.tag, "2o"), self.size(4))
        self.hand(self.bo)


def normed(values, gain):
    floats = values.astype(F32)
    mean = jnp.mean(floats * floats, axis=-1, keepdims=True)
    return (floats * lax.rsqrt(mean + EPS) * gain).astype(BF16)


def kernel(
    tok, g1, gate1, up1, down1, mixg, pool, scale, g2, gate2, up2, down2, out,
    w, pw, xt, xq, n, h1, h2, wd1, wd2, maps, own1, pm, pp, so, sm, sp, ra, rb, a1, hs, hr, mg, ob, sq, rq, base, rx,
    ss, rs, ls,
):
    rep = lax.axis_index("rep")
    fs = lax.axis_index("fs")
    c = lax.axis_index("tp")
    o = 1 - c
    j = lax.div(fs, 16)
    z = rep * 2 + j
    y = lax.rem(lax.div(fs, 4), 4)
    x = lax.rem(fs, 4)
    zp, zo, zm = (lax.rem(z + k, 4) for k in (1, 2, 3))
    yp, yo, ym = (lax.rem(y + k, 4) for k in (1, 2, 3))
    xp, xo, xm = (lax.rem(x + k, 4) for k in (1, 2, 3))

    def dev(z_, y_, x_, c_):
        return (lax.div(z_, 2), lax.rem(z_, 2) * 16 + y_ * 4 + x_, c_)

    sibling = dev(z, y, x, o)
    net = Net(ss, rs, ls, sibling)
    keeper = c == j
    taker = c != j
    zq = lax.rem(z + 1 + 2 * lax.rem(z + c, 2), 4)

    def cols(k):
        return pl.ds(pl.multiple_of(k * UNIT, 128), UNIT)

    def feats(k):
        return pl.ds(pl.multiple_of(k * HALF, 128), HALF)

    def rows(k):
        return pl.ds(pl.multiple_of(k * ROWS, 128), ROWS)

    mats = ((gate1, up1, down1), (gate2, up2, down2), (gate2, up2, down2))
    subs = (lax.div(z, 2), 0, 1)

    own_tok = net.local(tok.at[rows(c), :], xt.at[z, :, feats(c)])
    own_tok.start()
    own_w = [net.slot() for u in range(3)]
    own_p = net.slot()

    def own_pool():
        return pltpu.make_async_copy(pool, pw.at[c, c, y, x], own_p)

    @pl.when(keeper)
    def _():
        for u in range(3):
            for m in range(3):
                pltpu.make_async_copy(mats[u][m].at[:, cols(subs[u])], w.at[u, m, c, y, x], own_w[u]).start()
        own_pool().start()

    own_mg = net.local(mixg, mg.at[0, c])
    own_sc = net.local(scale, mg.at[1, c])
    own_mg.start()
    own_sc.start()

    barrier = pltpu.get_barrier_semaphore()
    friends = [dev(z, y, x_, c) for x_ in (xp, xm, xo)] + [dev(z, y_, x, c) for y_ in (yp, ym, yo)] + [sibling]
    friends += [dev(z_, y, x, k) for z_ in (zp, zm) for k in range(2)]
    for friend in friends:
        pl.semaphore_signal(barrier, inc=1, device_id=friend, device_id_type=MESH)
    pl.semaphore_wait(barrier, len(friends))

    def exchange(u):
        for ab, z_ in ((0, zp), (1, zm)):
            sub = (lax.div(z_, 2), 0, 1)[u]
            part = pl.ds(16 * ab, 16)
            for m in range(3):
                net.send(
                    ("z", u),
                    lambda m=m, part=part, sub=sub, z_=z_: (
                        mats[u][m].at[part, cols(sub)],
                        w.at[u, m, o, y, x, part, :],
                        dev(z_, y, x, o),
                    ),
                    cond=taker,
                    batch=("z", u),
                    total=lambda: w.at[u, :, 0, 0, 0],
                )

    def own(u):
        ref = w.at[u, :, c, y, x]

        @pl.when(keeper)
        def _():
            pltpu.make_async_copy(ref, ref, own_w[u]).wait()

        @pl.when(taker)
        def _():
            net.recv(("z", u), ref)

    in_x = (x, xp, xm, xo, dev(z, y, xp, c), dev(z, y, xm, c), dev(z, y, xo, c))
    in_y = (y, yp, ym, yo, dev(z, yp, x, c), dev(z, ym, x, c), dev(z, yo, x, c))
    two, top, low = pl.ds(0, 2), pl.ds(0, 16), pl.ds(16, 16)

    def size_w(k):
        return {
            2: w.at[0, :, 0, two, 0, top],
            4: w.at[0, :, 0, :, 0, top],
            8: w.at[0, :, 0, two, :, top],
            16: w.at[0, :, 0, :, :, top],
            32: w.at[0, :, 0],
        }[k]

    def size_p(k):
        return {1: pw.at[:, 0, 0, 0], 2: pw.at[:, 0, two, 0], 4: pw.at[:, 0, 0], 8: pw.at[:, 0, two], 16: pw.at[:, 0]}[k]

    def stream_a(u):
        return Stream(
            net, u, "a", u == 0,
            lambda a, b: w.at[u, :, c, b, a, top, :],
            lambda b: w.at[u, :, c, b, :, top, :],
            size_w, 2, in_x, in_y, sibling,
        )

    def stream_b(u):
        return Stream(
            net, u, "b", u == 0,
            lambda a, b: w.at[u, :, c, a, b, low, :],
            lambda b: w.at[u, :, c, :, b, low, :],
            size_w, 2, in_y, in_x, sibling,
        )

    sa = [stream_a(u) for u in range(3)]
    sb = [stream_b(u) for u in range(3)]
    spool = Stream(
        net, "p", "a", False, lambda a, b: pw.at[:, c, b, a], lambda b: pw.at[:, c, b], size_p, 1, in_x, in_y, sibling
    )

    def start(u):
        own(u)
        sa[u].one()
        sb[u].one()
        sa[u].then()
        sb[u].then()

    def handed(u):
        net.recv((u, "d"), w.at[u, :, o])

    def spread_tokens():
        for k in range(2):
            for key, z_ in (("tm", zp), ("tp", zm)):
                net.send(
                    key,
                    lambda k=k, z_=z_: (tok.at[rows(k), :], xt.at[z, :, feats(c)], dev(z_, y, x, k)),
                    width=2, shift=c, batch="t4", total=lambda: xt.at[pl.ds(0, 2)],
                )
        net.send("ts", lambda: (tok.at[rows(o), :], xt.at[z, :, feats(c)], sibling))

    def relay_tokens():
        for key, who, half, to in (("tm", zm, 0, zp), ("tp", zp, 1, zm)):
            net.recv(key, xt.at[who, :, feats(half)], half, 2)
            net.send(
                "to",
                lambda who=who, half=half, to=to: (
                    xt.at[who, :, feats(half)], xt.at[who, :, feats(half)], dev(to, y, x, c)
                ),
                batch="t2", total=lambda: xt.at[0],
            )
        net.recv("tm", xt.at[zm, :, feats(1)], 1, 2)
        net.recv("tp", xt.at[zp, :, feats(0)], 0, 2)

    def gate_up(u, at, count, put):
        for k in range(UNIT // 128):
            part = pl.ds(k * 128, 128)
            wg = w[u, 0, :, :, :, :, part].reshape(D, 128)
            wu = w[u, 1, :, :, :, :, part].reshape(D, 128)
            both = jnp.dot(
                n[pl.ds(at, count), :], jnp.concatenate([wg, wu], axis=1), preferred_element_type=F32
            )
            gate, up = both[:, :128], both[:, 128:]
            put(k * 128, (gate * jax.nn.sigmoid(gate) * up).astype(BF16))

    def put1(at, count):
        def put(k, value):
            h1[pl.ds(at, count), pl.ds(k, 128)] = value

        return put

    def put2(at, count, first):
        def put(k, value):
            h2[pl.ds(at, count), pl.ds(first + k, 128)] = value

        return put

    def turn(u, part, wide, at):
        for k in range(2):
            block = w[u, 2, part, 2 * k : 2 * k + 2].reshape(256, UNIT)
            wide[pl.ds(at, UNIT), pl.ds(pl.multiple_of(part * HALF + 256 * k, 128), 256)] = block.T

    def dot(lhs, rhs):
        return jnp.dot(lhs, rhs, preferred_element_type=F32)

    exchange(0)
    spread_tokens()
    start(0)
    exchange(1)
    exchange(2)
    net.send("ps", lambda: (pool, pw.at[c, o, y, x], sibling), cond=taker)
    net.send("pz", lambda: (pool, pw.at[c, j, y, x], dev(zp, y, x, j)), width=2, shift=c)
    own_mg.wait()
    own_sc.wait()
    net.send("mg", lambda: (mixg, mg.at[0, c], sibling), batch="mg", total=lambda: mg.at[:, 0])
    net.send("mg", lambda: (scale, mg.at[1, c], sibling), batch="mg", total=lambda: mg.at[:, 0])

    sa[0].two()
    sb[0].two()
    gain1 = g1[...]
    own_tok.wait()
    net.recv("ts", xt.at[z, :, feats(o)])
    n[pl.ds(0, ROWS), :] = normed(xt[z], gain1)
    sa[0].three()
    sb[0].three()
    relay_tokens()
    sa[0].four()
    sb[0].four()
    start(1)

    @pl.when(keeper)
    def _():
        own_pool().wait()
        net.recv("ps", pw.at[o, c, y, x])

    @pl.when(taker)
    def _():
        net.recv("pz", pw.at[0, c, y, x], 0, 2)
        net.recv("pz", pw.at[1, c, y, x], 1, 2)

    spool.one()
    spool.then()
    start(2)
    n[pl.ds(ROWS, ROWS), :] = normed(xt[zm], gain1)
    n[pl.ds(2 * ROWS, ROWS), :] = normed(xt[zp], gain1)
    net.recv("to", xt.at[zo])
    n[pl.ds(3 * ROWS, ROWS), :] = normed(xt[zo], gain1)
    sa[0].five()
    sb[0].five()
    turn(0, c, wd1, 0)
    handed(0)

    gate_up(0, 3 * ROWS, ROWS, put1(3 * ROWS, ROWS))
    turn(0, o, wd1, 0)
    so[...] = dot(h1[pl.ds(3 * ROWS, ROWS), :], wd1[...]).astype(BF16)
    net.send("r0", lambda: (so.at[:, feats(0)], ra.at[0], dev(zp, y, x, c)), batch="r", total=lambda: so)
    net.send("r1", lambda: (so.at[:, feats(1)], ra.at[1], dev(zm, y, x, c)), batch="r", total=lambda: so)
    sa[1].two()
    sb[1].two()
    spool.two()
    gate_up(0, ROWS, 2 * ROWS, put1(ROWS, 2 * ROWS))
    sums = dot(h1[pl.ds(ROWS, 2 * ROWS), :], wd1[...])
    sm[:, :HALF] = sums[:ROWS, :HALF].astype(BF16)
    sp[:, HALF:] = sums[ROWS:, HALF:].astype(BF16)
    pm[...] = sums[:ROWS, HALF:]
    pp[...] = sums[ROWS:, :HALF]

    def pass_on(key, buf, k, half, z_):
        net.send(
            f"{key}{half}",
            lambda: (buf.at[:, feats(half)], rb.at[k, :, feats(half)], dev(z_, y, x, c)),
            batch="q", total=lambda: xt.at[two],
        )

    pass_on("qm", sp, 0, 1, zp)
    pass_on("qp", sm, 1, 0, zm)
    sa[1].three()
    sb[1].three()
    spool.three()
    gate_up(0, 0, ROWS, put1(0, ROWS))
    own1[...] = dot(h1[pl.ds(0, ROWS), :], wd1[...])
    net.recv("r0", ra.at[0])
    sp[:, :HALF] = (pp[...] + ra[0].astype(F32)).astype(BF16)
    net.recv("r1", ra.at[1])
    sm[:, HALF:] = (pm[...] + ra[1].astype(F32)).astype(BF16)
    pass_on("qm", sp, 0, 0, zp)
    pass_on("qp", sm, 1, 1, zm)
    sa[2].two()
    sb[2].two()
    sa[1].four()
    sb[1].four()
    spool.four()
    sa[2].three()
    sb[2].three()
    spool.five()
    net.recv(("p", "d"), pw.at[:, o])
    for g in range(4):
        wide = pw[g // 2].reshape(32, 16, 256).astype(F32)
        maps[g] = wide[:, 8 * (g % 2) : 8 * (g % 2) + 8, :].reshape(256, 256).astype(BF16).T
    sa[1].five()
    sb[1].five()
    turn(1, c, wd2, 0)
    for key, k, half in (("qm", 0, 1), ("qp", 1, 0), ("qm", 0, 0), ("qp", 1, 1)):
        net.recv(f"{key}{half}", rb.at[k, :, feats(half)])
    block = own1[...] + rb[0].astype(F32) + rb[1].astype(F32)
    a1[...] = (xt[z].astype(F32) + 0.5 * block).astype(BF16)

    net.recv("mg", mg.at[:, o])
    mix_gain = jnp.concatenate([mg[0, 0], mg[0, 1]], axis=1)
    mix_scale = jnp.concatenate([mg[1, 0], mg[1, 1]], axis=1)
    hidden = normed(a1[...], mix_gain)
    hs[...] = hidden
    net.send("h", lambda: (hs.at[pl.ds(112, 16), :], hr, sibling))
    net.recv("h", hr)
    before = jnp.where(c == 1, hr[...].astype(F32), 0.0)
    floats = hs[...].astype(F32)
    longer = jnp.concatenate([before, floats], axis=0)
    positions = c * ROWS + lax.broadcasted_iota(jnp.int32, (ROWS, 256), 0)
    for g in range(4):
        lanes = slice(256 * g, 256 * g + 256)
        total = longer[:, lanes]
        for k in range(g + 1):
            total = total + pltpu.roll(total, 2**k, axis=0)
        counts = jnp.minimum(positions + 1, 2 ** (g + 1)).astype(F32)
        diff = (total[16:] / counts - floats[:, lanes]).astype(BF16)
        mixed = dot(diff, maps[g])
        after = a1[:, lanes].astype(F32) + mixed * mix_scale[:, lanes]
        ob[:, lanes] = after.astype(BF16)

    net.send("a", lambda: (ob, xq, dev(zq, y, x, c)))
    gain2 = g2[...]
    n[pl.ds(0, ROWS), :] = normed(ob[...], gain2)
    sa[2].four()
    sb[2].four()
    handed(1)
    gate_up(1, 0, ROWS, put2(0, ROWS, 0))
    turn(1, o, wd2, 0)
    sa[2].five()
    sb[2].five()
    turn(2, c, wd2, UNIT)
    net.recv("a", xq)
    n[pl.ds(ROWS, ROWS), :] = normed(xq[...], gain2)
    gate_up(1, ROWS, ROWS, put2(ROWS, ROWS, 0))
    handed(2)
    gate_up(2, ROWS, ROWS, put2(ROWS, ROWS, UNIT))
    turn(2, o, wd2, UNIT)
    sq[...] = dot(h2[pl.ds(ROWS, ROWS), :], wd2[...]).astype(BF16)
    for k in range(2):
        net.send(
            "b",
            lambda k=k: (sq.at[:, feats(k)], rq.at[c], dev(zq, y, x, k)),
            width=2, shift=c, batch="b", total=lambda: sq,
        )
    gate_up(2, 0, ROWS, put2(0, ROWS, UNIT))
    base[...] = ob[...].astype(F32) + 0.5 * dot(h2[pl.ds(0, ROWS), :], wd2[...])
    net.send("f", lambda: (base.at[:, feats(o)], rx, sibling))
    net.recv("b", rq.at[c], c, 2)
    out[rows(c), :] = (base[:, feats(c)] + 0.5 * rq[c].astype(F32)).astype(BF16)
    net.recv("f", rx)
    net.recv("b", rq.at[o], o, 2)
    out[rows(o), :] = (rx[...] + 0.5 * rq[o].astype(F32)).astype(BF16)
    net.finish()


def local(tok, g1, gate1, up1, down1, mixg, pool, scale, g2, gate2, up2, down2):
    hbm = pl.BlockSpec(memory_space=pl.ANY)
    vmem = pl.BlockSpec(memory_space=pltpu.VMEM)
    result = pl.pallas_call(
        kernel,
        out_shape=jax.ShapeDtypeStruct((256, HALF), BF16),
        in_specs=[hbm, vmem, hbm, hbm, hbm, hbm, hbm, hbm, vmem, hbm, hbm, hbm],
        out_specs=vmem,
        scratch_shapes=[
            pltpu.VMEM((3, 3, 2, 4, 4, 32, UNIT), BF16),
            pltpu.VMEM((2, 2, 4, 4, 16, 256), BF16),
            pltpu.VMEM((4, ROWS, D), BF16),
            pltpu.VMEM((ROWS, D), BF16),
            pltpu.VMEM((4 * ROWS, D), BF16),
            pltpu.VMEM((4 * ROWS, UNIT), BF16),
            pltpu.VMEM((2 * ROWS, 2 * UNIT), BF16),
            pltpu.VMEM((UNIT, D), BF16),
            pltpu.VMEM((2 * UNIT, D), BF16),
            pltpu.VMEM((4, 256, 256), BF16),
            pltpu.VMEM((ROWS, D), F32),
            pltpu.VMEM((ROWS, HALF), F32),
            pltpu.VMEM((ROWS, HALF), F32),
            pltpu.VMEM((ROWS, D), BF16),
            pltpu.VMEM((ROWS, D), BF16),
            pltpu.VMEM((ROWS, D), BF16),
            pltpu.VMEM((2, ROWS, HALF), BF16),
            pltpu.VMEM((2, ROWS, D), BF16),
            pltpu.VMEM((ROWS, D), BF16),
            pltpu.VMEM((ROWS, D), BF16),
            pltpu.VMEM((16, D), BF16),
            pltpu.VMEM((2, 2, 1, HALF), F32),
            pltpu.VMEM((ROWS, D), BF16),
            pltpu.VMEM((ROWS, D), BF16),
            pltpu.VMEM((2, ROWS, HALF), BF16),
            pltpu.VMEM((ROWS, D), F32),
            pltpu.VMEM((ROWS, HALF), F32),
            pltpu.SemaphoreType.DMA((N_SEND,)),
            pltpu.SemaphoreType.DMA((N_RECV,)),
            pltpu.SemaphoreType.DMA((N_LOCAL,)),
        ],
        compiler_params=pltpu.CompilerParams(collective_id=0, has_side_effects=True, vmem_limit_bytes=67043328),
    )(
        tok.reshape(256, HALF), g1.reshape(1, D), gate1, up1, down1.T, mixg.reshape(1, HALF),
        pool.transpose(0, 2, 1).reshape(16, 256), scale.reshape(1, HALF), g2.reshape(1, D), gate2, up2, down2.T,
    )
    return result.reshape(1, 256, HALF)


def solution(mesh):
    placed = (
        P(("rep", "fs"), None, "tp"),
        P(),
        P("fs", "tp"),
        P("fs", "tp"),
        P("tp", "fs"),
        P("tp"),
        P("tp", None, "fs"),
        P("tp"),
        P(),
        P("fs", "tp"),
        P("fs", "tp"),
        P("tp", "fs"),
    )
    return jax.shard_map(
        local, mesh=mesh, in_specs=placed, out_specs=P(("rep", "fs"), None, "tp"), check_vma=False
    )
```

```python
import jax
import jax.numpy as jnp
from jax import lax
from jax.experimental import pallas as pl
from jax.experimental.pallas import tpu as pltpu
from jax.sharding import PartitionSpec as P

MESH = pl.DeviceIdType.MESH
BF16 = jnp.bfloat16
F32 = jnp.float32
EPS = 1e-06
D = 1024
HALF = 512
ROWS = 128
UNIT = 640
DIRECT = True
N_SEND = 35
N_RECV = 90
N_LOCAL = 10


class Net:
    def __init__(self, ss, rs, ls, here):
        self.ss, self.rs, self.ls, self.here = ss, rs, ls, here
        self.names = {}
        self.batches = {}
        self.locals = 0
        self.sends = 0
        self.pending = []

    def name(self, key, width=1):
        if key not in self.names:
            self.names[key] = sum(w for _, w in self.names.values()), width
        return self.names[key][0]

    def send(self, key, make, cond=None, width=1, shift=None, batch=None, total=None):
        base = self.name(key, width)
        first = batch is None or batch not in self.batches
        if first:
            slot = self.sends
            self.sends += 1
            if batch is not None:
                self.batches[batch] = slot
        else:
            slot = self.batches[batch]

        def copy(src, dst, device):
            where = base if shift is None else base + shift
            return pltpu.make_async_remote_copy(
                src, dst, self.ss.at[slot], self.rs.at[where], device_id=device, device_id_type=MESH
            )

        def end():
            ref = make()[0] if total is None else total()
            copy(ref, ref, self.here).wait_send()

        if cond is None:
            copy(*make()).start()
        else:
            pl.when(cond)(lambda: copy(*make()).start())
        if first:
            self.pending.append(end if cond is None else lambda: pl.when(cond)(end))

    def recv(self, key, ref, offset=0, width=1):
        where = self.name(key, width) + offset
        pltpu.make_async_remote_copy(
            ref, ref, self.ss.at[0], self.rs.at[where], device_id=self.here, device_id_type=MESH
        ).wait_recv()

    def slot(self):
        self.locals += 1
        return self.ls.at[self.locals - 1]

    def local(self, src, dst):
        return pltpu.make_async_copy(src, dst, self.slot())

    def finish(self):
        for end in self.pending:
            end()
        assert self.sends == N_SEND and self.locals == N_LOCAL
        assert sum(w for _, w in self.names.values()) == N_RECV


class Stream:
    def __init__(self, net, unit, tag, direct, piece, group, size, many, first, second, sibling):
        self.net, self.unit, self.tag, self.direct = net, unit, (unit, tag), direct
        self.piece, self.group, self.size, self.many = piece, group, size, many
        self.a, self.ap, self.am, self.ao, self.to_ap, self.to_am, self.to_ao = first
        self.b, self.bp, self.bm, self.bo, self.to_bp, self.to_bm, self.to_bo = second
        self.sibling = sibling

    def send(self, what, a, b, device, kind, count):
        self.net.send(
            (self.tag, what),
            lambda: (self.piece(a, b), self.piece(a, b), device),
            batch=(self.unit, kind),
            total=lambda: self.size(count * self.many),
        )

    def recv(self, what, a, b):
        self.net.recv((self.tag, what), self.piece(a, b))

    def both(self, k, a):
        late_m, late_p = ("2m23" if k >= 2 else f"2m{k}"), ("2p01" if k < 2 else f"2p{k}")
        self.send(late_m, a, self.b, self.to_bp, "both", 8)
        self.send(late_p, a, self.b, self.to_bm, "both", 8)

    def hand(self, b):
        self.net.send(
            (self.unit, "d"),
            lambda: (self.group(b), self.group(b), self.sibling),
            batch=(self.unit, "hand"),
            total=lambda: self.size(16 * self.many),
        )

    def one(self):
        self.send("1m", self.a, self.b, self.to_ap, "ring", 2)
        self.send("1p", self.a, self.b, self.to_am, "ring", 2)
        if self.direct:
            self.send("1o", self.a, self.b, self.to_ao, "far", 1)

    def then(self):
        self.both(0, self.a)

    def two(self):
        self.recv("1m", self.am, self.b)
        if not self.direct:
            self.send("1o", self.am, self.b, self.to_ap, "far", 1)
        self.both(1, self.am)
        self.recv("1p", self.ap, self.b)
        self.both(2, self.ap)

    def three(self):
        self.recv("1o", self.ao, self.b)
        self.both(3, self.ao)
        self.hand(self.b)

    def pre(self):
        self.recv("2m0", self.a, self.bm)
        self.send("2o", self.a, self.bm, self.to_bp, "on", 4)

    def four(self):
        self.recv("2m1", self.am, self.bm)
        self.send("2o", self.am, self.bm, self.to_bp, "on", 4)
        self.recv("2p2", self.ap, self.bp)
        self.send("2o", self.ap, self.bp, self.to_bm, "on", 4)
        self.recv("2p3", self.ao, self.bp)
        self.send("2o", self.ao, self.bp, self.to_bm, "on", 4)
        self.net.recv((self.tag, "2p01"), self.size(2))
        self.hand(self.bp)
        self.net.recv((self.tag, "2m23"), self.size(2))
        self.hand(self.bm)

    def five(self):
        self.net.recv((self.tag, "2o"), self.size(4))
        self.hand(self.bo)


class Coarse:
    def __init__(self, net, buf, c, y, x, to_row, to_column, sibling):
        self.net, self.buf, self.c, self.y, self.x = net, buf, c, y, x
        self.to_row, self.to_column, self.sibling = to_row, to_column, sibling

    def send(self, key, make, device, size):
        self.net.send(key, lambda: (make(), make(), device), batch=key, total=lambda: size)

    def first(self):
        for device in self.to_row:
            self.send("p1", lambda: self.buf.at[:, self.c, self.y, self.x], device, self.buf.at[:, 0, 0, pl.ds(0, 3)])

    def second(self):
        self.net.recv("p1", self.buf.at[:, 0, 0, pl.ds(0, 3)])
        for device in self.to_column:
            self.send("p2", lambda: self.buf.at[:, self.c, self.y], device, self.buf.at[:, 0, pl.ds(0, 3)])

    def third(self):
        self.net.recv("p2", self.buf.at[:, 0, pl.ds(0, 3)])
        self.send("p3", lambda: self.buf.at[:, self.c], self.sibling, self.buf.at[:, 0])

    def last(self, o):
        self.net.recv("p3", self.buf.at[:, o])


def normed(values, gain):
    floats = values.astype(F32)
    mean = jnp.mean(floats * floats, axis=-1, keepdims=True)
    return (floats * lax.rsqrt(mean + EPS) * gain).astype(BF16)


def kernel(
    tok, g1, gate1, up1, down1, mixg, pool, scale, g2, gate2, up2, down2, out,
    w, pw, xt, xq, n, h1, h2, wd1, wd2, maps, own1, pm, pp, so, sm, sp, ra, rb, a1, hs, hr, mg, ob, sq, rq, base, rx, st, tokv,
    ss, rs, ls,
):
    rep = lax.axis_index("rep")
    fs = lax.axis_index("fs")
    c = lax.axis_index("tp")
    o = 1 - c
    j = lax.div(fs, 16)
    z = rep * 2 + j
    y = lax.rem(lax.div(fs, 4), 4)
    x = lax.rem(fs, 4)
    zp, zo, zm = (lax.rem(z + k, 4) for k in (1, 2, 3))
    yp, yo, ym = (lax.rem(y + k, 4) for k in (1, 2, 3))
    xp, xo, xm = (lax.rem(x + k, 4) for k in (1, 2, 3))

    def dev(z_, y_, x_, c_):
        return (lax.div(z_, 2), lax.rem(z_, 2) * 16 + y_ * 4 + x_, c_)

    sibling = dev(z, y, x, o)
    net = Net(ss, rs, ls, sibling)
    keeper = c == j
    taker = c != j
    zq = lax.rem(z + 1 + 2 * lax.rem(z + c, 2), 4)

    def cols(k):
        return pl.ds(pl.multiple_of(k * UNIT, 128), UNIT)

    def feats(k):
        return pl.ds(pl.multiple_of(k * HALF, 128), HALF)

    def rows(k):
        return pl.ds(pl.multiple_of(k * ROWS, 128), ROWS)

    mats = ((gate1, up1, down1), (gate2, up2, down2), (gate2, up2, down2))
    subs = (lax.div(z, 2), 0, 1)

    own_tok = net.local(tok.at[rows(c), :], xt.at[z, :, feats(c)])
    own_tok.start()
    own_w = [net.slot() for u in range(3)]
    own_p = net.slot()

    def own_pool():
        return pltpu.make_async_copy(pool, pw.at[c, c, y, x], own_p)

    stage_t = net.local(tok, tokv)
    stage_t.start()
    stage_w = [net.slot(), net.slot()]

    @pl.when(taker)
    def _():
        for k in range(2):
            for m in range(3):
                pltpu.make_async_copy(mats[k][m], st.at[k, m], stage_w[k]).start()

    @pl.when(keeper)
    def _():
        for u in range(3):
            for m in range(3):
                pltpu.make_async_copy(mats[u][m].at[:, cols(subs[u])], w.at[u, m, c, y, x], own_w[u]).start()
        own_pool().start()

    own_mg = net.local(mixg, mg.at[0, c])
    own_sc = net.local(scale, mg.at[1, c])
    own_mg.start()
    own_sc.start()

    barrier = pltpu.get_barrier_semaphore()
    friends = [dev(z, y, x_, c) for x_ in (xp, xm, xo)] + [dev(z, y_, x, c) for y_ in (yp, ym, yo)] + [sibling]
    friends += [dev(z_, y, x, k) for z_ in (zp, zm) for k in range(2)]
    for friend in friends:
        pl.semaphore_signal(barrier, inc=1, device_id=friend, device_id_type=MESH)
    pl.semaphore_wait(barrier, len(friends))

    def staged(k):
        @pl.when(taker)
        def _():
            pltpu.make_async_copy(st.at[k], st.at[k], stage_w[k]).wait()

    def exchange(u):
        for ab, z_ in ((0, zp), (1, zm)):
            sub = (lax.div(z_, 2), 0, 1)[u]
            part = pl.ds(16 * ab, 16)
            for m in range(3):
                net.send(
                    ("z", u),
                    lambda m=m, part=part, sub=sub, z_=z_: (
                        st.at[min(u, 1), m, part, cols(sub)],
                        w.at[u, m, o, y, x, part, :],
                        dev(z_, y, x, o),
                    ),
                    cond=taker,
                    batch=("z", u),
                    total=lambda: w.at[u, :, 0, 0, 0],
                )

    def own(u):
        ref = w.at[u, :, c, y, x]

        @pl.when(keeper)
        def _():
            pltpu.make_async_copy(ref, ref, own_w[u]).wait()

        @pl.when(taker)
        def _():
            net.recv(("z", u), ref)

    in_x = (x, xp, xm, xo, dev(z, y, xp, c), dev(z, y, xm, c), dev(z, y, xo, c))
    in_y = (y, yp, ym, yo, dev(z, yp, x, c), dev(z, ym, x, c), dev(z, yo, x, c))
    two, top, low = pl.ds(0, 2), pl.ds(0, 16), pl.ds(16, 16)

    def size_w(k):
        return {
            2: w.at[0, :, 0, two, 0, top],
            4: w.at[0, :, 0, :, 0, top],
            8: w.at[0, :, 0, two, :, top],
            16: w.at[0, :, 0, :, :, top],
            32: w.at[0, :, 0],
        }[k]

    def stream_a(u):
        return Stream(
            net, u, "a", DIRECT and u == 0,
            lambda a, b: w.at[u, :, c, b, a, top, :],
            lambda b: w.at[u, :, c, b, :, top, :],
            size_w, 2, in_x, in_y, sibling,
        )

    def stream_b(u):
        return Stream(
            net, u, "b", DIRECT and u == 0,
            lambda a, b: w.at[u, :, c, a, b, low, :],
            lambda b: w.at[u, :, c, :, b, low, :],
            size_w, 2, in_y, in_x, sibling,
        )

    sa = [stream_a(u) for u in range(3)]
    sb = [stream_b(u) for u in range(3)]
    spool = Coarse(net, pw, c, y, x, (in_x[4], in_x[5], in_x[6]), (in_y[4], in_y[5], in_y[6]), sibling)

    def start(u):
        own(u)
        sa[u].one()
        sb[u].one()
        sa[u].then()
        sb[u].then()

    def handed(u):
        net.recv((u, "d"), w.at[u, :, o])

    def spread_tokens(tag, cond):
        for k in range(2):
            for key, z_ in (("tm", zp), ("tp", zm)):
                net.send(
                    key,
                    lambda k=k, z_=z_: (tokv.at[rows(k), :], xt.at[z, :, feats(c)], dev(z_, y, x, k)),
                    cond=cond, width=2, shift=c, batch=("t4", tag), total=lambda: xt.at[pl.ds(0, 2)],
                )
        net.send("ts", lambda: (tokv.at[rows(o), :], xt.at[z, :, feats(c)], sibling), cond=cond)

    def relay_tokens():
        for key, who, half, to in (("tm", zm, 0, zp), ("tp", zp, 1, zm)):
            net.recv(key, xt.at[who, :, feats(half)], half, 2)
            net.send(
                "to",
                lambda who=who, half=half, to=to: (
                    xt.at[who, :, feats(half)], xt.at[who, :, feats(half)], dev(to, y, x, c)
                ),
                batch="t2", total=lambda: xt.at[0],
            )
        net.recv("tm", xt.at[zm, :, feats(1)], 1, 2)
        net.recv("tp", xt.at[zp, :, feats(0)], 0, 2)

    def gate_up(u, at, count, put):
        for k in range(UNIT // 128):
            part = pl.ds(k * 128, 128)
            wg = w[u, 0, :, :, :, :, part].reshape(D, 128)
            wu = w[u, 1, :, :, :, :, part].reshape(D, 128)
            both = jnp.dot(
                n[pl.ds(at, count), :], jnp.concatenate([wg, wu], axis=1), preferred_element_type=F32
            )
            gate, up = both[:, :128], both[:, 128:]
            put(k * 128, (gate * jax.nn.sigmoid(gate) * up).astype(BF16))

    def put1(at, count):
        def put(k, value):
            h1[pl.ds(at, count), pl.ds(k, 128)] = value

        return put

    def put2(at, count, first):
        def put(k, value):
            h2[pl.ds(at, count), pl.ds(first + k, 128)] = value

        return put

    def turn(u, part, wide, at):
        for k in range(2):
            block = w[u, 2, part, 2 * k : 2 * k + 2].reshape(256, UNIT)
            wide[pl.ds(at, UNIT), pl.ds(pl.multiple_of(part * HALF + 256 * k, 128), 256)] = block.T

    def dot(lhs, rhs):
        return jnp.dot(lhs, rhs, preferred_element_type=F32)

    staged(0)
    exchange(0)
    stage_t.wait()
    staged(1)
    exchange(1)
    spread_tokens(0, taker)
    start(0)
    start(1)
    exchange(2)
    net.send("ps", lambda: (pool, pw.at[c, o, y, x], sibling), cond=taker)
    net.send("pz", lambda: (pool, pw.at[c, j, y, x], dev(zp, y, x, j)), width=2, shift=c)
    own_mg.wait()
    own_sc.wait()
    net.send("mg", lambda: (mixg, mg.at[0, c], sibling), batch="mg", total=lambda: mg.at[:, 0])
    net.send("mg", lambda: (scale, mg.at[1, c], sibling), batch="mg", total=lambda: mg.at[:, 0])

    sa[0].two()
    sb[0].two()
    gain1 = g1[...]
    sa[0].pre()
    sb[0].pre()
    spread_tokens(1, keeper)
    sa[0].three()
    sb[0].three()
    relay_tokens()
    sa[0].four()
    sb[0].four()

    @pl.when(keeper)
    def _():
        own_pool().wait()
        net.recv("ps", pw.at[o, c, y, x])

    @pl.when(taker)
    def _():
        net.recv("pz", pw.at[0, c, y, x], 0, 2)
        net.recv("pz", pw.at[1, c, y, x], 1, 2)

    spool.first()
    start(2)
    own_tok.wait()
    net.recv("ts", xt.at[z, :, feats(o)])
    n[pl.ds(0, ROWS), :] = normed(xt[z], gain1)
    n[pl.ds(ROWS, ROWS), :] = normed(xt[zm], gain1)
    n[pl.ds(2 * ROWS, ROWS), :] = normed(xt[zp], gain1)
    net.recv("to", xt.at[zo])
    n[pl.ds(3 * ROWS, ROWS), :] = normed(xt[zo], gain1)
    sa[0].five()
    sb[0].five()
    turn(0, c, wd1, 0)
    sa[1].two()
    sb[1].two()
    spool.second()
    handed(0)

    gate_up(0, 3 * ROWS, ROWS, put1(3 * ROWS, ROWS))
    turn(0, o, wd1, 0)
    so[...] = dot(h1[pl.ds(3 * ROWS, ROWS), :], wd1[...]).astype(BF16)
    net.send("r0", lambda: (so.at[:, feats(0)], ra.at[0], dev(zp, y, x, c)), batch="r", total=lambda: so)
    net.send("r1", lambda: (so.at[:, feats(1)], ra.at[1], dev(zm, y, x, c)), batch="r", total=lambda: so)
    sa[2].two()
    sb[2].two()
    gate_up(0, ROWS, 2 * ROWS, put1(ROWS, 2 * ROWS))
    sums = dot(h1[pl.ds(ROWS, 2 * ROWS), :], wd1[...])
    sm[:, :HALF] = sums[:ROWS, :HALF].astype(BF16)
    sp[:, HALF:] = sums[ROWS:, HALF:].astype(BF16)
    pm[...] = sums[:ROWS, HALF:]
    pp[...] = sums[ROWS:, :HALF]

    def pass_on(key, buf, k, half, z_):
        net.send(
            f"{key}{half}",
            lambda: (buf.at[:, feats(half)], rb.at[k, :, feats(half)], dev(z_, y, x, c)),
            batch="q", total=lambda: xt.at[two],
        )

    pass_on("qm", sp, 0, 1, zp)
    pass_on("qp", sm, 1, 0, zm)
    sa[1].pre()
    sb[1].pre()
    gate_up(0, 0, ROWS, put1(0, ROWS))
    own1[...] = dot(h1[pl.ds(0, ROWS), :], wd1[...])
    sa[1].three()
    sb[1].three()
    net.recv("r0", ra.at[0])
    sp[:, :HALF] = (pp[...] + ra[0].astype(F32)).astype(BF16)
    net.recv("r1", ra.at[1])
    sm[:, HALF:] = (pm[...] + ra[1].astype(F32)).astype(BF16)
    pass_on("qm", sp, 0, 0, zp)
    pass_on("qp", sm, 1, 1, zm)
    spool.third()
    sa[2].pre()
    sb[2].pre()
    sa[1].four()
    sb[1].four()
    sa[2].three()
    sb[2].three()
    spool.last(o)
    for g in range(4):
        wide = pw[g // 2].reshape(32, 16, 256).astype(F32)
        maps[g] = wide[:, 8 * (g % 2) : 8 * (g % 2) + 8, :].reshape(256, 256).astype(BF16).T
    for key, k, half in (("qm", 0, 1), ("qp", 1, 0), ("qm", 0, 0), ("qp", 1, 1)):
        net.recv(f"{key}{half}", rb.at[k, :, feats(half)])
    block = own1[...] + rb[0].astype(F32) + rb[1].astype(F32)
    a1[...] = (xt[z].astype(F32) + 0.5 * block).astype(BF16)

    net.recv("mg", mg.at[:, o])
    mix_gain = jnp.concatenate([mg[0, 0], mg[0, 1]], axis=1)
    mix_scale = jnp.concatenate([mg[1, 0], mg[1, 1]], axis=1)
    hidden = normed(a1[...], mix_gain)
    hs[...] = hidden
    net.send("h", lambda: (hs.at[pl.ds(112, 16), :], hr, sibling))
    net.recv("h", hr)
    before = jnp.where(c == 1, hr[...].astype(F32), 0.0)
    floats = hs[...].astype(F32)
    longer = jnp.concatenate([before, floats], axis=0)
    positions = c * ROWS + lax.broadcasted_iota(jnp.int32, (ROWS, 256), 0)
    for g in range(4):
        lanes = slice(256 * g, 256 * g + 256)
        total = longer[:, lanes]
        for k in range(g + 1):
            total = total + pltpu.roll(total, 2**k, axis=0)
        counts = jnp.minimum(positions + 1, 2 ** (g + 1)).astype(F32)
        diff = (total[16:] / counts - floats[:, lanes]).astype(BF16)
        mixed = dot(diff, maps[g])
        after = a1[:, lanes].astype(F32) + mixed * mix_scale[:, lanes]
        ob[:, lanes] = after.astype(BF16)

    net.send("a", lambda: (ob, xq, dev(zq, y, x, c)))
    gain2 = g2[...]
    n[pl.ds(0, ROWS), :] = normed(ob[...], gain2)
    sa[1].five()
    sb[1].five()
    sa[2].four()
    sb[2].four()
    turn(1, c, wd2, 0)
    handed(1)
    gate_up(1, 0, ROWS, put2(0, ROWS, 0))
    turn(1, o, wd2, 0)
    sa[2].five()
    sb[2].five()
    turn(2, c, wd2, UNIT)
    net.recv("a", xq)
    n[pl.ds(ROWS, ROWS), :] = normed(xq[...], gain2)
    gate_up(1, ROWS, ROWS, put2(ROWS, ROWS, 0))
    handed(2)
    gate_up(2, ROWS, ROWS, put2(ROWS, ROWS, UNIT))
    turn(2, o, wd2, UNIT)
    sq[...] = dot(h2[pl.ds(ROWS, ROWS), :], wd2[...]).astype(BF16)
    for k in range(2):
        net.send(
            "b",
            lambda k=k: (sq.at[:, feats(k)], rq.at[c], dev(zq, y, x, k)),
            width=2, shift=c, batch="b", total=lambda: sq,
        )
    gate_up(2, 0, ROWS, put2(0, ROWS, UNIT))
    base[...] = ob[...].astype(F32) + 0.5 * dot(h2[pl.ds(0, ROWS), :], wd2[...])
    net.send("f", lambda: (base.at[:, feats(o)], rx, sibling))
    net.recv("b", rq.at[c], c, 2)
    out[rows(c), :] = (base[:, feats(c)] + 0.5 * rq[c].astype(F32)).astype(BF16)
    net.recv("f", rx)
    net.recv("b", rq.at[o], o, 2)
    out[rows(o), :] = (rx[...] + 0.5 * rq[o].astype(F32)).astype(BF16)
    net.finish()


def local(tok, g1, gate1, up1, down1, mixg, pool, scale, g2, gate2, up2, down2):
    hbm = pl.BlockSpec(memory_space=pl.ANY)
    vmem = pl.BlockSpec(memory_space=pltpu.VMEM)
    result = pl.pallas_call(
        kernel,
        out_shape=jax.ShapeDtypeStruct((256, HALF), BF16),
        in_specs=[hbm, vmem, hbm, hbm, hbm, hbm, hbm, hbm, vmem, hbm, hbm, hbm],
        out_specs=vmem,
        scratch_shapes=[
            pltpu.VMEM((3, 3, 2, 4, 4, 32, UNIT), BF16),
            pltpu.VMEM((2, 2, 4, 4, 16, 256), BF16),
            pltpu.VMEM((4, ROWS, D), BF16),
            pltpu.VMEM((ROWS, D), BF16),
            pltpu.VMEM((4 * ROWS, D), BF16),
            pltpu.VMEM((4 * ROWS, UNIT), BF16),
            pltpu.VMEM((2 * ROWS, 2 * UNIT), BF16),
            pltpu.VMEM((UNIT, D), BF16),
            pltpu.VMEM((2 * UNIT, D), BF16),
            pltpu.VMEM((4, 256, 256), BF16),
            pltpu.VMEM((ROWS, D), F32),
            pltpu.VMEM((ROWS, HALF), F32),
            pltpu.VMEM((ROWS, HALF), F32),
            pltpu.VMEM((ROWS, D), BF16),
            pltpu.VMEM((ROWS, D), BF16),
            pltpu.VMEM((ROWS, D), BF16),
            pltpu.VMEM((2, ROWS, HALF), BF16),
            pltpu.VMEM((2, ROWS, D), BF16),
            pltpu.VMEM((ROWS, D), BF16),
            pltpu.VMEM((ROWS, D), BF16),
            pltpu.VMEM((16, D), BF16),
            pltpu.VMEM((2, 2, 1, HALF), F32),
            pltpu.VMEM((ROWS, D), BF16),
            pltpu.VMEM((ROWS, D), BF16),
            pltpu.VMEM((2, ROWS, HALF), BF16),
            pltpu.VMEM((ROWS, D), F32),
            pltpu.VMEM((ROWS, HALF), F32),
            pltpu.VMEM((2, 3, 32, 1280), BF16),
            pltpu.VMEM((256, HALF), BF16),
            pltpu.SemaphoreType.DMA((N_SEND,)),
            pltpu.SemaphoreType.DMA((N_RECV,)),
            pltpu.SemaphoreType.DMA((N_LOCAL,)),
        ],
        compiler_params=pltpu.CompilerParams(collective_id=0, has_side_effects=True, vmem_limit_bytes=67043328),
    )(
        tok.reshape(256, HALF), g1.reshape(1, D), gate1, up1, down1.T, mixg.reshape(1, HALF),
        pool.transpose(0, 2, 1).reshape(16, 256), scale.reshape(1, HALF), g2.reshape(1, D), gate2, up2, down2.T,
    )
    return result.reshape(1, 256, HALF)


def solution(mesh):
    placed = (
        P(("rep", "fs"), None, "tp"),
        P(),
        P("fs", "tp"),
        P("fs", "tp"),
        P("tp", "fs"),
        P("tp"),
        P("tp", None, "fs"),
        P("tp"),
        P(),
        P("fs", "tp"),
        P("fs", "tp"),
        P("tp", "fs"),
    )
    return jax.shard_map(
        local, mesh=mesh, in_specs=placed, out_specs=P(("rep", "fs"), None, "tp"), check_vma=False
    )
```

```python
import jax
import jax.numpy as jnp
from jax import lax
from jax.experimental import pallas as pl
from jax.experimental.pallas import tpu as pltpu
from jax.sharding import PartitionSpec as P

MESH = pl.DeviceIdType.MESH
BF16 = jnp.bfloat16
F32 = jnp.float32
EPS = 1e-06
D = 1024
HALF = 512
ROWS = 128
UNIT = 640
DIRECT = True
N_SEND = 36
N_RECV = 92
N_LOCAL = 10


class Net:
    def __init__(self, ss, rs, ls, here):
        self.ss, self.rs, self.ls, self.here = ss, rs, ls, here
        self.names = {}
        self.batches = {}
        self.locals = 0
        self.sends = 0
        self.pending = []

    def name(self, key, width=1):
        if key not in self.names:
            self.names[key] = sum(w for _, w in self.names.values()), width
        return self.names[key][0]

    def send(self, key, make, cond=None, width=1, shift=None, batch=None, total=None):
        base = self.name(key, width)
        first = batch is None or batch not in self.batches
        if first:
            slot = self.sends
            self.sends += 1
            if batch is not None:
                self.batches[batch] = slot
        else:
            slot = self.batches[batch]

        def copy(src, dst, device):
            where = base if shift is None else base + shift
            return pltpu.make_async_remote_copy(
                src, dst, self.ss.at[slot], self.rs.at[where], device_id=device, device_id_type=MESH
            )

        def end():
            ref = make()[0] if total is None else total()
            copy(ref, ref, self.here).wait_send()

        if cond is None:
            copy(*make()).start()
        else:
            pl.when(cond)(lambda: copy(*make()).start())
        if first:
            self.pending.append(end if cond is None else lambda: pl.when(cond)(end))

    def recv(self, key, ref, offset=0, width=1):
        where = self.name(key, width) + offset
        pltpu.make_async_remote_copy(
            ref, ref, self.ss.at[0], self.rs.at[where], device_id=self.here, device_id_type=MESH
        ).wait_recv()

    def slot(self):
        self.locals += 1
        return self.ls.at[self.locals - 1]

    def local(self, src, dst):
        return pltpu.make_async_copy(src, dst, self.slot())

    def finish(self):
        for end in self.pending:
            end()
        assert self.sends == N_SEND and self.locals == N_LOCAL
        assert sum(w for _, w in self.names.values()) == N_RECV


class Stream:
    def __init__(self, net, unit, tag, direct, piece, group, size, many, first, second, sibling):
        self.net, self.unit, self.tag, self.direct = net, unit, (unit, tag), direct
        self.piece, self.group, self.size, self.many = piece, group, size, many
        self.a, self.ap, self.am, self.ao, self.to_ap, self.to_am, self.to_ao = first
        self.b, self.bp, self.bm, self.bo, self.to_bp, self.to_bm, self.to_bo = second
        self.sibling = sibling

    def send(self, what, a, b, device, kind, count):
        self.net.send(
            (self.tag, what),
            lambda: (self.piece(a, b), self.piece(a, b), device),
            batch=(self.unit, kind),
            total=lambda: self.size(count * self.many),
        )

    def recv(self, what, a, b):
        self.net.recv((self.tag, what), self.piece(a, b))

    def both(self, k, a):
        late_m, late_p = ("2m23" if k >= 2 else f"2m{k}"), ("2p01" if k < 2 else f"2p{k}")
        self.send(late_m, a, self.b, self.to_bp, "both", 8)
        self.send(late_p, a, self.b, self.to_bm, "both", 8)

    def hand(self, b):
        self.net.send(
            (self.unit, "d"),
            lambda: (self.group(b), self.group(b), self.sibling),
            batch=(self.unit, "hand"),
            total=lambda: self.size(16 * self.many),
        )

    def one(self):
        self.send("1m", self.a, self.b, self.to_ap, "ring", 2)
        self.send("1p", self.a, self.b, self.to_am, "ring", 2)
        if self.direct:
            self.send("1o", self.a, self.b, self.to_ao, "far", 1)

    def then(self):
        self.both(0, self.a)

    def two(self):
        self.recv("1p", self.ap, self.b)
        if not self.direct:
            self.send("1o", self.ap, self.b, self.to_am, "far", 1)
        self.both(2, self.ap)
        self.recv("1m", self.am, self.b)
        self.both(1, self.am)

    def three(self):
        self.recv("1o", self.ao, self.b)
        self.both(3, self.ao)
        self.hand(self.b)

    def pre(self):
        self.recv("2m0", self.a, self.bm)
        self.send("2o", self.a, self.bm, self.to_bp, "on", 4)

    def four(self):
        self.recv("2m1", self.am, self.bm)
        self.send("2o", self.am, self.bm, self.to_bp, "on", 4)
        self.recv("2p2", self.ap, self.bp)
        self.send("2o", self.ap, self.bp, self.to_bm, "on", 4)
        self.recv("2p3", self.ao, self.bp)
        self.send("2o", self.ao, self.bp, self.to_bm, "on", 4)
        self.net.recv((self.tag, "2p01"), self.size(2))
        self.hand(self.bp)
        self.net.recv((self.tag, "2m23"), self.size(2))
        self.hand(self.bm)

    def five(self):
        self.net.recv((self.tag, "2o"), self.size(4))
        self.hand(self.bo)


class Coarse:
    def __init__(self, net, buf, c, y, x, to_row, column, sibling):
        self.net, self.buf, self.c, self.y, self.x = net, buf, c, y, x
        self.to_row, self.sibling = to_row, sibling
        _, self.yp, self.ym, self.yo, self.to_yp, self.to_ym, _ = column

    def send(self, key, make, device, batch, total):
        self.net.send(key, lambda: (make(), make(), device), batch=batch, total=lambda: total)

    def row(self, y):
        return self.buf.at[:, self.c, y]

    def part(self, y, k):
        return self.buf.at[:, self.c, y, pl.ds(2 * k, 2)]

    def first(self):
        for device in self.to_row:
            self.send(
                "p1", lambda: self.buf.at[:, self.c, self.y, self.x], device, "p1", self.buf.at[:, 0, 0, pl.ds(0, 3)]
            )

    def second(self):
        self.net.recv("p1", self.buf.at[:, 0, 0, pl.ds(0, 3)])
        for key, device in (("p2m", self.to_yp), ("p2p", self.to_ym)):
            self.send(key, lambda: self.row(self.y), device, "p2", self.buf.at[:, 0, pl.ds(0, 2)])

    def third(self):
        for key, y, k, device in (("p2m", self.ym, 0, self.to_yp), ("p2p", self.yp, 1, self.to_ym)):
            self.net.recv(key, self.row(y))
            self.send("p3", lambda y=y, k=k: self.part(y, k), device, "p3", self.row(0))

    def fourth(self):
        self.net.recv("p3", self.row(self.yo))
        self.send("p4", lambda: self.buf.at[:, self.c], self.sibling, "p4", self.buf.at[:, 0])

    def last(self, o):
        self.net.recv("p4", self.buf.at[:, o])


def normed(values, gain):
    floats = values.astype(F32)
    mean = jnp.mean(floats * floats, axis=-1, keepdims=True)
    return (floats * lax.rsqrt(mean + EPS) * gain).astype(BF16)


def kernel(
    tok, g1, gate1, up1, down1, mixg, pool, scale, g2, gate2, up2, down2, out,
    w, pw, xt, xq, n, h1, h2, wd1, wd2, maps, own1, pm, pp, so, sm, sp, ra, rb, a1, hs, hr, mg, ob, sq, rq, base, rx, st, tokv,
    ss, rs, ls,
):
    rep = lax.axis_index("rep")
    fs = lax.axis_index("fs")
    c = lax.axis_index("tp")
    o = 1 - c
    j = lax.div(fs, 16)
    z = rep * 2 + j
    y = lax.rem(lax.div(fs, 4), 4)
    x = lax.rem(fs, 4)
    zp, zo, zm = (lax.rem(z + k, 4) for k in (1, 2, 3))
    yp, yo, ym = (lax.rem(y + k, 4) for k in (1, 2, 3))
    xp, xo, xm = (lax.rem(x + k, 4) for k in (1, 2, 3))

    def dev(z_, y_, x_, c_):
        return (lax.div(z_, 2), lax.rem(z_, 2) * 16 + y_ * 4 + x_, c_)

    sibling = dev(z, y, x, o)
    net = Net(ss, rs, ls, sibling)
    keeper = c == j
    taker = c != j
    zq = lax.rem(z + 1 + 2 * lax.rem(z + c, 2), 4)

    def cols(k):
        return pl.ds(pl.multiple_of(k * UNIT, 128), UNIT)

    def feats(k):
        return pl.ds(pl.multiple_of(k * HALF, 128), HALF)

    def rows(k):
        return pl.ds(pl.multiple_of(k * ROWS, 128), ROWS)

    mats = ((gate1, up1, down1), (gate2, up2, down2), (gate2, up2, down2))
    subs = (lax.div(z, 2), 0, 1)

    own_tok = net.local(tok.at[rows(c), :], xt.at[z, :, feats(c)])
    own_tok.start()
    own_w = [net.slot() for u in range(3)]
    own_p = net.slot()

    def own_pool():
        return pltpu.make_async_copy(pool, pw.at[c, c, y, x], own_p)

    stage_t = net.local(tok, tokv)
    stage_t.start()
    stage_w = [net.slot(), net.slot()]

    @pl.when(taker)
    def _():
        for k in range(2):
            for m in range(3):
                pltpu.make_async_copy(mats[k][m], st.at[k, m], stage_w[k]).start()

    @pl.when(keeper)
    def _():
        for u in range(3):
            for m in range(3):
                pltpu.make_async_copy(mats[u][m].at[:, cols(subs[u])], w.at[u, m, c, y, x], own_w[u]).start()
        own_pool().start()

    own_mg = net.local(mixg, mg.at[0, c])
    own_sc = net.local(scale, mg.at[1, c])
    own_mg.start()
    own_sc.start()

    barrier = pltpu.get_barrier_semaphore()
    friends = [dev(z, y, x_, c) for x_ in (xp, xm, xo)] + [dev(z, y_, x, c) for y_ in (yp, ym, yo)] + [sibling]
    friends += [dev(z_, y, x, k) for z_ in (zp, zm) for k in range(2)]
    for friend in friends:
        pl.semaphore_signal(barrier, inc=1, device_id=friend, device_id_type=MESH)
    pl.semaphore_wait(barrier, len(friends))

    def staged(k):
        @pl.when(taker)
        def _():
            pltpu.make_async_copy(st.at[k], st.at[k], stage_w[k]).wait()

    def exchange(u):
        for ab, z_ in ((0, zp), (1, zm)):
            sub = (lax.div(z_, 2), 0, 1)[u]
            part = pl.ds(16 * ab, 16)
            for m in range(3):
                net.send(
                    ("z", u),
                    lambda m=m, part=part, sub=sub, z_=z_: (
                        st.at[min(u, 1), m, part, cols(sub)],
                        w.at[u, m, o, y, x, part, :],
                        dev(z_, y, x, o),
                    ),
                    cond=taker,
                    batch=("z", u),
                    total=lambda: w.at[u, :, 0, 0, 0],
                )

    def own(u):
        ref = w.at[u, :, c, y, x]

        @pl.when(keeper)
        def _():
            pltpu.make_async_copy(ref, ref, own_w[u]).wait()

        @pl.when(taker)
        def _():
            net.recv(("z", u), ref)

    in_x = (x, xp, xm, xo, dev(z, y, xp, c), dev(z, y, xm, c), dev(z, y, xo, c))
    in_y = (y, yp, ym, yo, dev(z, yp, x, c), dev(z, ym, x, c), dev(z, yo, x, c))
    two, top, low = pl.ds(0, 2), pl.ds(0, 16), pl.ds(16, 16)

    def size_w(k):
        return {
            2: w.at[0, :, 0, two, 0, top],
            4: w.at[0, :, 0, :, 0, top],
            8: w.at[0, :, 0, two, :, top],
            16: w.at[0, :, 0, :, :, top],
            32: w.at[0, :, 0],
        }[k]

    def stream_a(u):
        return Stream(
            net, u, "a", DIRECT and u == 0,
            lambda a, b: w.at[u, :, c, b, a, top, :],
            lambda b: w.at[u, :, c, b, :, top, :],
            size_w, 2, in_x, in_y, sibling,
        )

    def stream_b(u):
        return Stream(
            net, u, "b", DIRECT and u == 0,
            lambda a, b: w.at[u, :, c, a, b, low, :],
            lambda b: w.at[u, :, c, :, b, low, :],
            size_w, 2, in_y, in_x, sibling,
        )

    sa = [stream_a(u) for u in range(3)]
    sb = [stream_b(u) for u in range(3)]
    spool = Coarse(net, pw, c, y, x, (in_x[4], in_x[5], in_x[6]), in_y, sibling)

    def start(u):
        own(u)
        sa[u].one()
        sb[u].one()
        sa[u].then()
        sb[u].then()

    def handed(u):
        net.recv((u, "d"), w.at[u, :, o])

    def spread_tokens(tag, cond):
        for k in range(2):
            for key, z_ in (("tm", zp), ("tp", zm)):
                net.send(
                    key,
                    lambda k=k, z_=z_: (tokv.at[rows(k), :], xt.at[z, :, feats(c)], dev(z_, y, x, k)),
                    cond=cond, width=2, shift=c, batch=("t4", tag), total=lambda: xt.at[pl.ds(0, 2)],
                )
        net.send("ts", lambda: (tokv.at[rows(o), :], xt.at[z, :, feats(c)], sibling), cond=cond)

    def relay_tokens():
        for key, who, half, to in (("tm", zm, 0, zp), ("tp", zp, 1, zm)):
            net.recv(key, xt.at[who, :, feats(half)], half, 2)
            net.send(
                "to",
                lambda who=who, half=half, to=to: (
                    xt.at[who, :, feats(half)], xt.at[who, :, feats(half)], dev(to, y, x, c)
                ),
                batch="t2", total=lambda: xt.at[0],
            )
        net.recv("tm", xt.at[zm, :, feats(1)], 1, 2)
        net.recv("tp", xt.at[zp, :, feats(0)], 0, 2)

    def gate_up(u, at, count, put):
        for k in range(UNIT // 128):
            part = pl.ds(k * 128, 128)
            wg = w[u, 0, :, :, :, :, part].reshape(D, 128)
            wu = w[u, 1, :, :, :, :, part].reshape(D, 128)
            both = jnp.dot(
                n[pl.ds(at, count), :], jnp.concatenate([wg, wu], axis=1), preferred_element_type=F32
            )
            gate, up = both[:, :128], both[:, 128:]
            put(k * 128, (gate * jax.nn.sigmoid(gate) * up).astype(BF16))

    def put1(at, count):
        def put(k, value):
            h1[pl.ds(at, count), pl.ds(k, 128)] = value

        return put

    def put2(at, count, first):
        def put(k, value):
            h2[pl.ds(at, count), pl.ds(first + k, 128)] = value

        return put

    def turn(u, part, wide, at):
        for k in range(2):
            block = w[u, 2, part, 2 * k : 2 * k + 2].reshape(256, UNIT)
            wide[pl.ds(at, UNIT), pl.ds(pl.multiple_of(part * HALF + 256 * k, 128), 256)] = block.T

    def dot(lhs, rhs):
        return jnp.dot(lhs, rhs, preferred_element_type=F32)

    staged(0)
    exchange(0)
    stage_t.wait()
    staged(1)
    exchange(1)
    spread_tokens(0, taker)
    start(0)
    start(1)
    exchange(2)
    net.send("ps", lambda: (pool, pw.at[c, o, y, x], sibling), cond=taker)
    net.send("pz", lambda: (pool, pw.at[c, j, y, x], dev(zp, y, x, j)), width=2, shift=c)
    own_mg.wait()
    own_sc.wait()
    net.send("mg", lambda: (mixg, mg.at[0, c], sibling), batch="mg", total=lambda: mg.at[:, 0])
    net.send("mg", lambda: (scale, mg.at[1, c], sibling), batch="mg", total=lambda: mg.at[:, 0])

    sa[0].two()
    sb[0].two()
    gain1 = g1[...]
    sa[0].pre()
    sb[0].pre()
    spread_tokens(1, keeper)
    sa[0].three()
    sb[0].three()
    relay_tokens()
    sa[0].four()
    sb[0].four()

    @pl.when(keeper)
    def _():
        own_pool().wait()
        net.recv("ps", pw.at[o, c, y, x])

    @pl.when(taker)
    def _():
        net.recv("pz", pw.at[0, c, y, x], 0, 2)
        net.recv("pz", pw.at[1, c, y, x], 1, 2)

    spool.first()
    start(2)
    own_tok.wait()
    net.recv("ts", xt.at[z, :, feats(o)])
    n[pl.ds(0, ROWS), :] = normed(xt[z], gain1)
    n[pl.ds(ROWS, ROWS), :] = normed(xt[zm], gain1)
    n[pl.ds(2 * ROWS, ROWS), :] = normed(xt[zp], gain1)
    net.recv("to", xt.at[zo])
    n[pl.ds(3 * ROWS, ROWS), :] = normed(xt[zo], gain1)
    sa[0].five()
    sb[0].five()
    turn(0, c, wd1, 0)
    sa[1].two()
    sb[1].two()
    spool.second()
    handed(0)

    gate_up(0, 3 * ROWS, ROWS, put1(3 * ROWS, ROWS))
    turn(0, o, wd1, 0)
    so[...] = dot(h1[pl.ds(3 * ROWS, ROWS), :], wd1[...]).astype(BF16)
    net.send("r0", lambda: (so.at[:, feats(0)], ra.at[0], dev(zp, y, x, c)), batch="r", total=lambda: so)
    net.send("r1", lambda: (so.at[:, feats(1)], ra.at[1], dev(zm, y, x, c)), batch="r", total=lambda: so)
    sa[2].two()
    sb[2].two()
    gate_up(0, ROWS, 2 * ROWS, put1(ROWS, 2 * ROWS))
    sums = dot(h1[pl.ds(ROWS, 2 * ROWS), :], wd1[...])
    sm[:, :HALF] = sums[:ROWS, :HALF].astype(BF16)
    sp[:, HALF:] = sums[ROWS:, HALF:].astype(BF16)
    pm[...] = sums[:ROWS, HALF:]
    pp[...] = sums[ROWS:, :HALF]

    def pass_on(key, buf, k, half, z_):
        net.send(
            f"{key}{half}",
            lambda: (buf.at[:, feats(half)], rb.at[k, :, feats(half)], dev(z_, y, x, c)),
            batch="q", total=lambda: xt.at[two],
        )

    pass_on("qm", sp, 0, 1, zp)
    pass_on("qp", sm, 1, 0, zm)
    spool.third()
    sa[1].pre()
    sb[1].pre()
    gate_up(0, 0, ROWS, put1(0, ROWS))
    own1[...] = dot(h1[pl.ds(0, ROWS), :], wd1[...])
    sa[1].three()
    sb[1].three()
    net.recv("r0", ra.at[0])
    sp[:, :HALF] = (pp[...] + ra[0].astype(F32)).astype(BF16)
    net.recv("r1", ra.at[1])
    sm[:, HALF:] = (pm[...] + ra[1].astype(F32)).astype(BF16)
    pass_on("qm", sp, 0, 0, zp)
    pass_on("qp", sm, 1, 1, zm)
    sa[2].three()
    sb[2].three()
    sa[2].pre()
    sb[2].pre()
    spool.fourth()
    sa[1].four()
    sb[1].four()
    spool.last(o)
    for g in range(4):
        wide = pw[g // 2].reshape(32, 16, 256).astype(F32)
        maps[g] = wide[:, 8 * (g % 2) : 8 * (g % 2) + 8, :].reshape(256, 256).astype(BF16).T
    for key, k, half in (("qm", 0, 1), ("qp", 1, 0), ("qm", 0, 0), ("qp", 1, 1)):
        net.recv(f"{key}{half}", rb.at[k, :, feats(half)])
    block = own1[...] + rb[0].astype(F32) + rb[1].astype(F32)
    a1[...] = (xt[z].astype(F32) + 0.5 * block).astype(BF16)

    net.recv("mg", mg.at[:, o])
    mix_gain = jnp.concatenate([mg[0, 0], mg[0, 1]], axis=1)
    mix_scale = jnp.concatenate([mg[1, 0], mg[1, 1]], axis=1)
    hidden = normed(a1[...], mix_gain)
    hs[...] = hidden
    net.send("h", lambda: (hs.at[pl.ds(112, 16), :], hr, sibling))
    net.recv("h", hr)
    before = jnp.where(c == 1, hr[...].astype(F32), 0.0)
    floats = hs[...].astype(F32)
    longer = jnp.concatenate([before, floats], axis=0)
    positions = c * ROWS + lax.broadcasted_iota(jnp.int32, (ROWS, 256), 0)
    for g in range(4):
        lanes = slice(256 * g, 256 * g + 256)
        total = longer[:, lanes]
        for k in range(g + 1):
            total = total + pltpu.roll(total, 2**k, axis=0)
        counts = jnp.minimum(positions + 1, 2 ** (g + 1)).astype(F32)
        diff = (total[16:] / counts - floats[:, lanes]).astype(BF16)
        mixed = dot(diff, maps[g])
        after = a1[:, lanes].astype(F32) + mixed * mix_scale[:, lanes]
        ob[:, lanes] = after.astype(BF16)

    net.send("a", lambda: (ob, xq, dev(zq, y, x, c)))
    gain2 = g2[...]
    n[pl.ds(0, ROWS), :] = normed(ob[...], gain2)
    sa[1].five()
    sb[1].five()
    sa[2].four()
    sb[2].four()
    turn(1, c, wd2, 0)
    handed(1)
    gate_up(1, 0, ROWS, put2(0, ROWS, 0))
    turn(1, o, wd2, 0)
    sa[2].five()
    sb[2].five()
    turn(2, c, wd2, UNIT)
    net.recv("a", xq)
    n[pl.ds(ROWS, ROWS), :] = normed(xq[...], gain2)
    gate_up(1, ROWS, ROWS, put2(ROWS, ROWS, 0))
    handed(2)
    gate_up(2, ROWS, ROWS, put2(ROWS, ROWS, UNIT))
    turn(2, o, wd2, UNIT)
    sq[...] = dot(h2[pl.ds(ROWS, ROWS), :], wd2[...]).astype(BF16)
    for k in range(2):
        net.send(
            "b",
            lambda k=k: (sq.at[:, feats(k)], rq.at[c], dev(zq, y, x, k)),
            width=2, shift=c, batch="b", total=lambda: sq,
        )
    gate_up(2, 0, ROWS, put2(0, ROWS, UNIT))
    base[...] = ob[...].astype(F32) + 0.5 * dot(h2[pl.ds(0, ROWS), :], wd2[...])
    net.send("f", lambda: (base.at[:, feats(o)], rx, sibling))
    net.recv("b", rq.at[c], c, 2)
    out[rows(c), :] = (base[:, feats(c)] + 0.5 * rq[c].astype(F32)).astype(BF16)
    net.recv("f", rx)
    net.recv("b", rq.at[o], o, 2)
    out[rows(o), :] = (rx[...] + 0.5 * rq[o].astype(F32)).astype(BF16)
    net.finish()


def local(tok, g1, gate1, up1, down1, mixg, pool, scale, g2, gate2, up2, down2):
    hbm = pl.BlockSpec(memory_space=pl.ANY)
    vmem = pl.BlockSpec(memory_space=pltpu.VMEM)
    result = pl.pallas_call(
        kernel,
        out_shape=pltpu.VMEM((256, HALF), BF16),
        in_specs=[hbm, vmem, hbm, hbm, hbm, hbm, hbm, hbm, vmem, hbm, hbm, hbm],
        out_specs=vmem,
        scratch_shapes=[
            pltpu.VMEM((3, 3, 2, 4, 4, 32, UNIT), BF16),
            pltpu.VMEM((2, 2, 4, 4, 16, 256), BF16),
            pltpu.VMEM((4, ROWS, D), BF16),
            pltpu.VMEM((ROWS, D), BF16),
            pltpu.VMEM((4 * ROWS, D), BF16),
            pltpu.VMEM((4 * ROWS, UNIT), BF16),
            pltpu.VMEM((2 * ROWS, 2 * UNIT), BF16),
            pltpu.VMEM((UNIT, D), BF16),
            pltpu.VMEM((2 * UNIT, D), BF16),
            pltpu.VMEM((4, 256, 256), BF16),
            pltpu.VMEM((ROWS, D), F32),
            pltpu.VMEM((ROWS, HALF), F32),
            pltpu.VMEM((ROWS, HALF), F32),
            pltpu.VMEM((ROWS, D), BF16),
            pltpu.VMEM((ROWS, D), BF16),
            pltpu.VMEM((ROWS, D), BF16),
            pltpu.VMEM((2, ROWS, HALF), BF16),
            pltpu.VMEM((2, ROWS, D), BF16),
            pltpu.VMEM((ROWS, D), BF16),
            pltpu.VMEM((ROWS, D), BF16),
            pltpu.VMEM((16, D), BF16),
            pltpu.VMEM((2, 2, 1, HALF), F32),
            pltpu.VMEM((ROWS, D), BF16),
            pltpu.VMEM((ROWS, D), BF16),
            pltpu.VMEM((2, ROWS, HALF), BF16),
            pltpu.VMEM((ROWS, D), F32),
            pltpu.VMEM((ROWS, HALF), F32),
            pltpu.VMEM((2, 3, 32, 1280), BF16),
            pltpu.VMEM((256, HALF), BF16),
            pltpu.SemaphoreType.DMA((N_SEND,)),
            pltpu.SemaphoreType.DMA((N_RECV,)),
            pltpu.SemaphoreType.DMA((N_LOCAL,)),
        ],
        compiler_params=pltpu.CompilerParams(collective_id=0, has_side_effects=True, vmem_limit_bytes=52 * 2**20),
    )(
        *(
            pltpu.with_memory_space_constraint(value, pltpu.HBM)
            for value in (
                tok.reshape(256, HALF), g1.reshape(1, D), gate1, up1, down1.T, mixg.reshape(1, HALF),
                pool.transpose(0, 2, 1).reshape(16, 256), scale.reshape(1, HALF), g2.reshape(1, D), gate2, up2, down2.T,
            )
        )
    )
    return result.reshape(1, 256, HALF)


def solution(mesh):
    placed = (
        P(("rep", "fs"), None, "tp"),
        P(),
        P("fs", "tp"),
        P("fs", "tp"),
        P("tp", "fs"),
        P("tp"),
        P("tp", None, "fs"),
        P("tp"),
        P(),
        P("fs", "tp"),
        P("fs", "tp"),
        P("tp", "fs"),
    )
    return jax.shard_map(
        local, mesh=mesh, in_specs=placed, out_specs=P(("rep", "fs"), None, "tp"), check_vma=False
    )
```

```python
import jax
import jax.numpy as jnp
from jax import lax
from jax.experimental import pallas as pl
from jax.experimental.pallas import tpu as pltpu
from jax.sharding import PartitionSpec as P

MESH = pl.DeviceIdType.MESH
BF16 = jnp.bfloat16
F32 = jnp.float32
EPS = 1e-06
D = 1024
HALF = 512
ROWS = 128
UNIT = 640
DIRECT = True
N_SEND = 36
N_RECV = 92
N_LOCAL = 10


class Net:
    def __init__(self, ss, rs, ls, here):
        self.ss, self.rs, self.ls, self.here = ss, rs, ls, here
        self.names = {}
        self.batches = {}
        self.locals = 0
        self.sends = 0
        self.pending = []

    def name(self, key, width=1):
        if key not in self.names:
            self.names[key] = sum(w for _, w in self.names.values()), width
        return self.names[key][0]

    def send(self, key, make, cond=None, width=1, shift=None, batch=None, total=None):
        base = self.name(key, width)
        first = batch is None or batch not in self.batches
        if first:
            slot = self.sends
            self.sends += 1
            if batch is not None:
                self.batches[batch] = slot
        else:
            slot = self.batches[batch]

        def copy(src, dst, device):
            where = base if shift is None else base + shift
            return pltpu.make_async_remote_copy(
                src, dst, self.ss.at[slot], self.rs.at[where], device_id=device, device_id_type=MESH
            )

        def end():
            ref = make()[0] if total is None else total()
            copy(ref, ref, self.here).wait_send()

        if cond is None:
            copy(*make()).start()
        else:
            pl.when(cond)(lambda: copy(*make()).start())
        if first:
            self.pending.append(end if cond is None else lambda: pl.when(cond)(end))

    def recv(self, key, ref, offset=0, width=1):
        where = self.name(key, width) + offset
        pltpu.make_async_remote_copy(
            ref, ref, self.ss.at[0], self.rs.at[where], device_id=self.here, device_id_type=MESH
        ).wait_recv()

    def slot(self):
        self.locals += 1
        return self.ls.at[self.locals - 1]

    def local(self, src, dst):
        return pltpu.make_async_copy(src, dst, self.slot())

    def finish(self):
        for end in self.pending:
            end()
        assert self.sends == N_SEND and self.locals == N_LOCAL
        assert sum(w for _, w in self.names.values()) == N_RECV


class Stream:
    def __init__(self, net, unit, tag, direct, piece, group, size, many, first, second, sibling):
        self.net, self.unit, self.tag, self.direct = net, unit, (unit, tag), direct
        self.piece, self.group, self.size, self.many = piece, group, size, many
        self.a, self.ap, self.am, self.ao, self.to_ap, self.to_am, self.to_ao = first
        self.b, self.bp, self.bm, self.bo, self.to_bp, self.to_bm, self.to_bo = second
        self.sibling = sibling
        self.flip = unit == 2

    def send(self, what, a, b, device, kind, count):
        self.net.send(
            (self.tag, what),
            lambda: (self.piece(a, b), self.piece(a, b), device),
            batch=(self.unit, kind),
            total=lambda: self.size(count * self.many),
        )

    def recv(self, what, a, b):
        self.net.recv((self.tag, what), self.piece(a, b))

    def both(self, k, a):
        late_m, late_p = ("2m23" if k >= 2 else f"2m{k}"), ("2p01" if k < 2 else f"2p{k}")
        self.send(late_m, a, self.b, self.to_bp, "both", 8)
        self.send(late_p, a, self.b, self.to_bm, "both", 8)

    def hand(self, b):
        self.net.send(
            (self.unit, "d"),
            lambda: (self.group(b), self.group(b), self.sibling),
            batch=(self.unit, "hand"),
            total=lambda: self.size(16 * self.many),
        )

    def one(self):
        self.send("1m", self.a, self.b, self.to_ap, "ring", 2)
        self.send("1p", self.a, self.b, self.to_am, "ring", 2)
        if self.direct:
            self.send("1o", self.a, self.b, self.to_ao, "far", 1)

    def then(self):
        self.both(0, self.a)

    def two(self):
        for key, k, a, to in (("1p", 2, self.ap, self.to_am), ("1m", 1, self.am, self.to_ap))[:: -1 if self.flip else 1]:
            self.recv(key, a, self.b)
            if key == ("1m" if self.flip else "1p") and not self.direct:
                self.send("1o", a, self.b, to, "far", 1)
            self.both(k, a)

    def three(self):
        self.recv("1o", self.ao, self.b)
        self.both(3, self.ao)
        self.hand(self.b)

    def pre(self):
        self.recv("2m0", self.a, self.bm)
        self.send("2o", self.a, self.bm, self.to_bp, "on", 4)

    def four(self):
        self.recv("2m1", self.am, self.bm)
        self.send("2o", self.am, self.bm, self.to_bp, "on", 4)
        self.recv("2p2", self.ap, self.bp)
        self.send("2o", self.ap, self.bp, self.to_bm, "on", 4)
        self.recv("2p3", self.ao, self.bp)
        self.send("2o", self.ao, self.bp, self.to_bm, "on", 4)
        self.net.recv((self.tag, "2p01"), self.size(2))
        self.hand(self.bp)
        self.net.recv((self.tag, "2m23"), self.size(2))
        self.hand(self.bm)

    def five(self):
        self.net.recv((self.tag, "2o"), self.size(4))
        self.hand(self.bo)


class Coarse:
    def __init__(self, net, buf, c, y, x, to_row, column, sibling):
        self.net, self.buf, self.c, self.y, self.x = net, buf, c, y, x
        self.to_row, self.sibling = to_row, sibling
        _, self.yp, self.ym, self.yo, self.to_yp, self.to_ym, _ = column

    def send(self, key, make, device, batch, total):
        self.net.send(key, lambda: (make(), make(), device), batch=batch, total=lambda: total)

    def row(self, y):
        return self.buf.at[:, self.c, y]

    def part(self, y, k):
        return self.buf.at[:, self.c, y, pl.ds(2 * k, 2)]

    def first(self):
        for device in self.to_row:
            self.send(
                "p1", lambda: self.buf.at[:, self.c, self.y, self.x], device, "p1", self.buf.at[:, 0, 0, pl.ds(0, 3)]
            )

    def second(self):
        self.net.recv("p1", self.buf.at[:, 0, 0, pl.ds(0, 3)])
        for key, device in (("p2m", self.to_yp), ("p2p", self.to_ym)):
            self.send(key, lambda: self.row(self.y), device, "p2", self.buf.at[:, 0, pl.ds(0, 2)])

    def third(self):
        for key, y, k, device in (("p2m", self.ym, 0, self.to_yp), ("p2p", self.yp, 1, self.to_ym)):
            self.net.recv(key, self.row(y))
            self.send("p3", lambda y=y, k=k: self.part(y, k), device, "p3", self.row(0))

    def fourth(self):
        self.net.recv("p3", self.row(self.yo))
        self.send("p4", lambda: self.buf.at[:, self.c], self.sibling, "p4", self.buf.at[:, 0])

    def last(self, o):
        self.net.recv("p4", self.buf.at[:, o])


def normed(values, gain):
    floats = values.astype(F32)
    mean = jnp.mean(floats * floats, axis=-1, keepdims=True)
    return (floats * lax.rsqrt(mean + EPS) * gain).astype(BF16)


def kernel(
    tok, g1, gate1, up1, down1, mixg, pool, scale, g2, gate2, up2, down2, out,
    w, pw, xt, xq, n, h1, h2, wd1, wd2, maps, own1, pm, pp, so, sm, sp, ra, rb, a1, hs, hr, mg, ob, sq, rq, base, rx, st, tokv, gu, part1,
    ss, rs, ls,
):
    rep = lax.axis_index("rep")
    fs = lax.axis_index("fs")
    c = lax.axis_index("tp")
    o = 1 - c
    j = lax.div(fs, 16)
    z = rep * 2 + j
    y = lax.rem(lax.div(fs, 4), 4)
    x = lax.rem(fs, 4)
    zp, zo, zm = (lax.rem(z + k, 4) for k in (1, 2, 3))
    yp, yo, ym = (lax.rem(y + k, 4) for k in (1, 2, 3))
    xp, xo, xm = (lax.rem(x + k, 4) for k in (1, 2, 3))

    def dev(z_, y_, x_, c_):
        return (lax.div(z_, 2), lax.rem(z_, 2) * 16 + y_ * 4 + x_, c_)

    sibling = dev(z, y, x, o)
    net = Net(ss, rs, ls, sibling)
    keeper = c == j
    taker = c != j
    zq = lax.rem(z + 1 + 2 * lax.rem(z + c, 2), 4)

    def cols(k):
        return pl.ds(pl.multiple_of(k * UNIT, 128), UNIT)

    def feats(k):
        return pl.ds(pl.multiple_of(k * HALF, 128), HALF)

    def rows(k):
        return pl.ds(pl.multiple_of(k * ROWS, 128), ROWS)

    mats = ((gate1, up1, down1), (gate2, up2, down2), (gate2, up2, down2))
    subs = (lax.div(z, 2), 0, 1)

    own_tok = net.local(tok.at[rows(c), :], xt.at[z, :, feats(c)])
    own_tok.start()
    own_w = [net.slot() for u in range(3)]
    own_p = net.slot()

    def own_pool():
        return pltpu.make_async_copy(pool, pw.at[c, c, y, x], own_p)

    stage_t = net.local(tok, tokv)
    stage_t.start()
    stage_w = [net.slot(), net.slot()]

    @pl.when(taker)
    def _():
        for k in range(2):
            for m in range(3):
                pltpu.make_async_copy(mats[k][m], st.at[k, m], stage_w[k]).start()

    @pl.when(keeper)
    def _():
        for u in range(3):
            for m in range(3):
                pltpu.make_async_copy(mats[u][m].at[:, cols(subs[u])], w.at[u, m, c, y, x], own_w[u]).start()
        own_pool().start()

    own_mg = net.local(mixg, mg.at[0, c])
    own_sc = net.local(scale, mg.at[1, c])
    own_mg.start()
    own_sc.start()

    barrier = pltpu.get_barrier_semaphore()
    friends = [dev(z, y, x_, c) for x_ in (xp, xm, xo)] + [dev(z, y_, x, c) for y_ in (yp, ym, yo)] + [sibling]
    friends += [dev(z_, y, x, k) for z_ in (zp, zm) for k in range(2)]
    for friend in friends:
        pl.semaphore_signal(barrier, inc=1, device_id=friend, device_id_type=MESH)
    pl.semaphore_wait(barrier, len(friends))

    def staged(k):
        @pl.when(taker)
        def _():
            pltpu.make_async_copy(st.at[k], st.at[k], stage_w[k]).wait()

    def exchange(u):
        for ab, z_ in ((0, zp), (1, zm)):
            sub = (lax.div(z_, 2), 0, 1)[u]
            part = pl.ds(16 * ab, 16)
            for m in range(3):
                net.send(
                    ("z", u),
                    lambda m=m, part=part, sub=sub, z_=z_: (
                        st.at[min(u, 1), m, part, cols(sub)],
                        w.at[u, m, o, y, x, part, :],
                        dev(z_, y, x, o),
                    ),
                    cond=taker,
                    batch=("z", u),
                    total=lambda: w.at[u, :, 0, 0, 0],
                )

    def own(u):
        ref = w.at[u, :, c, y, x]

        @pl.when(keeper)
        def _():
            pltpu.make_async_copy(ref, ref, own_w[u]).wait()

        @pl.when(taker)
        def _():
            net.recv(("z", u), ref)

    in_x = (x, xp, xm, xo, dev(z, y, xp, c), dev(z, y, xm, c), dev(z, y, xo, c))
    in_y = (y, yp, ym, yo, dev(z, yp, x, c), dev(z, ym, x, c), dev(z, yo, x, c))
    two, top, low = pl.ds(0, 2), pl.ds(0, 16), pl.ds(16, 16)

    def size_w(k):
        return {
            2: w.at[0, :, 0, two, 0, top],
            4: w.at[0, :, 0, :, 0, top],
            8: w.at[0, :, 0, two, :, top],
            16: w.at[0, :, 0, :, :, top],
            32: w.at[0, :, 0],
        }[k]

    def stream_a(u):
        return Stream(
            net, u, "a", DIRECT and u == 0,
            lambda a, b: w.at[u, :, c, b, a, top, :],
            lambda b: w.at[u, :, c, b, :, top, :],
            size_w, 2, in_x, in_y, sibling,
        )

    def stream_b(u):
        return Stream(
            net, u, "b", DIRECT and u == 0,
            lambda a, b: w.at[u, :, c, a, b, low, :],
            lambda b: w.at[u, :, c, :, b, low, :],
            size_w, 2, in_y, in_x, sibling,
        )

    sa = [stream_a(u) for u in range(3)]
    sb = [stream_b(u) for u in range(3)]
    spool = Coarse(net, pw, c, y, x, (in_x[4], in_x[5], in_x[6]), in_y, sibling)

    def start(u):
        own(u)
        sa[u].one()
        sb[u].one()
        sa[u].then()
        sb[u].then()

    def handed(u):
        net.recv((u, "d"), w.at[u, :, o])

    def spread_tokens(tag, cond):
        for k in range(2):
            for key, z_ in (("tm", zp), ("tp", zm)):
                net.send(
                    key,
                    lambda k=k, z_=z_: (tokv.at[rows(k), :], xt.at[z, :, feats(c)], dev(z_, y, x, k)),
                    cond=cond, width=2, shift=c, batch=("t4", tag), total=lambda: xt.at[pl.ds(0, 2)],
                )
        net.send("ts", lambda: (tokv.at[rows(o), :], xt.at[z, :, feats(c)], sibling), cond=cond)

    def relay_tokens():
        for key, who, half, to in (("tm", zm, 0, zp), ("tp", zp, 1, zm)):
            net.recv(key, xt.at[who, :, feats(half)], half, 2)
            net.send(
                "to",
                lambda who=who, half=half, to=to: (
                    xt.at[who, :, feats(half)], xt.at[who, :, feats(half)], dev(to, y, x, c)
                ),
                batch="t2", total=lambda: xt.at[0],
            )
        net.recv("tm", xt.at[zm, :, feats(1)], 1, 2)
        net.recv("tp", xt.at[zp, :, feats(0)], 0, 2)

    def dot(lhs, rhs):
        return jnp.dot(lhs, rhs, preferred_element_type=F32)

    def gate_up(u, at, count, put):
        for k in range(UNIT // 128):
            part = pl.ds(k * 128, 128)
            wg = w[u, 0, :, :, :, :, part].reshape(D, 128)
            wu = w[u, 1, :, :, :, :, part].reshape(D, 128)
            both = jnp.dot(
                n[pl.ds(at, count), :], jnp.concatenate([wg, wu], axis=1), preferred_element_type=F32
            )
            gate, up = both[:, :128], both[:, 128:]
            put(k * 128, (gate * jax.nn.sigmoid(gate) * up).astype(BF16))

    def put1(at, count):
        def put(k, value):
            h1[pl.ds(at, count), pl.ds(k, 128)] = value

        return put

    def put2(at, count, first):
        def put(k, value):
            h2[pl.ds(at, count), pl.ds(first + k, 128)] = value

        return put

    def gate_up_half(u, at, count, part, put=None):
        lanes = feats(part)
        for k in range(UNIT // 128):
            hid = pl.ds(k * 128, 128)
            wg = w[u, 0, part, :, :, :, hid].reshape(HALF, 128)
            wu = w[u, 1, part, :, :, :, hid].reshape(HALF, 128)
            both = dot(n[pl.ds(at, count), lanes], jnp.concatenate([wg, wu], axis=1))
            if put is None:
                gu[:, pl.ds(k * 256, 256)] = both
            else:
                both = both + gu[:, pl.ds(k * 256, 256)]
                gate, up = both[:, :128], both[:, 128:]
                put(k * 128, (gate * jax.nn.sigmoid(gate) * up).astype(BF16))

    def turn(u, part, wide, at):
        for k in range(2):
            block = w[u, 2, part, 2 * k : 2 * k + 2].reshape(256, UNIT)
            wide[pl.ds(at, UNIT), pl.ds(pl.multiple_of(part * HALF + 256 * k, 128), 256)] = block.T

    def start_pool():
        @pl.when(keeper)
        def _():
            own_pool().wait()
            net.recv("ps", pw.at[o, c, y, x])

        @pl.when(taker)
        def _():
            net.recv("pz", pw.at[0, c, y, x], 0, 2)
            net.recv("pz", pw.at[1, c, y, x], 1, 2)

        spool.first()

    def norm_own():
        own_tok.wait()
        net.recv("ts", xt.at[z, :, feats(o)])
        n[pl.ds(0, ROWS), :] = normed(xt[z], gain1)

    def norm_next():
        n[pl.ds(ROWS, ROWS), :] = normed(xt[zm], gain1)
        n[pl.ds(2 * ROWS, ROWS), :] = normed(xt[zp], gain1)

    def norm_last():
        net.recv("to", xt.at[zo])
        n[pl.ds(3 * ROWS, ROWS), :] = normed(xt[zo], gain1)

    def first_near():
        turn(0, c, wd1, 0)
        gate_up_half(0, 3 * ROWS, ROWS, c)

    def first_opposite():
        gate_up_half(0, 3 * ROWS, ROWS, o, put1(3 * ROWS, ROWS))
        turn(0, o, wd1, 0)
        for k, z_ in ((0, zp), (1, zm)):
            lanes = slice(HALF * k, HALF * k + HALF)
            so[:, lanes] = dot(h1[pl.ds(3 * ROWS, ROWS), :], wd1[:, lanes]).astype(BF16)
            net.send(
                f"r{k}", lambda k=k, z_=z_: (so.at[:, feats(k)], ra.at[k], dev(z_, y, x, c)), batch="r", total=lambda: so
            )

    def pass_on(key, buf, k, half, z_):
        net.send(
            f"{key}{half}",
            lambda: (buf.at[:, feats(half)], rb.at[k, :, feats(half)], dev(z_, y, x, c)),
            batch="q", total=lambda: xt.at[two],
        )

    def first_neighbours():
        gate_up(0, ROWS, 2 * ROWS, put1(ROWS, 2 * ROWS))
        sums = dot(h1[pl.ds(ROWS, 2 * ROWS), :], wd1[...])
        sm[:, :HALF] = sums[:ROWS, :HALF].astype(BF16)
        sp[:, HALF:] = sums[ROWS:, HALF:].astype(BF16)
        pm[...] = sums[:ROWS, HALF:]
        pp[...] = sums[ROWS:, :HALF]
        pass_on("qm", sp, 0, 1, zp)
        pass_on("qp", sm, 1, 0, zm)

    def first_own():
        gate_up(0, 0, ROWS, put1(0, ROWS))
        own1[...] = dot(h1[pl.ds(0, ROWS), :], wd1[...])

    def first_pass_on():
        net.recv("r0", ra.at[0])
        sp[:, :HALF] = (pp[...] + ra[0].astype(F32)).astype(BF16)
        pass_on("qm", sp, 0, 0, zp)
        net.recv("r1", ra.at[1])
        sm[:, HALF:] = (pm[...] + ra[1].astype(F32)).astype(BF16)
        pass_on("qp", sm, 1, 1, zm)

    def pool_maps():
        spool.last(o)
        for g in range(4):
            wide = pw[g // 2].reshape(32, 16, 256).astype(F32)
            maps[g] = wide[:, 8 * (g % 2) : 8 * (g % 2) + 8, :].reshape(256, 256).astype(BF16).T

    def joined(k):
        return jnp.concatenate([mg[k, 0], mg[k, 1]], axis=1)

    def first_sum():
        for key, k, half in (("qm", 0, 1), ("qp", 1, 0), ("qm", 0, 0), ("qp", 1, 1)):
            net.recv(f"{key}{half}", rb.at[k, :, feats(half)])
        net.recv("mg", mg.at[:, o])

    def halo():
        for part in (slice(ROWS - 16, ROWS), slice(0, ROWS - 16)):
            block = own1[part] + rb[0, part].astype(F32) + rb[1, part].astype(F32)
            value = (xt[z, part].astype(F32) + 0.5 * block).astype(BF16)
            a1[part] = value
            hs[part] = normed(value, joined(0))
            if part.start:
                net.send("h", lambda: (hs.at[pl.ds(112, 16), :], hr, sibling))

    def mix():
        net.recv("h", hr)
        before = jnp.where(c == 1, hr[...].astype(F32), 0.0)
        floats = hs[...].astype(F32)
        longer = jnp.concatenate([before, floats], axis=0)
        positions = c * ROWS + lax.broadcasted_iota(jnp.int32, (ROWS, 256), 0)
        mix_scale = joined(1)
        for g in range(4):
            lanes = slice(256 * g, 256 * g + 256)
            total = longer[:, lanes]
            for k in range(g + 1):
                total = total + pltpu.roll(total, 2**k, axis=0)
            counts = jnp.minimum(positions + 1, 2 ** (g + 1)).astype(F32)
            diff = (total[16:] / counts - floats[:, lanes]).astype(BF16)
            mixed = dot(diff, maps[g])
            after = a1[:, lanes].astype(F32) + mixed * mix_scale[:, lanes]
            ob[:, lanes] = after.astype(BF16)
            if g % 2:
                half = feats(g // 2)
                net.send(
                    "a", lambda half=half: (ob.at[:, half], xq.at[:, half], dev(zq, y, x, c)), batch="a", total=lambda: ob
                )

    def second_norm():
        n[pl.ds(0, ROWS), :] = normed(ob[...], gain2)

    def second_own_1():
        turn(1, 0, wd2, 0)
        turn(1, 1, wd2, 0)
        gate_up(1, 0, ROWS, put2(0, ROWS, 0))

    def second_peer_1():
        net.recv("a", xq)
        n[pl.ds(ROWS, ROWS), :] = normed(xq[...], gain2)
        gate_up(1, ROWS, ROWS, put2(ROWS, ROWS, 0))
        part1[...] = dot(h2[pl.ds(ROWS, ROWS), :UNIT], wd2[:UNIT])

    def second_near():
        turn(2, c, wd2, UNIT)
        gate_up_half(2, ROWS, ROWS, c)

    def second_peer_2():
        gate_up_half(2, ROWS, ROWS, o, put2(ROWS, ROWS, UNIT))
        turn(2, o, wd2, UNIT)
        for k in range(2):
            lanes = slice(HALF * k, HALF * k + HALF)
            sq[:, lanes] = (part1[:, lanes] + dot(h2[pl.ds(ROWS, ROWS), UNIT:], wd2[UNIT:, lanes])).astype(BF16)
            net.send(
                "b",
                lambda k=k: (sq.at[:, feats(k)], rq.at[c], dev(zq, y, x, k)),
                width=2, shift=c, batch="b", total=lambda: sq,
            )

    def second_own_2():
        gate_up(2, 0, ROWS, put2(0, ROWS, UNIT))
        base[...] = ob[...].astype(F32) + 0.5 * dot(h2[pl.ds(0, ROWS), :], wd2[...])
        net.send("f", lambda: (base.at[:, feats(o)], rx, sibling))

    def last_sum():
        net.recv("f", rx)
        net.recv("b", rq.at[c], c, 2)
        out[rows(c), :] = (base[:, feats(c)] + 0.5 * rq[c].astype(F32)).astype(BF16)
        net.recv("b", rq.at[o], o, 2)
        out[rows(o), :] = (rx[...] + 0.5 * rq[o].astype(F32)).astype(BF16)

    staged(0)
    exchange(0)
    stage_t.wait()
    staged(1)
    exchange(1)
    spread_tokens(0, taker)
    start(0)
    start(1)
    exchange(2)
    net.send("ps", lambda: (pool, pw.at[c, o, y, x], sibling), cond=taker)
    net.send("pz", lambda: (pool, pw.at[c, j, y, x], dev(zp, y, x, j)), width=2, shift=c)
    own_mg.wait()
    own_sc.wait()
    net.send("mg", lambda: (mixg, mg.at[0, c], sibling), batch="mg", total=lambda: mg.at[:, 0])
    net.send("mg", lambda: (scale, mg.at[1, c], sibling), batch="mg", total=lambda: mg.at[:, 0])
    gain1 = g1[...]
    gain2 = g2[...]
    sa[0].two()
    sb[0].two()
    sa[0].pre()
    sb[0].pre()
    spread_tokens(1, keeper)
    sa[0].three()
    sb[0].three()
    relay_tokens()
    sa[0].four()
    sb[0].four()
    start_pool()
    start(2)
    norm_own()
    norm_next()
    norm_last()
    sa[0].five()
    sb[0].five()
    first_near()
    sa[1].two()
    sb[1].two()
    spool.second()
    handed(0)
    first_opposite()
    sa[2].two()
    sb[2].two()
    first_neighbours()
    spool.third()
    sa[1].pre()
    sb[1].pre()
    first_own()
    sa[1].three()
    sb[1].three()
    first_pass_on()
    sa[2].three()
    sb[2].three()
    sa[2].pre()
    sb[2].pre()
    spool.fourth()
    sa[1].four()
    sb[1].four()
    pool_maps()
    first_sum()
    halo()
    mix()
    sa[1].five()
    sb[1].five()
    sa[2].four()
    sb[2].four()
    second_norm()
    handed(1)
    second_own_1()
    sa[2].five()
    sb[2].five()
    second_peer_1()
    second_near()
    handed(2)
    second_peer_2()
    second_own_2()
    last_sum()
    net.finish()


def local(tok, g1, gate1, up1, down1, mixg, pool, scale, g2, gate2, up2, down2):
    hbm = pl.BlockSpec(memory_space=pl.ANY)
    vmem = pl.BlockSpec(memory_space=pltpu.VMEM)
    result = pl.pallas_call(
        kernel,
        out_shape=pltpu.VMEM((256, HALF), BF16),
        in_specs=[hbm, vmem, hbm, hbm, hbm, hbm, hbm, hbm, vmem, hbm, hbm, hbm],
        out_specs=vmem,
        scratch_shapes=[
            pltpu.VMEM((3, 3, 2, 4, 4, 32, UNIT), BF16),
            pltpu.VMEM((2, 2, 4, 4, 16, 256), BF16),
            pltpu.VMEM((4, ROWS, D), BF16),
            pltpu.VMEM((ROWS, D), BF16),
            pltpu.VMEM((4 * ROWS, D), BF16),
            pltpu.VMEM((4 * ROWS, UNIT), BF16),
            pltpu.VMEM((2 * ROWS, 2 * UNIT), BF16),
            pltpu.VMEM((UNIT, D), BF16),
            pltpu.VMEM((2 * UNIT, D), BF16),
            pltpu.VMEM((4, 256, 256), BF16),
            pltpu.VMEM((ROWS, D), F32),
            pltpu.VMEM((ROWS, HALF), F32),
            pltpu.VMEM((ROWS, HALF), F32),
            pltpu.VMEM((ROWS, D), BF16),
            pltpu.VMEM((ROWS, D), BF16),
            pltpu.VMEM((ROWS, D), BF16),
            pltpu.VMEM((2, ROWS, HALF), BF16),
            pltpu.VMEM((2, ROWS, D), BF16),
            pltpu.VMEM((ROWS, D), BF16),
            pltpu.VMEM((ROWS, D), BF16),
            pltpu.VMEM((16, D), BF16),
            pltpu.VMEM((2, 2, 1, HALF), F32),
            pltpu.VMEM((ROWS, D), BF16),
            pltpu.VMEM((ROWS, D), BF16),
            pltpu.VMEM((2, ROWS, HALF), BF16),
            pltpu.VMEM((ROWS, D), F32),
            pltpu.VMEM((ROWS, HALF), F32),
            pltpu.VMEM((2, 3, 32, 1280), BF16),
            pltpu.VMEM((256, HALF), BF16),
            pltpu.VMEM((ROWS, 2 * UNIT), F32),
            pltpu.VMEM((ROWS, D), F32),
            pltpu.SemaphoreType.DMA((N_SEND,)),
            pltpu.SemaphoreType.DMA((N_RECV,)),
            pltpu.SemaphoreType.DMA((N_LOCAL,)),
        ],
        compiler_params=pltpu.CompilerParams(collective_id=0, has_side_effects=True, vmem_limit_bytes=52 * 2**20),
    )(
        *(
            pltpu.with_memory_space_constraint(value, pltpu.HBM)
            for value in (
                tok.reshape(256, HALF), g1.reshape(1, D), gate1, up1, down1.T, mixg.reshape(1, HALF),
                pool.transpose(0, 2, 1).reshape(16, 256), scale.reshape(1, HALF), g2.reshape(1, D), gate2, up2, down2.T,
            )
        )
    )
    return result.reshape(1, 256, HALF)


def solution(mesh):
    placed = (
        P(("rep", "fs"), None, "tp"),
        P(),
        P("fs", "tp"),
        P("fs", "tp"),
        P("tp", "fs"),
        P("tp"),
        P("tp", None, "fs"),
        P("tp"),
        P(),
        P("fs", "tp"),
        P("fs", "tp"),
        P("tp", "fs"),
    )
    return jax.shard_map(
        local, mesh=mesh, in_specs=placed, out_specs=P(("rep", "fs"), None, "tp"), check_vma=False
    )
```

```python
import jax
import jax.numpy as jnp
from jax import lax
from jax.experimental import pallas as pl
from jax.experimental.pallas import tpu as pltpu
from jax.sharding import PartitionSpec as P

MESH = pl.DeviceIdType.MESH
BF16 = jnp.bfloat16
F32 = jnp.float32
EPS = 1e-06
D = 1024
HALF = 512
ROWS = 128
UNIT = 640
DIRECT = True
N_SEND = 35
N_RECV = 90
N_LOCAL = 10


class Net:
    def __init__(self, ss, rs, ls, here):
        self.ss, self.rs, self.ls, self.here = ss, rs, ls, here
        self.names = {}
        self.batches = {}
        self.locals = 0
        self.sends = 0
        self.pending = []

    def name(self, key, width=1):
        if key not in self.names:
            self.names[key] = sum(w for _, w in self.names.values()), width
        return self.names[key][0]

    def send(self, key, make, cond=None, width=1, shift=None, batch=None, total=None):
        base = self.name(key, width)
        first = batch is None or batch not in self.batches
        if first:
            slot = self.sends
            self.sends += 1
            if batch is not None:
                self.batches[batch] = slot
        else:
            slot = self.batches[batch]

        def copy(src, dst, device):
            where = base if shift is None else base + shift
            return pltpu.make_async_remote_copy(
                src, dst, self.ss.at[slot], self.rs.at[where], device_id=device, device_id_type=MESH
            )

        def end():
            ref = make()[0] if total is None else total()
            copy(ref, ref, self.here).wait_send()

        if cond is None:
            copy(*make()).start()
        else:
            pl.when(cond)(lambda: copy(*make()).start())
        if first:
            self.pending.append(end if cond is None else lambda: pl.when(cond)(end))

    def recv(self, key, ref, offset=0, width=1):
        where = self.name(key, width) + offset
        pltpu.make_async_remote_copy(
            ref, ref, self.ss.at[0], self.rs.at[where], device_id=self.here, device_id_type=MESH
        ).wait_recv()

    def slot(self):
        self.locals += 1
        return self.ls.at[self.locals - 1]

    def local(self, src, dst):
        return pltpu.make_async_copy(src, dst, self.slot())

    def finish(self):
        for end in self.pending:
            end()
        assert self.sends == N_SEND and self.locals == N_LOCAL
        assert sum(w for _, w in self.names.values()) == N_RECV


class Stream:
    def __init__(self, net, unit, tag, direct, piece, group, size, many, first, second, sibling):
        self.net, self.unit, self.tag, self.direct = net, unit, (unit, tag), direct
        self.piece, self.group, self.size, self.many = piece, group, size, many
        self.a, self.ap, self.am, self.ao, self.to_ap, self.to_am, self.to_ao = first
        self.b, self.bp, self.bm, self.bo, self.to_bp, self.to_bm, self.to_bo = second
        self.sibling = sibling
        self.flip = unit == 2

    def send(self, what, a, b, device, kind, count):
        self.net.send(
            (self.tag, what),
            lambda: (self.piece(a, b), self.piece(a, b), device),
            batch=(self.unit, kind),
            total=lambda: self.size(count * self.many),
        )

    def recv(self, what, a, b):
        self.net.recv((self.tag, what), self.piece(a, b))

    def both(self, k, a):
        late_m, late_p = ("2m23" if k >= 2 else f"2m{k}"), ("2p01" if k < 2 else f"2p{k}")
        self.send(late_m, a, self.b, self.to_bp, "both", 8)
        self.send(late_p, a, self.b, self.to_bm, "both", 8)

    def hand(self, b):
        self.net.send(
            (self.unit, "d"),
            lambda: (self.group(b), self.group(b), self.sibling),
            batch=(self.unit, "hand"),
            total=lambda: self.size(16 * self.many),
        )

    def one(self):
        self.send("1m", self.a, self.b, self.to_ap, "ring", 2)
        self.send("1p", self.a, self.b, self.to_am, "ring", 2)
        if self.direct:
            self.send("1o", self.a, self.b, self.to_ao, "far", 1)

    def then(self):
        self.both(0, self.a)

    def two(self):
        for key, k, a, to in (("1p", 2, self.ap, self.to_am), ("1m", 1, self.am, self.to_ap))[:: -1 if self.flip else 1]:
            self.recv(key, a, self.b)
            if key == ("1m" if self.flip else "1p") and not self.direct:
                self.send("1o", a, self.b, to, "far", 1)
            self.both(k, a)

    def three(self):
        self.recv("1o", self.ao, self.b)
        self.both(3, self.ao)
        self.hand(self.b)

    def pre(self):
        self.recv("2m0", self.a, self.bm)
        self.send("2o", self.a, self.bm, self.to_bp, "on", 4)

    def mid(self):
        self.recv("2m1", self.am, self.bm)
        self.send("2o", self.am, self.bm, self.to_bp, "on", 4)
        self.recv("2p2", self.ap, self.bp)
        self.send("2o", self.ap, self.bp, self.to_bm, "on", 4)

    def four(self):
        self.recv("2p3", self.ao, self.bp)
        self.send("2o", self.ao, self.bp, self.to_bm, "on", 4)
        self.net.recv((self.tag, "2p01"), self.size(2))
        self.hand(self.bp)
        self.net.recv((self.tag, "2m23"), self.size(2))
        self.hand(self.bm)

    def five(self):
        self.net.recv((self.tag, "2o"), self.size(4))
        self.hand(self.bo)


class Coarse:
    def __init__(self, net, piece, some, first, second, sibling):
        self.net, self.piece, self.some, self.first_axis, self.second_axis = net, piece, some, first, second
        self.sibling = sibling

    def send(self, key, a, device, total):
        self.net.send(
            key, lambda: (self.piece(a, self.second_axis[0]), self.piece(a, self.second_axis[0]), device),
            batch=key, total=lambda: total,
        )

    def first(self):
        for device in self.first_axis[4:]:
            self.send("p1", self.first_axis[0], device, self.some(1, 3))

    def second(self):
        self.net.recv("p1", self.some(1, 3))
        for device in self.second_axis[4:]:
            for a in self.first_axis[:4]:
                self.send("p2", a, device, self.some(3, 4))

    def third(self, mine):
        self.net.recv("p2", self.some(3, 4))
        self.net.send("p3", lambda: (mine, mine, self.sibling))

    def last(self, theirs):
        self.net.recv("p3", theirs)


def normed(values, gain):
    floats = values.astype(F32)
    mean = jnp.mean(floats * floats, axis=-1, keepdims=True)
    return (floats * lax.rsqrt(mean + EPS) * gain).astype(BF16)


def kernel(
    tok, g1, gate1, up1, down1, mixg, pool, scale, g2, gate2, up2, down2, out,
    w, pw, xt, xq, n, h1, h2, wd1, wd2, maps, own1, pm, pp, so, sm, sp, ra, rb, a1, hs, hr, mg, ob, sq, rq, base, rx, st, tokv, gu, part1,
    ss, rs, ls,
):
    rep = lax.axis_index("rep")
    fs = lax.axis_index("fs")
    c = lax.axis_index("tp")
    o = 1 - c
    j = lax.div(fs, 16)
    z = rep * 2 + j
    y = lax.rem(lax.div(fs, 4), 4)
    x = lax.rem(fs, 4)
    zp, zo, zm = (lax.rem(z + k, 4) for k in (1, 2, 3))
    yp, yo, ym = (lax.rem(y + k, 4) for k in (1, 2, 3))
    xp, xo, xm = (lax.rem(x + k, 4) for k in (1, 2, 3))

    def dev(z_, y_, x_, c_):
        return (lax.div(z_, 2), lax.rem(z_, 2) * 16 + y_ * 4 + x_, c_)

    sibling = dev(z, y, x, o)
    net = Net(ss, rs, ls, sibling)
    keeper = c == j
    taker = c != j
    zq = lax.rem(z + 1 + 2 * lax.rem(z + c, 2), 4)

    def cols(k):
        return pl.ds(pl.multiple_of(k * UNIT, 128), UNIT)

    def feats(k):
        return pl.ds(pl.multiple_of(k * HALF, 128), HALF)

    def rows(k):
        return pl.ds(pl.multiple_of(k * ROWS, 128), ROWS)

    mats = ((gate1, up1, down1), (gate2, up2, down2), (gate2, up2, down2))
    subs = (lax.div(z, 2), 0, 1)

    own_tok = net.local(tok.at[rows(c), :], xt.at[z, :, feats(c)])
    own_tok.start()
    own_w = [net.slot() for u in range(3)]
    own_p = net.slot()

    def own_pool():
        return pltpu.make_async_copy(pool, pw.at[c, c, y, x], own_p)

    stage_t = net.local(tok, tokv)
    stage_t.start()
    stage_w = [net.slot(), net.slot()]

    @pl.when(taker)
    def _():
        for k in range(2):
            for m in range(3):
                pltpu.make_async_copy(mats[k][m], st.at[k, m], stage_w[k]).start()

    @pl.when(keeper)
    def _():
        for u in range(3):
            for m in range(3):
                pltpu.make_async_copy(mats[u][m].at[:, cols(subs[u])], w.at[u, m, c, y, x], own_w[u]).start()
        own_pool().start()

    own_mg = net.local(mixg, mg.at[0, c])
    own_sc = net.local(scale, mg.at[1, c])
    own_mg.start()
    own_sc.start()

    barrier = pltpu.get_barrier_semaphore()
    friends = [dev(z, y, x_, c) for x_ in (xp, xm, xo)] + [dev(z, y_, x, c) for y_ in (yp, ym, yo)] + [sibling]
    friends += [dev(z_, y, x, k) for z_ in (zp, zm) for k in range(2)]
    for friend in friends:
        pl.semaphore_signal(barrier, inc=1, device_id=friend, device_id_type=MESH)
    pl.semaphore_wait(barrier, len(friends))

    def staged(k):
        @pl.when(taker)
        def _():
            pltpu.make_async_copy(st.at[k], st.at[k], stage_w[k]).wait()

    def exchange(u):
        for ab, z_ in ((0, zp), (1, zm)):
            sub = (lax.div(z_, 2), 0, 1)[u]
            part = pl.ds(16 * ab, 16)
            for m in range(3):
                net.send(
                    ("z", u),
                    lambda m=m, part=part, sub=sub, z_=z_: (
                        st.at[min(u, 1), m, part, cols(sub)],
                        w.at[u, m, o, y, x, part, :],
                        dev(z_, y, x, o),
                    ),
                    cond=taker,
                    batch=("z", u),
                    total=lambda: w.at[u, :, 0, 0, 0],
                )

    def own(u):
        ref = w.at[u, :, c, y, x]

        @pl.when(keeper)
        def _():
            pltpu.make_async_copy(ref, ref, own_w[u]).wait()

        @pl.when(taker)
        def _():
            net.recv(("z", u), ref)

    in_x = (x, xp, xm, xo, dev(z, y, xp, c), dev(z, y, xm, c), dev(z, y, xo, c))
    in_y = (y, yp, ym, yo, dev(z, yp, x, c), dev(z, ym, x, c), dev(z, yo, x, c))
    two, top, low = pl.ds(0, 2), pl.ds(0, 16), pl.ds(16, 16)

    def size_w(k):
        return {
            2: w.at[0, :, 0, two, 0, top],
            4: w.at[0, :, 0, :, 0, top],
            8: w.at[0, :, 0, two, :, top],
            16: w.at[0, :, 0, :, :, top],
            32: w.at[0, :, 0],
        }[k]

    def stream_a(u):
        return Stream(
            net, u, "a", DIRECT and u == 0,
            lambda a, b: w.at[u, :, c, b, a, top, :],
            lambda b: w.at[u, :, c, b, :, top, :],
            size_w, 2, in_x, in_y, sibling,
        )

    def stream_b(u):
        return Stream(
            net, u, "b", DIRECT and u == 0,
            lambda a, b: w.at[u, :, c, a, b, low, :],
            lambda b: w.at[u, :, c, :, b, low, :],
            size_w, 2, in_y, in_x, sibling,
        )

    sa = [stream_a(u) for u in range(3)]
    sb = [stream_b(u) for u in range(3)]
    def pick(k, l):
        return k * o + l * c

    xs, ys = (x, xp, xm, xo), (y, yp, ym, yo)
    first = [pick(k, l) for k, l in zip(xs, ys)]
    second = [pick(l, k) for k, l in zip(xs, ys)]
    first += [dev(z, pick(y, l), pick(k, x), c) for k, l in zip(xs[1:], ys[1:])]
    second += [dev(z, pick(l, y), pick(x, k), c) for k, l in zip(xs[1:], ys[1:])]
    spool = Coarse(
        net, lambda a, b: pw.at[:, c, pick(b, a), pick(a, b)], lambda k, l: pw.at[:, 0, pl.ds(0, k), pl.ds(0, l)],
        first, second, sibling,
    )

    def start(u):
        own(u)
        sa[u].one()
        sb[u].one()
        sa[u].then()
        sb[u].then()

    def handed(u):
        net.recv((u, "d"), w.at[u, :, o])

    def spread_tokens(tag, cond):
        for k in range(2):
            for key, z_ in (("tm", zp), ("tp", zm)):
                net.send(
                    key,
                    lambda k=k, z_=z_: (tokv.at[rows(k), :], xt.at[z, :, feats(c)], dev(z_, y, x, k)),
                    cond=cond, width=2, shift=c, batch=("t4", tag), total=lambda: xt.at[pl.ds(0, 2)],
                )
        net.send("ts", lambda: (tokv.at[rows(o), :], xt.at[z, :, feats(c)], sibling), cond=cond)

    def relay_tokens():
        for key, who, half, to in (("tm", zm, 0, zp), ("tp", zp, 1, zm)):
            net.recv(key, xt.at[who, :, feats(half)], half, 2)
            net.send(
                "to",
                lambda who=who, half=half, to=to: (
                    xt.at[who, :, feats(half)], xt.at[who, :, feats(half)], dev(to, y, x, c)
                ),
                batch="t2", total=lambda: xt.at[0],
            )
        net.recv("tm", xt.at[zm, :, feats(1)], 1, 2)
        net.recv("tp", xt.at[zp, :, feats(0)], 0, 2)

    def dot(lhs, rhs):
        return jnp.dot(lhs, rhs, preferred_element_type=F32)

    def gate_up(u, at, count, put):
        for k in range(UNIT // 128):
            part = pl.ds(k * 128, 128)
            wg = w[u, 0, :, :, :, :, part].reshape(D, 128)
            wu = w[u, 1, :, :, :, :, part].reshape(D, 128)
            both = jnp.dot(
                n[pl.ds(at, count), :], jnp.concatenate([wg, wu], axis=1), preferred_element_type=F32
            )
            gate, up = both[:, :128], both[:, 128:]
            put(k * 128, (gate * jax.nn.sigmoid(gate) * up).astype(BF16))

    def put1(at, count):
        def put(k, value):
            h1[pl.ds(at, count), pl.ds(k, 128)] = value

        return put

    def put2(at, count, first):
        def put(k, value):
            h2[pl.ds(at, count), pl.ds(first + k, 128)] = value

        return put

    def gate_up_half(u, at, count, part, put=None):
        lanes = feats(part)
        for k in range(UNIT // 128):
            hid = pl.ds(k * 128, 128)
            wg = w[u, 0, part, :, :, :, hid].reshape(HALF, 128)
            wu = w[u, 1, part, :, :, :, hid].reshape(HALF, 128)
            both = dot(n[pl.ds(at, count), lanes], jnp.concatenate([wg, wu], axis=1))
            if put is None:
                gu[:, pl.ds(k * 256, 256)] = both
            else:
                both = both + gu[:, pl.ds(k * 256, 256)]
                gate, up = both[:, :128], both[:, 128:]
                put(k * 128, (gate * jax.nn.sigmoid(gate) * up).astype(BF16))

    def turn(u, part, wide, at):
        for k in range(2):
            block = w[u, 2, part, 2 * k : 2 * k + 2].reshape(256, UNIT)
            wide[pl.ds(at, UNIT), pl.ds(pl.multiple_of(part * HALF + 256 * k, 128), 256)] = block.T

    def start_pool():
        @pl.when(keeper)
        def _():
            own_pool().wait()
            net.recv("ps", pw.at[o, c, y, x])

        @pl.when(taker)
        def _():
            net.recv("pz", pw.at[0, c, y, x], 0, 2)
            net.recv("pz", pw.at[1, c, y, x], 1, 2)

        spool.first()

    def norm_own():
        own_tok.wait()
        net.recv("ts", xt.at[z, :, feats(o)])
        n[pl.ds(0, ROWS), :] = normed(xt[z], gain1)

    def norm_next():
        n[pl.ds(ROWS, ROWS), :] = normed(xt[zm], gain1)
        n[pl.ds(2 * ROWS, ROWS), :] = normed(xt[zp], gain1)

    def norm_last():
        net.recv("to", xt.at[zo])
        n[pl.ds(3 * ROWS, ROWS), :] = normed(xt[zo], gain1)

    def first_near():
        turn(0, c, wd1, 0)
        gate_up_half(0, 3 * ROWS, ROWS, c)

    def first_opposite():
        gate_up_half(0, 3 * ROWS, ROWS, o, put1(3 * ROWS, ROWS))
        turn(0, o, wd1, 0)
        for k, z_ in ((0, zp), (1, zm)):
            lanes = slice(HALF * k, HALF * k + HALF)
            so[:, lanes] = dot(h1[pl.ds(3 * ROWS, ROWS), :], wd1[:, lanes]).astype(BF16)
            net.send(
                f"r{k}", lambda k=k, z_=z_: (so.at[:, feats(k)], ra.at[k], dev(z_, y, x, c)), batch="r", total=lambda: so
            )

    def pass_on(key, buf, k, half, z_):
        net.send(
            f"{key}{half}",
            lambda: (buf.at[:, feats(half)], rb.at[k, :, feats(half)], dev(z_, y, x, c)),
            batch="q", total=lambda: xt.at[two],
        )

    def first_neighbours():
        gate_up(0, ROWS, 2 * ROWS, put1(ROWS, 2 * ROWS))
        sums = dot(h1[pl.ds(ROWS, 2 * ROWS), :], wd1[...])
        sm[:, :HALF] = sums[:ROWS, :HALF].astype(BF16)
        sp[:, HALF:] = sums[ROWS:, HALF:].astype(BF16)
        pm[...] = sums[:ROWS, HALF:]
        pp[...] = sums[ROWS:, :HALF]
        pass_on("qm", sp, 0, 1, zp)
        pass_on("qp", sm, 1, 0, zm)

    def first_own():
        gate_up(0, 0, ROWS, put1(0, ROWS))
        own1[...] = dot(h1[pl.ds(0, ROWS), :], wd1[...])

    def first_pass_on():
        net.recv("r0", ra.at[0])
        sp[:, :HALF] = (pp[...] + ra[0].astype(F32)).astype(BF16)
        pass_on("qm", sp, 0, 0, zp)
        net.recv("r1", ra.at[1])
        sm[:, HALF:] = (pm[...] + ra[1].astype(F32)).astype(BF16)
        pass_on("qp", sm, 1, 1, zm)

    def pool_maps():
        spool.last(pw.at[:, o])
        for g in range(4):
            wide = pw[g // 2].reshape(32, 16, 256).astype(F32)
            maps[g] = wide[:, 8 * (g % 2) : 8 * (g % 2) + 8, :].reshape(256, 256).astype(BF16).T

    def joined(k):
        return jnp.concatenate([mg[k, 0], mg[k, 1]], axis=1)

    def first_sum():
        for key, k, half in (("qm", 0, 1), ("qp", 1, 0), ("qm", 0, 0), ("qp", 1, 1)):
            net.recv(f"{key}{half}", rb.at[k, :, feats(half)])
        net.recv("mg", mg.at[:, o])

    def halo():
        for part in (slice(ROWS - 16, ROWS), slice(0, ROWS - 16)):
            block = own1[part] + rb[0, part].astype(F32) + rb[1, part].astype(F32)
            value = (xt[z, part].astype(F32) + 0.5 * block).astype(BF16)
            a1[part] = value
            hs[part] = normed(value, joined(0))
            if part.start:
                net.send("h", lambda: (hs.at[pl.ds(112, 16), :], hr, sibling))

    def mix():
        net.recv("h", hr)
        before = jnp.where(c == 1, hr[...].astype(F32), 0.0)
        floats = hs[...].astype(F32)
        longer = jnp.concatenate([before, floats], axis=0)
        positions = c * ROWS + lax.broadcasted_iota(jnp.int32, (ROWS, 256), 0)
        mix_scale = joined(1)
        for g in range(4):
            lanes = slice(256 * g, 256 * g + 256)
            total = longer[:, lanes]
            for k in range(g + 1):
                total = total + pltpu.roll(total, 2**k, axis=0)
            counts = jnp.minimum(positions + 1, 2 ** (g + 1)).astype(F32)
            diff = (total[16:] / counts - floats[:, lanes]).astype(BF16)
            mixed = dot(diff, maps[g])
            after = a1[:, lanes].astype(F32) + mixed * mix_scale[:, lanes]
            ob[:, lanes] = after.astype(BF16)
            if g % 2:
                half = feats(g // 2)
                net.send(
                    "a", lambda half=half: (ob.at[:, half], xq.at[:, half], dev(zq, y, x, c)), batch="a", total=lambda: ob
                )

    def second_norm():
        n[pl.ds(0, ROWS), :] = normed(ob[...], gain2)

    def second_own_1():
        turn(1, 0, wd2, 0)
        turn(1, 1, wd2, 0)
        gate_up(1, 0, ROWS, put2(0, ROWS, 0))

    def second_peer_1():
        net.recv("a", xq)
        n[pl.ds(ROWS, ROWS), :] = normed(xq[...], gain2)
        gate_up(1, ROWS, ROWS, put2(ROWS, ROWS, 0))
        part1[...] = dot(h2[pl.ds(ROWS, ROWS), :UNIT], wd2[:UNIT])

    def second_near():
        turn(2, c, wd2, UNIT)
        gate_up_half(2, ROWS, ROWS, c)

    def second_peer_2():
        gate_up_half(2, ROWS, ROWS, o, put2(ROWS, ROWS, UNIT))
        turn(2, o, wd2, UNIT)
        for k in range(2):
            lanes = slice(HALF * k, HALF * k + HALF)
            sq[:, lanes] = (part1[:, lanes] + dot(h2[pl.ds(ROWS, ROWS), UNIT:], wd2[UNIT:, lanes])).astype(BF16)
            net.send(
                "b",
                lambda k=k: (sq.at[:, feats(k)], rq.at[c], dev(zq, y, x, k)),
                width=2, shift=c, batch="b", total=lambda: sq,
            )

    def second_own_2():
        gate_up(2, 0, ROWS, put2(0, ROWS, UNIT))
        base[...] = ob[...].astype(F32) + 0.5 * dot(h2[pl.ds(0, ROWS), :], wd2[...])
        net.send("f", lambda: (base.at[:, feats(o)], rx, sibling))

    def last_sum():
        net.recv("f", rx)
        net.recv("b", rq.at[c], c, 2)
        out[rows(c), :] = (base[:, feats(c)] + 0.5 * rq[c].astype(F32)).astype(BF16)
        net.recv("b", rq.at[o], o, 2)
        out[rows(o), :] = (rx[...] + 0.5 * rq[o].astype(F32)).astype(BF16)

    staged(0)
    exchange(0)
    stage_t.wait()
    staged(1)
    exchange(1)
    spread_tokens(0, taker)
    start(0)
    start(1)
    exchange(2)
    net.send("ps", lambda: (pool, pw.at[c, o, y, x], sibling), cond=taker)
    net.send("pz", lambda: (pool, pw.at[c, j, y, x], dev(zp, y, x, j)), width=2, shift=c)
    own_mg.wait()
    own_sc.wait()
    net.send("mg", lambda: (mixg, mg.at[0, c], sibling), batch="mg", total=lambda: mg.at[:, 0])
    net.send("mg", lambda: (scale, mg.at[1, c], sibling), batch="mg", total=lambda: mg.at[:, 0])
    gain1 = g1[...]
    gain2 = g2[...]
    sa[0].two()
    sb[0].two()
    sa[0].pre()
    sb[0].pre()
    spread_tokens(1, keeper)
    sa[0].three()
    sb[0].three()
    relay_tokens()
    sa[0].mid()
    sb[0].mid()
    sa[0].four()
    sb[0].four()
    start_pool()
    start(2)
    norm_own()
    norm_next()
    norm_last()
    sa[0].five()
    sb[0].five()
    first_near()
    sa[1].two()
    sb[1].two()
    spool.second()
    handed(0)
    first_opposite()
    sa[2].two()
    sb[2].two()
    first_neighbours()
    sa[1].pre()
    sb[1].pre()
    first_own()
    sa[1].three()
    sb[1].three()
    sa[1].mid()
    sb[1].mid()
    first_pass_on()
    sa[2].three()
    sb[2].three()
    sa[2].pre()
    sb[2].pre()
    spool.third(pw.at[:, c])
    sa[1].four()
    sb[1].four()
    sa[2].mid()
    sb[2].mid()
    pool_maps()
    first_sum()
    halo()
    mix()
    sa[1].five()
    sb[1].five()
    sa[2].four()
    sb[2].four()
    second_norm()
    handed(1)
    second_own_1()
    sa[2].five()
    sb[2].five()
    second_peer_1()
    second_near()
    handed(2)
    second_peer_2()
    second_own_2()
    last_sum()
    net.finish()


def local(tok, g1, gate1, up1, down1, mixg, pool, scale, g2, gate2, up2, down2):
    hbm = pl.BlockSpec(memory_space=pl.ANY)
    vmem = pl.BlockSpec(memory_space=pltpu.VMEM)
    result = pl.pallas_call(
        kernel,
        out_shape=pltpu.VMEM((256, HALF), BF16),
        in_specs=[hbm, vmem, hbm, hbm, hbm, hbm, hbm, hbm, vmem, hbm, hbm, hbm],
        out_specs=vmem,
        scratch_shapes=[
            pltpu.VMEM((3, 3, 2, 4, 4, 32, UNIT), BF16),
            pltpu.VMEM((2, 2, 4, 4, 16, 256), BF16),
            pltpu.VMEM((4, ROWS, D), BF16),
            pltpu.VMEM((ROWS, D), BF16),
            pltpu.VMEM((4 * ROWS, D), BF16),
            pltpu.VMEM((4 * ROWS, UNIT), BF16),
            pltpu.VMEM((2 * ROWS, 2 * UNIT), BF16),
            pltpu.VMEM((UNIT, D), BF16),
            pltpu.VMEM((2 * UNIT, D), BF16),
            pltpu.VMEM((4, 256, 256), BF16),
            pltpu.VMEM((ROWS, D), F32),
            pltpu.VMEM((ROWS, HALF), F32),
            pltpu.VMEM((ROWS, HALF), F32),
            pltpu.VMEM((ROWS, D), BF16),
            pltpu.VMEM((ROWS, D), BF16),
            pltpu.VMEM((ROWS, D), BF16),
            pltpu.VMEM((2, ROWS, HALF), BF16),
            pltpu.VMEM((2, ROWS, D), BF16),
            pltpu.VMEM((ROWS, D), BF16),
            pltpu.VMEM((ROWS, D), BF16),
            pltpu.VMEM((16, D), BF16),
            pltpu.VMEM((2, 2, 1, HALF), F32),
            pltpu.VMEM((ROWS, D), BF16),
            pltpu.VMEM((ROWS, D), BF16),
            pltpu.VMEM((2, ROWS, HALF), BF16),
            pltpu.VMEM((ROWS, D), F32),
            pltpu.VMEM((ROWS, HALF), F32),
            pltpu.VMEM((2, 3, 32, 1280), BF16),
            pltpu.VMEM((256, HALF), BF16),
            pltpu.VMEM((ROWS, 2 * UNIT), F32),
            pltpu.VMEM((ROWS, D), F32),
            pltpu.SemaphoreType.DMA((N_SEND,)),
            pltpu.SemaphoreType.DMA((N_RECV,)),
            pltpu.SemaphoreType.DMA((N_LOCAL,)),
        ],
        compiler_params=pltpu.CompilerParams(collective_id=0, has_side_effects=True, vmem_limit_bytes=52 * 2**20),
    )(
        *(
            pltpu.with_memory_space_constraint(value, pltpu.HBM)
            for value in (
                tok.reshape(256, HALF), g1.reshape(1, D), gate1, up1, down1.T, mixg.reshape(1, HALF),
                pool.transpose(0, 2, 1).reshape(16, 256), scale.reshape(1, HALF), g2.reshape(1, D), gate2, up2, down2.T,
            )
        )
    )
    return result.reshape(1, 256, HALF)


def solution(mesh):
    placed = (
        P(("rep", "fs"), None, "tp"),
        P(),
        P("fs", "tp"),
        P("fs", "tp"),
        P("tp", "fs"),
        P("tp"),
        P("tp", None, "fs"),
        P("tp"),
        P(),
        P("fs", "tp"),
        P("fs", "tp"),
        P("tp", "fs"),
    )
    return jax.shard_map(
        local, mesh=mesh, in_specs=placed, out_specs=P(("rep", "fs"), None, "tp"), check_vma=False
    )
```

```python
import jax
import jax.numpy as jnp
from jax import lax
from jax.experimental import pallas as pl
from jax.experimental.pallas import tpu as pltpu
from jax.sharding import PartitionSpec as P

MESH = pl.DeviceIdType.MESH
BF16 = jnp.bfloat16
F32 = jnp.float32
EPS = 1e-06
D = 1024
HALF = 512
ROWS = 128
UNIT = 640
DIRECT = False
N_SEND = 35
N_RECV = 90
N_LOCAL = 10


class Net:
    def __init__(self, ss, rs, ls, here):
        self.ss, self.rs, self.ls, self.here = ss, rs, ls, here
        self.names = {}
        self.batches = {}
        self.locals = 0
        self.sends = 0
        self.pending = []

    def name(self, key, width=1):
        if key not in self.names:
            self.names[key] = sum(w for _, w in self.names.values()), width
        return self.names[key][0]

    def send(self, key, make, cond=None, width=1, shift=None, batch=None, total=None):
        base = self.name(key, width)
        first = batch is None or batch not in self.batches
        if first:
            slot = self.sends
            self.sends += 1
            if batch is not None:
                self.batches[batch] = slot
        else:
            slot = self.batches[batch]

        def copy(src, dst, device):
            where = base if shift is None else base + shift
            return pltpu.make_async_remote_copy(
                src, dst, self.ss.at[slot], self.rs.at[where], device_id=device, device_id_type=MESH
            )

        def end():
            ref = make()[0] if total is None else total()
            copy(ref, ref, self.here).wait_send()

        if cond is None:
            copy(*make()).start()
        else:
            pl.when(cond)(lambda: copy(*make()).start())
        if first:
            self.pending.append(end if cond is None else lambda: pl.when(cond)(end))

    def recv(self, key, ref, offset=0, width=1):
        where = self.name(key, width) + offset
        pltpu.make_async_remote_copy(
            ref, ref, self.ss.at[0], self.rs.at[where], device_id=self.here, device_id_type=MESH
        ).wait_recv()

    def slot(self):
        self.locals += 1
        return self.ls.at[self.locals - 1]

    def local(self, src, dst):
        return pltpu.make_async_copy(src, dst, self.slot())

    def finish(self):
        for end in self.pending:
            end()
        assert self.sends == N_SEND and self.locals == N_LOCAL
        assert sum(w for _, w in self.names.values()) == N_RECV


class Stream:
    def __init__(self, net, unit, tag, direct, piece, group, size, many, first, second, sibling):
        self.net, self.unit, self.tag, self.direct = net, unit, (unit, tag), direct
        self.piece, self.group, self.size, self.many = piece, group, size, many
        self.a, self.ap, self.am, self.ao, self.to_ap, self.to_am, self.to_ao = first
        self.b, self.bp, self.bm, self.bo, self.to_bp, self.to_bm, self.to_bo = second
        self.sibling = sibling
        self.flip = unit == 2

    def send(self, what, a, b, device, kind, count):
        self.net.send(
            (self.tag, what),
            lambda: (self.piece(a, b), self.piece(a, b), device),
            batch=(self.unit, kind),
            total=lambda: self.size(count * self.many),
        )

    def recv(self, what, a, b):
        self.net.recv((self.tag, what), self.piece(a, b))

    def both(self, k, a):
        late_m, late_p = ("2m23" if k >= 2 else f"2m{k}"), ("2p01" if k < 2 else f"2p{k}")
        self.send(late_m, a, self.b, self.to_bp, "both", 8)
        self.send(late_p, a, self.b, self.to_bm, "both", 8)

    def hand(self, b):
        self.net.send(
            (self.unit, "d"),
            lambda: (self.group(b), self.group(b), self.sibling),
            batch=(self.unit, "hand"),
            total=lambda: self.size(16 * self.many),
        )

    def one(self):
        self.send("1m", self.a, self.b, self.to_ap, "ring", 2)
        self.send("1p", self.a, self.b, self.to_am, "ring", 2)
        if self.direct:
            self.send("1o", self.a, self.b, self.to_ao, "far", 1)

    def then(self):
        self.both(0, self.a)

    def two(self):
        for key, k, a, to in (("1p", 2, self.ap, self.to_am), ("1m", 1, self.am, self.to_ap))[:: -1 if self.flip else 1]:
            self.recv(key, a, self.b)
            if key == ("1m" if self.flip else "1p") and not self.direct:
                self.send("1o", a, self.b, to, "far", 1)
            self.both(k, a)

    def three(self):
        self.recv("1o", self.ao, self.b)
        self.both(3, self.ao)
        self.hand(self.b)

    def pre(self):
        self.recv("2m0", self.a, self.bm)
        self.send("2o", self.a, self.bm, self.to_bp, "on", 4)

    def mid(self):
        self.recv("2m1", self.am, self.bm)
        self.send("2o", self.am, self.bm, self.to_bp, "on", 4)
        self.recv("2p2", self.ap, self.bp)
        self.send("2o", self.ap, self.bp, self.to_bm, "on", 4)

    def four(self):
        self.recv("2p3", self.ao, self.bp)
        self.send("2o", self.ao, self.bp, self.to_bm, "on", 4)
        self.net.recv((self.tag, "2p01"), self.size(2))
        self.hand(self.bp)
        self.net.recv((self.tag, "2m23"), self.size(2))
        self.hand(self.bm)

    def five(self):
        self.net.recv((self.tag, "2o"), self.size(4))
        self.hand(self.bo)


class Coarse:
    def __init__(self, net, piece, some, first, second, sibling):
        self.net, self.piece, self.some, self.first_axis, self.second_axis = net, piece, some, first, second
        self.sibling = sibling

    def send(self, key, a, device, total):
        self.net.send(
            key, lambda: (self.piece(a, self.second_axis[0]), self.piece(a, self.second_axis[0]), device),
            batch=key, total=lambda: total,
        )

    def first(self):
        for device in self.first_axis[4:]:
            self.send("p1", self.first_axis[0], device, self.some(1, 3))

    def second(self):
        self.net.recv("p1", self.some(1, 3))
        for device in self.second_axis[4:]:
            for a in self.first_axis[:4]:
                self.send("p2", a, device, self.some(3, 4))

    def third(self, mine):
        self.net.recv("p2", self.some(3, 4))
        self.net.send("p3", lambda: (mine, mine, self.sibling))

    def last(self, theirs):
        self.net.recv("p3", theirs)


def normed(values, gain):
    floats = values.astype(F32)
    mean = jnp.mean(floats * floats, axis=-1, keepdims=True)
    return (floats * lax.rsqrt(mean + EPS) * gain).astype(BF16)


def kernel(
    tok, g1, gate1, up1, down1, mixg, pool, scale, g2, gate2, up2, down2, out,
    w, pw, xt, xq, n, h1, h2, wd1, wd2, maps, own1, pm, pp, so, sm, sp, ra, rb, a1, hs, hr, mg, ob, sq, rq, base, rx, st, tokv, gu, part1,
    ss, rs, ls,
):
    rep = lax.axis_index("rep")
    fs = lax.axis_index("fs")
    c = lax.axis_index("tp")
    o = 1 - c
    j = lax.div(fs, 16)
    z = rep * 2 + j
    y = lax.rem(lax.div(fs, 4), 4)
    x = lax.rem(fs, 4)
    zp, zo, zm = (lax.rem(z + k, 4) for k in (1, 2, 3))
    yp, yo, ym = (lax.rem(y + k, 4) for k in (1, 2, 3))
    xp, xo, xm = (lax.rem(x + k, 4) for k in (1, 2, 3))

    def dev(z_, y_, x_, c_):
        return (lax.div(z_, 2), lax.rem(z_, 2) * 16 + y_ * 4 + x_, c_)

    sibling = dev(z, y, x, o)
    net = Net(ss, rs, ls, sibling)
    keeper = c == j
    taker = c != j
    zq = lax.rem(z + 1 + 2 * lax.rem(z + c, 2), 4)

    def cols(k):
        return pl.ds(pl.multiple_of(k * UNIT, 128), UNIT)

    def feats(k):
        return pl.ds(pl.multiple_of(k * HALF, 128), HALF)

    def rows(k):
        return pl.ds(pl.multiple_of(k * ROWS, 128), ROWS)

    mats = ((gate1, up1, down1), (gate2, up2, down2), (gate2, up2, down2))
    subs = (lax.div(z, 2), 0, 1)

    own_tok = net.local(tok.at[rows(c), :], xt.at[z, :, feats(c)])
    own_tok.start()
    own_w = [net.slot() for u in range(3)]
    own_p = net.slot()

    def own_pool():
        return pltpu.make_async_copy(pool, pw.at[c, c, y, x], own_p)

    stage_t = net.local(tok, tokv)
    stage_t.start()
    stage_w = [net.slot(), net.slot()]

    @pl.when(taker)
    def _():
        for k in range(2):
            for m in range(3):
                pltpu.make_async_copy(mats[k][m], st.at[k, m], stage_w[k]).start()

    @pl.when(keeper)
    def _():
        for u in range(3):
            for m in range(3):
                pltpu.make_async_copy(mats[u][m].at[:, cols(subs[u])], w.at[u, m, c, y, x], own_w[u]).start()
        own_pool().start()

    own_mg = net.local(mixg, mg.at[0, c])
    own_sc = net.local(scale, mg.at[1, c])
    own_mg.start()
    own_sc.start()

    barrier = pltpu.get_barrier_semaphore()
    friends = [dev(z, y, x_, c) for x_ in (xp, xm, xo)] + [dev(z, y_, x, c) for y_ in (yp, ym, yo)] + [sibling]
    friends += [dev(z_, y, x, k) for z_ in (zp, zm) for k in range(2)]
    for friend in friends:
        pl.semaphore_signal(barrier, inc=1, device_id=friend, device_id_type=MESH)
    pl.semaphore_wait(barrier, len(friends))

    def staged(k):
        @pl.when(taker)
        def _():
            pltpu.make_async_copy(st.at[k], st.at[k], stage_w[k]).wait()

    def exchange(u):
        for ab, z_ in ((0, zp), (1, zm)):
            sub = (lax.div(z_, 2), 0, 1)[u]
            part = pl.ds(16 * ab, 16)
            for m in range(3):
                net.send(
                    ("z", u),
                    lambda m=m, part=part, sub=sub, z_=z_: (
                        st.at[min(u, 1), m, part, cols(sub)],
                        w.at[u, m, o, y, x, part, :],
                        dev(z_, y, x, o),
                    ),
                    cond=taker,
                    batch=("z", u),
                    total=lambda: w.at[u, :, 0, 0, 0],
                )

    def own(u):
        ref = w.at[u, :, c, y, x]

        @pl.when(keeper)
        def _():
            pltpu.make_async_copy(ref, ref, own_w[u]).wait()

        @pl.when(taker)
        def _():
            net.recv(("z", u), ref)

    in_x = (x, xp, xm, xo, dev(z, y, xp, c), dev(z, y, xm, c), dev(z, y, xo, c))
    in_y = (y, yp, ym, yo, dev(z, yp, x, c), dev(z, ym, x, c), dev(z, yo, x, c))
    two, top, low = pl.ds(0, 2), pl.ds(0, 16), pl.ds(16, 16)

    def size_w(k):
        return {
            2: w.at[0, :, 0, two, 0, top],
            4: w.at[0, :, 0, :, 0, top],
            8: w.at[0, :, 0, two, :, top],
            16: w.at[0, :, 0, :, :, top],
            32: w.at[0, :, 0],
        }[k]

    def stream_a(u):
        return Stream(
            net, u, "a", DIRECT and u == 0,
            lambda a, b: w.at[u, :, c, b, a, top, :],
            lambda b: w.at[u, :, c, b, :, top, :],
            size_w, 2, in_x, in_y, sibling,
        )

    def stream_b(u):
        return Stream(
            net, u, "b", DIRECT and u == 0,
            lambda a, b: w.at[u, :, c, a, b, low, :],
            lambda b: w.at[u, :, c, :, b, low, :],
            size_w, 2, in_y, in_x, sibling,
        )

    sa = [stream_a(u) for u in range(3)]
    sb = [stream_b(u) for u in range(3)]
    def pick(k, l):
        return k * o + l * c

    xs, ys = (x, xp, xm, xo), (y, yp, ym, yo)
    first = [pick(k, l) for k, l in zip(xs, ys)]
    second = [pick(l, k) for k, l in zip(xs, ys)]
    first += [dev(z, pick(y, l), pick(k, x), c) for k, l in zip(xs[1:], ys[1:])]
    second += [dev(z, pick(l, y), pick(x, k), c) for k, l in zip(xs[1:], ys[1:])]
    spool = Coarse(
        net, lambda a, b: pw.at[:, c, pick(b, a), pick(a, b)], lambda k, l: pw.at[:, 0, pl.ds(0, k), pl.ds(0, l)],
        first, second, sibling,
    )

    def start(u):
        own(u)
        sa[u].one()
        sb[u].one()
        sa[u].then()
        sb[u].then()

    def handed(u):
        net.recv((u, "d"), w.at[u, :, o])

    def spread_tokens(tag, cond):
        for k in range(2):
            for key, z_ in (("tm", zp), ("tp", zm)):
                net.send(
                    key,
                    lambda k=k, z_=z_: (tokv.at[rows(k), :], xt.at[z, :, feats(c)], dev(z_, y, x, k)),
                    cond=cond, width=2, shift=c, batch=("t4", tag), total=lambda: xt.at[pl.ds(0, 2)],
                )
        net.send("ts", lambda: (tokv.at[rows(o), :], xt.at[z, :, feats(c)], sibling), cond=cond)

    def relay_tokens():
        for key, who, half, to in (("tm", zm, 0, zp), ("tp", zp, 1, zm)):
            net.recv(key, xt.at[who, :, feats(half)], half, 2)
            net.send(
                "to",
                lambda who=who, half=half, to=to: (
                    xt.at[who, :, feats(half)], xt.at[who, :, feats(half)], dev(to, y, x, c)
                ),
                batch="t2", total=lambda: xt.at[0],
            )
        net.recv("tm", xt.at[zm, :, feats(1)], 1, 2)
        net.recv("tp", xt.at[zp, :, feats(0)], 0, 2)

    def dot(lhs, rhs):
        return jnp.dot(lhs, rhs, preferred_element_type=F32)

    def gate_up(u, at, count, put):
        for k in range(UNIT // 128):
            part = pl.ds(k * 128, 128)
            wg = w[u, 0, :, :, :, :, part].reshape(D, 128)
            wu = w[u, 1, :, :, :, :, part].reshape(D, 128)
            both = jnp.dot(
                n[pl.ds(at, count), :], jnp.concatenate([wg, wu], axis=1), preferred_element_type=F32
            )
            gate, up = both[:, :128], both[:, 128:]
            put(k * 128, (gate * jax.nn.sigmoid(gate) * up).astype(BF16))

    def put1(at, count):
        def put(k, value):
            h1[pl.ds(at, count), pl.ds(k, 128)] = value

        return put

    def put2(at, count, first):
        def put(k, value):
            h2[pl.ds(at, count), pl.ds(first + k, 128)] = value

        return put

    def gate_up_half(u, at, count, part, put=None):
        lanes = feats(part)
        for k in range(UNIT // 128):
            hid = pl.ds(k * 128, 128)
            wg = w[u, 0, part, :, :, :, hid].reshape(HALF, 128)
            wu = w[u, 1, part, :, :, :, hid].reshape(HALF, 128)
            both = dot(n[pl.ds(at, count), lanes], jnp.concatenate([wg, wu], axis=1))
            if put is None:
                gu[:, pl.ds(k * 256, 256)] = both
            else:
                both = both + gu[:, pl.ds(k * 256, 256)]
                gate, up = both[:, :128], both[:, 128:]
                put(k * 128, (gate * jax.nn.sigmoid(gate) * up).astype(BF16))

    def turn(u, part, wide, at):
        for k in range(2):
            block = w[u, 2, part, 2 * k : 2 * k + 2].reshape(256, UNIT)
            wide[pl.ds(at, UNIT), pl.ds(pl.multiple_of(part * HALF + 256 * k, 128), 256)] = block.T

    def start_pool():
        @pl.when(keeper)
        def _():
            own_pool().wait()
            net.recv("ps", pw.at[o, c, y, x])

        @pl.when(taker)
        def _():
            net.recv("pz", pw.at[0, c, y, x], 0, 2)
            net.recv("pz", pw.at[1, c, y, x], 1, 2)

        spool.first()

    def norm_own():
        own_tok.wait()
        net.recv("ts", xt.at[z, :, feats(o)])
        n[pl.ds(0, ROWS), :] = normed(xt[z], gain1)

    def norm_next():
        n[pl.ds(ROWS, ROWS), :] = normed(xt[zm], gain1)
        n[pl.ds(2 * ROWS, ROWS), :] = normed(xt[zp], gain1)

    def norm_last():
        net.recv("to", xt.at[zo])
        n[pl.ds(3 * ROWS, ROWS), :] = normed(xt[zo], gain1)

    def first_near():
        turn(0, c, wd1, 0)
        gate_up_half(0, 3 * ROWS, ROWS, c)

    def first_opposite():
        gate_up_half(0, 3 * ROWS, ROWS, o, put1(3 * ROWS, ROWS))
        turn(0, o, wd1, 0)
        for k, z_ in ((0, zp), (1, zm)):
            lanes = slice(HALF * k, HALF * k + HALF)
            so[:, lanes] = dot(h1[pl.ds(3 * ROWS, ROWS), :], wd1[:, lanes]).astype(BF16)
            net.send(
                f"r{k}", lambda k=k, z_=z_: (so.at[:, feats(k)], ra.at[k], dev(z_, y, x, c)), batch="r", total=lambda: so
            )

    def pass_on(key, buf, k, half, z_):
        net.send(
            f"{key}{half}",
            lambda: (buf.at[:, feats(half)], rb.at[k, :, feats(half)], dev(z_, y, x, c)),
            batch="q", total=lambda: xt.at[two],
        )

    def first_neighbours():
        gate_up(0, ROWS, 2 * ROWS, put1(ROWS, 2 * ROWS))
        sums = dot(h1[pl.ds(ROWS, 2 * ROWS), :], wd1[...])
        sm[:, :HALF] = sums[:ROWS, :HALF].astype(BF16)
        sp[:, HALF:] = sums[ROWS:, HALF:].astype(BF16)
        pm[...] = sums[:ROWS, HALF:]
        pp[...] = sums[ROWS:, :HALF]
        pass_on("qm", sp, 0, 1, zp)
        pass_on("qp", sm, 1, 0, zm)

    def first_own():
        gate_up(0, 0, ROWS, put1(0, ROWS))
        own1[...] = dot(h1[pl.ds(0, ROWS), :], wd1[...])

    def first_pass_on():
        net.recv("r0", ra.at[0])
        sp[:, :HALF] = (pp[...] + ra[0].astype(F32)).astype(BF16)
        pass_on("qm", sp, 0, 0, zp)
        net.recv("r1", ra.at[1])
        sm[:, HALF:] = (pm[...] + ra[1].astype(F32)).astype(BF16)
        pass_on("qp", sm, 1, 1, zm)

    def pool_maps():
        spool.last(pw.at[:, o])
        for g in range(4):
            wide = pw[g // 2].reshape(32, 16, 256).astype(F32)
            maps[g] = wide[:, 8 * (g % 2) : 8 * (g % 2) + 8, :].reshape(256, 256).astype(BF16).T

    def joined(k):
        return jnp.concatenate([mg[k, 0], mg[k, 1]], axis=1)

    def first_sum():
        for key, k, half in (("qm", 0, 1), ("qp", 1, 0), ("qm", 0, 0), ("qp", 1, 1)):
            net.recv(f"{key}{half}", rb.at[k, :, feats(half)])
        net.recv("mg", mg.at[:, o])

    def halo():
        for part in (slice(ROWS - 16, ROWS), slice(0, ROWS - 16)):
            block = own1[part] + rb[0, part].astype(F32) + rb[1, part].astype(F32)
            value = (xt[z, part].astype(F32) + 0.5 * block).astype(BF16)
            a1[part] = value
            hs[part] = normed(value, joined(0))
            if part.start:
                net.send("h", lambda: (hs.at[pl.ds(112, 16), :], hr, sibling))

    def mix():
        mix_scale = joined(1)
        for start in (64, 0):
            part = slice(start, start + 64)
            if start:
                longer = hs[48:ROWS].astype(F32)
            else:
                net.recv("h", hr)
                before = jnp.where(c == 1, hr[...].astype(F32), 0.0)
                longer = jnp.concatenate([before, hs[:64].astype(F32)], axis=0)
            positions = c * ROWS + start + lax.broadcasted_iota(jnp.int32, (64, 256), 0)
            for g in range(4):
                lanes = slice(256 * g, 256 * g + 256)
                total = longer[:, lanes]
                for k in range(g + 1):
                    total = total + pltpu.roll(total, 2**k, axis=0)
                counts = jnp.minimum(positions + 1, 2 ** (g + 1)).astype(F32)
                diff = (total[16:] / counts - longer[16:, lanes]).astype(BF16)
                mixed = dot(diff, maps[g])
                after = a1[part, lanes].astype(F32) + mixed * mix_scale[:, lanes]
                ob[part, lanes] = after.astype(BF16)
            half = pl.ds(start, 64)
            net.send(
                "a", lambda half=half: (ob.at[half], xq.at[half], dev(zq, y, x, c)), batch="a", total=lambda: ob
            )

    def second_norm():
        n[pl.ds(0, ROWS), :] = normed(ob[...], gain2)

    def second_own_1():
        turn(1, 0, wd2, 0)
        turn(1, 1, wd2, 0)
        gate_up(1, 0, ROWS, put2(0, ROWS, 0))

    def second_peer_1():
        net.recv("a", xq)
        n[pl.ds(ROWS, ROWS), :] = normed(xq[...], gain2)
        gate_up(1, ROWS, ROWS, put2(ROWS, ROWS, 0))
        part1[...] = dot(h2[pl.ds(ROWS, ROWS), :UNIT], wd2[:UNIT])

    def second_near():
        turn(2, c, wd2, UNIT)
        gate_up_half(2, ROWS, ROWS, c)

    def second_peer_2():
        gate_up_half(2, ROWS, ROWS, o, put2(ROWS, ROWS, UNIT))
        turn(2, o, wd2, UNIT)
        for k in range(2):
            lanes = slice(HALF * k, HALF * k + HALF)
            sq[:, lanes] = (part1[:, lanes] + dot(h2[pl.ds(ROWS, ROWS), UNIT:], wd2[UNIT:, lanes])).astype(BF16)
            net.send(
                "b",
                lambda k=k: (sq.at[:, feats(k)], rq.at[c], dev(zq, y, x, k)),
                width=2, shift=c, batch="b", total=lambda: sq,
            )

    def second_own_2():
        gate_up(2, 0, ROWS, put2(0, ROWS, UNIT))
        base[...] = ob[...].astype(F32) + 0.5 * dot(h2[pl.ds(0, ROWS), :], wd2[...])
        net.send("f", lambda: (base.at[:, feats(o)], rx, sibling))

    def last_sum():
        net.recv("f", rx)
        net.recv("b", rq.at[c], c, 2)
        out[rows(c), :] = (base[:, feats(c)] + 0.5 * rq[c].astype(F32)).astype(BF16)
        net.recv("b", rq.at[o], o, 2)
        out[rows(o), :] = (rx[...] + 0.5 * rq[o].astype(F32)).astype(BF16)

    staged(0)
    exchange(0)
    stage_t.wait()
    staged(1)
    exchange(1)
    spread_tokens(0, taker)
    start(0)
    start(1)
    exchange(2)
    net.send("ps", lambda: (pool, pw.at[c, o, y, x], sibling), cond=taker)
    net.send("pz", lambda: (pool, pw.at[c, j, y, x], dev(zp, y, x, j)), width=2, shift=c)
    own_mg.wait()
    own_sc.wait()
    net.send("mg", lambda: (mixg, mg.at[0, c], sibling), batch="mg", total=lambda: mg.at[:, 0])
    net.send("mg", lambda: (scale, mg.at[1, c], sibling), batch="mg", total=lambda: mg.at[:, 0])
    gain1 = g1[...]
    gain2 = g2[...]
    sa[0].two()
    sb[0].two()
    sa[0].pre()
    sb[0].pre()
    spread_tokens(1, keeper)
    sa[0].three()
    sb[0].three()
    relay_tokens()
    sa[0].mid()
    sb[0].mid()
    sa[0].four()
    sb[0].four()
    start_pool()
    start(2)
    norm_own()
    norm_next()
    norm_last()
    sa[0].five()
    sb[0].five()
    first_near()
    sa[1].two()
    sb[1].two()
    spool.second()
    handed(0)
    first_opposite()
    sa[2].two()
    sb[2].two()
    first_neighbours()
    sa[1].pre()
    sb[1].pre()
    first_own()
    sa[1].three()
    sb[1].three()
    sa[1].mid()
    sb[1].mid()
    first_pass_on()
    sa[2].three()
    sb[2].three()
    sa[2].pre()
    sb[2].pre()
    spool.third(pw.at[:, c])
    sa[1].four()
    sb[1].four()
    sa[2].mid()
    sb[2].mid()
    pool_maps()
    first_sum()
    halo()
    mix()
    sa[1].five()
    sb[1].five()
    sa[2].four()
    sb[2].four()
    second_norm()
    handed(1)
    second_own_1()
    sa[2].five()
    sb[2].five()
    second_peer_1()
    second_near()
    handed(2)
    second_peer_2()
    second_own_2()
    last_sum()
    net.finish()


def local(tok, g1, gate1, up1, down1, mixg, pool, scale, g2, gate2, up2, down2):
    hbm = pl.BlockSpec(memory_space=pl.ANY)
    vmem = pl.BlockSpec(memory_space=pltpu.VMEM)
    result = pl.pallas_call(
        kernel,
        out_shape=pltpu.VMEM((256, HALF), BF16),
        in_specs=[hbm, vmem, hbm, hbm, hbm, hbm, hbm, hbm, vmem, hbm, hbm, hbm],
        out_specs=vmem,
        scratch_shapes=[
            pltpu.VMEM((3, 3, 2, 4, 4, 32, UNIT), BF16),
            pltpu.VMEM((2, 2, 4, 4, 16, 256), BF16),
            pltpu.VMEM((4, ROWS, D), BF16),
            pltpu.VMEM((ROWS, D), BF16),
            pltpu.VMEM((4 * ROWS, D), BF16),
            pltpu.VMEM((4 * ROWS, UNIT), BF16),
            pltpu.VMEM((2 * ROWS, 2 * UNIT), BF16),
            pltpu.VMEM((UNIT, D), BF16),
            pltpu.VMEM((2 * UNIT, D), BF16),
            pltpu.VMEM((4, 256, 256), BF16),
            pltpu.VMEM((ROWS, D), F32),
            pltpu.VMEM((ROWS, HALF), F32),
            pltpu.VMEM((ROWS, HALF), F32),
            pltpu.VMEM((ROWS, D), BF16),
            pltpu.VMEM((ROWS, D), BF16),
            pltpu.VMEM((ROWS, D), BF16),
            pltpu.VMEM((2, ROWS, HALF), BF16),
            pltpu.VMEM((2, ROWS, D), BF16),
            pltpu.VMEM((ROWS, D), BF16),
            pltpu.VMEM((ROWS, D), BF16),
            pltpu.VMEM((16, D), BF16),
            pltpu.VMEM((2, 2, 1, HALF), F32),
            pltpu.VMEM((ROWS, D), BF16),
            pltpu.VMEM((ROWS, D), BF16),
            pltpu.VMEM((2, ROWS, HALF), BF16),
            pltpu.VMEM((ROWS, D), F32),
            pltpu.VMEM((ROWS, HALF), F32),
            pltpu.VMEM((2, 3, 32, 1280), BF16),
            pltpu.VMEM((256, HALF), BF16),
            pltpu.VMEM((ROWS, 2 * UNIT), F32),
            pltpu.VMEM((ROWS, D), F32),
            pltpu.SemaphoreType.DMA((N_SEND,)),
            pltpu.SemaphoreType.DMA((N_RECV,)),
            pltpu.SemaphoreType.DMA((N_LOCAL,)),
        ],
        compiler_params=pltpu.CompilerParams(collective_id=0, has_side_effects=True, vmem_limit_bytes=52 * 2**20),
    )(
        *(
            pltpu.with_memory_space_constraint(value, pltpu.HBM)
            for value in (
                tok.reshape(256, HALF), g1.reshape(1, D), gate1, up1, down1.T, mixg.reshape(1, HALF),
                pool.transpose(0, 2, 1).reshape(16, 256), scale.reshape(1, HALF), g2.reshape(1, D), gate2, up2, down2.T,
            )
        )
    )
    return result.reshape(1, 256, HALF)


def solution(mesh):
    placed = (
        P(("rep", "fs"), None, "tp"),
        P(),
        P("fs", "tp"),
        P("fs", "tp"),
        P("tp", "fs"),
        P("tp"),
        P("tp", None, "fs"),
        P("tp"),
        P(),
        P("fs", "tp"),
        P("fs", "tp"),
        P("tp", "fs"),
    )
    return jax.shard_map(
        local, mesh=mesh, in_specs=placed, out_specs=P(("rep", "fs"), None, "tp"), check_vma=False
    )
```

```python
import jax
import jax.numpy as jnp
from jax import lax
from jax.experimental import pallas as pl
from jax.experimental.pallas import tpu as pltpu
from jax.sharding import PartitionSpec as P

MESH = pl.DeviceIdType.MESH
BF16 = jnp.bfloat16
F32 = jnp.float32
EPS = 1e-06
D = 1024
HALF = 512
ROWS = 128
UNIT = 640
DIRECT = False
N_SEND = 23
N_RECV = 84
N_LOCAL = 10


class Net:
    def __init__(self, ss, rs, ls, here):
        self.ss, self.rs, self.ls, self.here = ss, rs, ls, here
        self.names = {}
        self.batches = {}
        self.locals = 0
        self.sends = 0
        self.pending = []

    def name(self, key, width=1):
        if key not in self.names:
            self.names[key] = sum(w for _, w in self.names.values()), width
        return self.names[key][0]

    def send(self, key, make, cond=None, width=1, shift=None, batch=None, total=None):
        base = self.name(key, width)
        first = batch is None or batch not in self.batches
        if first:
            slot = self.sends
            self.sends += 1
            if batch is not None:
                self.batches[batch] = slot
        else:
            slot = self.batches[batch]

        def copy(src, dst, device):
            where = base if shift is None else base + shift
            return pltpu.make_async_remote_copy(
                src, dst, self.ss.at[slot], self.rs.at[where], device_id=device, device_id_type=MESH
            )

        def end():
            ref = make()[0] if total is None else total()
            copy(ref, ref, self.here).wait_send()

        if cond is None:
            copy(*make()).start()
        else:
            pl.when(cond)(lambda: copy(*make()).start())
        if first:
            self.pending.append(end if cond is None else lambda: pl.when(cond)(end))

    def recv(self, key, ref, offset=0, width=1):
        where = self.name(key, width) + offset
        pltpu.make_async_remote_copy(
            ref, ref, self.ss.at[0], self.rs.at[where], device_id=self.here, device_id_type=MESH
        ).wait_recv()

    def slot(self):
        self.locals += 1
        return self.ls.at[self.locals - 1]

    def local(self, src, dst):
        return pltpu.make_async_copy(src, dst, self.slot())

    def finish(self):
        for end in self.pending:
            end()
        assert self.sends == N_SEND and self.locals == N_LOCAL
        assert sum(w for _, w in self.names.values()) == N_RECV


class Stream:
    def __init__(self, net, unit, tag, direct, piece, group, size, size_all, first, second, sibling):
        self.net, self.unit, self.tag, self.direct = net, unit, (unit, tag), direct
        self.piece, self.group, self.size, self.size_all = piece, group, size, size_all
        self.a, self.ap, self.am, self.ao, self.to_ap, self.to_am, self.to_ao = first
        self.b, self.bp, self.bm, self.bo, self.to_bp, self.to_bm, self.to_bo = second
        self.sibling = sibling
        self.flip = unit == 2

    def send(self, what, a, b, device, kind, count):
        self.net.send(
            (self.tag, what),
            lambda: (self.piece(a, b), self.piece(a, b), device),
            batch=kind,
            total=lambda: self.size_all(count),
        )

    def recv(self, what, a, b):
        self.net.recv((self.tag, what), self.piece(a, b))

    def both(self, k, a):
        late_m, late_p = ("2x" if k >= 2 else f"2m{k}"), ("2x" if k < 2 else f"2p{k}")
        self.send(late_m, a, self.b, self.to_bp, "both", 8)
        self.send(late_p, a, self.b, self.to_bm, "both", 8)

    def hand(self, b):
        self.net.send(
            (self.unit, "d"),
            lambda: (self.group(b), self.group(b), self.sibling),
            batch="hand",
            total=lambda: self.size_all(16),
        )

    def one(self):
        self.send("1m", self.a, self.b, self.to_ap, "ring", 2)
        self.send("1p", self.a, self.b, self.to_am, "ring", 2)
        if self.direct:
            self.send("1o", self.a, self.b, self.to_ao, "far", 1)

    def then(self):
        self.both(0, self.a)

    def two(self):
        for key, k, a, to in (("1p", 2, self.ap, self.to_am), ("1m", 1, self.am, self.to_ap))[:: -1 if self.flip else 1]:
            self.recv(key, a, self.b)
            if key == ("1m" if self.flip else "1p") and not self.direct:
                self.send("1o", a, self.b, to, "far", 1)
            self.both(k, a)

    def three(self):
        self.recv("1o", self.ao, self.b)
        self.both(3, self.ao)
        self.hand(self.b)

    def pre(self):
        self.recv("2m0", self.a, self.bm)
        self.send("2o", self.a, self.bm, self.to_bp, "on", 4)

    def mid(self):
        self.recv("2m1", self.am, self.bm)
        self.send("2o", self.am, self.bm, self.to_bp, "on", 4)
        self.recv("2p2", self.ap, self.bp)
        self.send("2o", self.ap, self.bp, self.to_bm, "on", 4)

    def four(self):
        self.recv("2p3", self.ao, self.bp)
        self.send("2o", self.ao, self.bp, self.to_bm, "on", 4)
        self.net.recv((self.tag, "2x"), self.size(4))
        self.hand(self.bp)
        self.hand(self.bm)

    def five(self):
        self.net.recv((self.tag, "2o"), self.size(4))
        self.hand(self.bo)


class Coarse:
    def __init__(self, net, piece, some, first, second, sibling):
        self.net, self.piece, self.some, self.first_axis, self.second_axis = net, piece, some, first, second
        self.sibling = sibling

    def send(self, key, a, device, total):
        self.net.send(
            key, lambda: (self.piece(a, self.second_axis[0]), self.piece(a, self.second_axis[0]), device),
            batch=key, total=lambda: total,
        )

    def first(self):
        for device in self.first_axis[4:]:
            self.send("p1", self.first_axis[0], device, self.some(1, 3))

    def second(self):
        self.net.recv("p1", self.some(1, 3))
        for device in self.second_axis[4:]:
            for a in self.first_axis[:4]:
                self.send("p2", a, device, self.some(3, 4))

    def third(self, mine):
        self.net.recv("p2", self.some(3, 4))
        self.net.send("p3", lambda: (mine, mine, self.sibling))

    def last(self, theirs):
        self.net.recv("p3", theirs)


def normed(values, gain):
    floats = values.astype(F32)
    mean = jnp.mean(floats * floats, axis=-1, keepdims=True)
    return (floats * lax.rsqrt(mean + EPS) * gain).astype(BF16)


def kernel(
    tok, g1, gate1, up1, down1, mixg, pool, scale, g2, gate2, up2, down2, out,
    w, pw, xt, xq, n, h1, h2, wd1, wd2, maps, own1, pm, pp, so, sm, sp, ra, rb, a1, hs, hr, mg, ob, sq, rq, base, rx, st, tokv, gu, part1,
    ss, rs, ls,
):
    rep = lax.axis_index("rep")
    fs = lax.axis_index("fs")
    c = lax.axis_index("tp")
    o = 1 - c
    j = lax.div(fs, 16)
    z = rep * 2 + j
    y = lax.rem(lax.div(fs, 4), 4)
    x = lax.rem(fs, 4)
    zp, zo, zm = (lax.rem(z + k, 4) for k in (1, 2, 3))
    yp, yo, ym = (lax.rem(y + k, 4) for k in (1, 2, 3))
    xp, xo, xm = (lax.rem(x + k, 4) for k in (1, 2, 3))

    def dev(z_, y_, x_, c_):
        return (lax.div(z_, 2), lax.rem(z_, 2) * 16 + y_ * 4 + x_, c_)

    sibling = dev(z, y, x, o)
    net = Net(ss, rs, ls, sibling)
    keeper = c == j
    taker = c != j
    zq = lax.rem(z + 1 + 2 * lax.rem(z + c, 2), 4)

    def cols(k):
        return pl.ds(pl.multiple_of(k * UNIT, 128), UNIT)

    def feats(k):
        return pl.ds(pl.multiple_of(k * HALF, 128), HALF)

    def rows(k):
        return pl.ds(pl.multiple_of(k * ROWS, 128), ROWS)

    mats = ((gate1, up1, down1), (gate2, up2, down2), (gate2, up2, down2))
    subs = (lax.div(z, 2), 0, 1)

    own_tok = net.local(tok.at[rows(c), :], xt.at[z, :, feats(c)])
    own_tok.start()
    own_w = [net.slot() for u in range(3)]
    own_p = net.slot()

    def own_pool():
        return pltpu.make_async_copy(pool, pw.at[c, c, y, x], own_p)

    stage_t = net.local(tok, tokv)
    stage_t.start()
    stage_w = [net.slot(), net.slot()]

    @pl.when(taker)
    def _():
        for k in range(2):
            for m in range(3):
                pltpu.make_async_copy(mats[k][m], st.at[k, m], stage_w[k]).start()

    @pl.when(keeper)
    def _():
        for u in range(3):
            for m in range(3):
                pltpu.make_async_copy(mats[u][m].at[:, cols(subs[u])], w.at[u, m, c, y, x], own_w[u]).start()
        own_pool().start()

    own_mg = net.local(mixg, mg.at[0, c])
    own_sc = net.local(scale, mg.at[1, c])
    own_mg.start()
    own_sc.start()

    barrier = pltpu.get_barrier_semaphore()
    friends = [dev(z, y, x_, c) for x_ in (xp, xm, xo)] + [dev(z, y_, x, c) for y_ in (yp, ym, yo)] + [sibling]
    friends += [dev(z_, y, x, k) for z_ in (zp, zm) for k in range(2)]
    for friend in friends:
        pl.semaphore_signal(barrier, inc=1, device_id=friend, device_id_type=MESH)
    pl.semaphore_wait(barrier, len(friends))

    def staged(k):
        @pl.when(taker)
        def _():
            pltpu.make_async_copy(st.at[k], st.at[k], stage_w[k]).wait()

    def exchange(u):
        for ab, z_ in ((0, zp), (1, zm)):
            sub = (lax.div(z_, 2), 0, 1)[u]
            part = pl.ds(16 * ab, 16)
            for m in range(3):
                net.send(
                    ("z", u),
                    lambda m=m, part=part, sub=sub, z_=z_: (
                        st.at[min(u, 1), m, part, cols(sub)],
                        w.at[u, m, o, y, x, part, :],
                        dev(z_, y, x, o),
                    ),
                    cond=taker,
                    batch="z",
                    total=lambda: w.at[:, :, 0, 0, 0],
                )

    def own(u):
        ref = w.at[u, :, c, y, x]

        @pl.when(keeper)
        def _():
            pltpu.make_async_copy(ref, ref, own_w[u]).wait()

        @pl.when(taker)
        def _():
            net.recv(("z", u), ref)

    in_x = (x, xp, xm, xo, dev(z, y, xp, c), dev(z, y, xm, c), dev(z, y, xo, c))
    in_y = (y, yp, ym, yo, dev(z, yp, x, c), dev(z, ym, x, c), dev(z, yo, x, c))
    two, top, low = pl.ds(0, 2), pl.ds(0, 16), pl.ds(16, 16)

    def size_w(k):
        return {2: w.at[0, :, 0, two, 0, top], 4: w.at[0, :, 0, :, 0, top]}[k]

    def size_all(k):
        return {
            1: w.at[:, :, 0, two, 0, top],
            2: w.at[:, :, 0, :, 0, top],
            4: w.at[:, :, 0, two, :, top],
            8: w.at[:, :, 0, :, :, top],
            16: w.at[:, :, 0],
        }[k]

    def stream_a(u):
        return Stream(
            net, u, "a", DIRECT and u == 0,
            lambda a, b: w.at[u, :, c, b, a, top, :],
            lambda b: w.at[u, :, c, b, :, top, :],
            size_w, size_all, in_x, in_y, sibling,
        )

    def stream_b(u):
        return Stream(
            net, u, "b", DIRECT and u == 0,
            lambda a, b: w.at[u, :, c, a, b, low, :],
            lambda b: w.at[u, :, c, :, b, low, :],
            size_w, size_all, in_y, in_x, sibling,
        )

    sa = [stream_a(u) for u in range(3)]
    sb = [stream_b(u) for u in range(3)]
    def pick(k, l):
        return k * o + l * c

    xs, ys = (x, xp, xm, xo), (y, yp, ym, yo)
    first = [pick(k, l) for k, l in zip(xs, ys)]
    second = [pick(l, k) for k, l in zip(xs, ys)]
    first += [dev(z, pick(y, l), pick(k, x), c) for k, l in zip(xs[1:], ys[1:])]
    second += [dev(z, pick(l, y), pick(x, k), c) for k, l in zip(xs[1:], ys[1:])]
    spool = Coarse(
        net, lambda a, b: pw.at[:, c, pick(b, a), pick(a, b)], lambda k, l: pw.at[:, 0, pl.ds(0, k), pl.ds(0, l)],
        first, second, sibling,
    )

    def start(u):
        own(u)
        sa[u].one()
        sb[u].one()
        sa[u].then()
        sb[u].then()

    def handed(u):
        net.recv((u, "d"), w.at[u, :, o])

    def spread_tokens(tag, cond):
        for k in range(2):
            for key, z_ in (("tm", zp), ("tp", zm)):
                net.send(
                    key,
                    lambda k=k, z_=z_: (tokv.at[rows(k), :], xt.at[z, :, feats(c)], dev(z_, y, x, k)),
                    cond=cond, width=2, shift=c, batch=("t4", tag), total=lambda: xt.at[pl.ds(0, 2)],
                )
        net.send("ts", lambda: (tokv.at[rows(o), :], xt.at[z, :, feats(c)], sibling), cond=cond)

    def relay_tokens():
        for key, who, half, to in (("tm", zm, 0, zp), ("tp", zp, 1, zm)):
            net.recv(key, xt.at[who, :, feats(half)], half, 2)
            net.send(
                "to",
                lambda who=who, half=half, to=to: (
                    xt.at[who, :, feats(half)], xt.at[who, :, feats(half)], dev(to, y, x, c)
                ),
                batch="t2", total=lambda: xt.at[0],
            )
        net.recv("tm", xt.at[zm, :, feats(1)], 1, 2)
        net.recv("tp", xt.at[zp, :, feats(0)], 0, 2)

    def dot(lhs, rhs):
        return jnp.dot(lhs, rhs, preferred_element_type=F32)

    def gate_up(u, at, count, put):
        for k in range(UNIT // 128):
            part = pl.ds(k * 128, 128)
            wg = w[u, 0, :, :, :, :, part].reshape(D, 128)
            wu = w[u, 1, :, :, :, :, part].reshape(D, 128)
            both = jnp.dot(
                n[pl.ds(at, count), :], jnp.concatenate([wg, wu], axis=1), preferred_element_type=F32
            )
            gate, up = both[:, :128], both[:, 128:]
            put(k * 128, (gate * jax.nn.sigmoid(gate) * up).astype(BF16))

    def put1(at, count):
        def put(k, value):
            h1[pl.ds(at, count), pl.ds(k, 128)] = value

        return put

    def put2(at, count, first):
        def put(k, value):
            h2[pl.ds(at, count), pl.ds(first + k, 128)] = value

        return put

    def gate_up_half(u, at, count, part, put=None):
        lanes = feats(part)
        for k in range(UNIT // 128):
            hid = pl.ds(k * 128, 128)
            wg = w[u, 0, part, :, :, :, hid].reshape(HALF, 128)
            wu = w[u, 1, part, :, :, :, hid].reshape(HALF, 128)
            both = dot(n[pl.ds(at, count), lanes], jnp.concatenate([wg, wu], axis=1))
            if put is None:
                gu[:, pl.ds(k * 256, 256)] = both
            else:
                both = both + gu[:, pl.ds(k * 256, 256)]
                gate, up = both[:, :128], both[:, 128:]
                put(k * 128, (gate * jax.nn.sigmoid(gate) * up).astype(BF16))

    def turn(u, part, wide, at):
        for k in range(2):
            block = w[u, 2, part, 2 * k : 2 * k + 2].reshape(256, UNIT)
            wide[pl.ds(at, UNIT), pl.ds(pl.multiple_of(part * HALF + 256 * k, 128), 256)] = block.T

    def start_pool():
        @pl.when(keeper)
        def _():
            own_pool().wait()
            net.recv("ps", pw.at[o, c, y, x])

        @pl.when(taker)
        def _():
            net.recv("pz", pw.at[0, c, y, x], 0, 2)
            net.recv("pz", pw.at[1, c, y, x], 1, 2)

        spool.first()

    def norm_own():
        own_tok.wait()
        net.recv("ts", xt.at[z, :, feats(o)])
        n[pl.ds(0, ROWS), :] = normed(xt[z], gain1)

    def norm_next():
        n[pl.ds(ROWS, ROWS), :] = normed(xt[zm], gain1)
        n[pl.ds(2 * ROWS, ROWS), :] = normed(xt[zp], gain1)

    def norm_last():
        net.recv("to", xt.at[zo])
        n[pl.ds(3 * ROWS, ROWS), :] = normed(xt[zo], gain1)

    def first_near():
        turn(0, c, wd1, 0)
        gate_up_half(0, 3 * ROWS, ROWS, c)

    def first_opposite():
        gate_up_half(0, 3 * ROWS, ROWS, o, put1(3 * ROWS, ROWS))
        turn(0, o, wd1, 0)
        for k, z_ in ((0, zp), (1, zm)):
            lanes = slice(HALF * k, HALF * k + HALF)
            so[:, lanes] = dot(h1[pl.ds(3 * ROWS, ROWS), :], wd1[:, lanes]).astype(BF16)
            net.send(
                f"r{k}", lambda k=k, z_=z_: (so.at[:, feats(k)], ra.at[k], dev(z_, y, x, c)), batch="r", total=lambda: so
            )

    def pass_on(key, buf, k, half, z_):
        net.send(
            f"{key}{half}",
            lambda: (buf.at[:, feats(half)], rb.at[k, :, feats(half)], dev(z_, y, x, c)),
            batch="q", total=lambda: xt.at[two],
        )

    def first_neighbours():
        gate_up(0, ROWS, 2 * ROWS, put1(ROWS, 2 * ROWS))
        sums = dot(h1[pl.ds(ROWS, 2 * ROWS), :], wd1[...])
        sm[:, :HALF] = sums[:ROWS, :HALF].astype(BF16)
        sp[:, HALF:] = sums[ROWS:, HALF:].astype(BF16)
        pm[...] = sums[:ROWS, HALF:]
        pp[...] = sums[ROWS:, :HALF]
        pass_on("qm", sp, 0, 1, zp)
        pass_on("qp", sm, 1, 0, zm)

    def first_own():
        gate_up(0, 0, ROWS, put1(0, ROWS))
        own1[...] = dot(h1[pl.ds(0, ROWS), :], wd1[...])

    def first_pass_on():
        net.recv("r0", ra.at[0])
        sp[:, :HALF] = (pp[...] + ra[0].astype(F32)).astype(BF16)
        pass_on("qm", sp, 0, 0, zp)
        net.recv("r1", ra.at[1])
        sm[:, HALF:] = (pm[...] + ra[1].astype(F32)).astype(BF16)
        pass_on("qp", sm, 1, 1, zm)

    def pool_maps():
        spool.last(pw.at[:, o])
        for g in range(4):
            wide = pw[g // 2].reshape(32, 16, 256).astype(F32)
            maps[g] = wide[:, 8 * (g % 2) : 8 * (g % 2) + 8, :].reshape(256, 256).astype(BF16).T

    def joined(k):
        return jnp.concatenate([mg[k, 0], mg[k, 1]], axis=1)

    def first_sum():
        for key, k, half in (("qm", 0, 1), ("qp", 1, 0), ("qm", 0, 0), ("qp", 1, 1)):
            net.recv(f"{key}{half}", rb.at[k, :, feats(half)])
        net.recv("mg", mg.at[:, o])

    def halo():
        for part in (slice(ROWS - 16, ROWS), slice(0, ROWS - 16)):
            block = own1[part] + rb[0, part].astype(F32) + rb[1, part].astype(F32)
            value = (xt[z, part].astype(F32) + 0.5 * block).astype(BF16)
            a1[part] = value
            hs[part] = normed(value, joined(0))
            if part.start:
                net.send("h", lambda: (hs.at[pl.ds(112, 16), :], hr, sibling))

    def mix():
        mix_scale = joined(1)
        for start in (64, 0):
            part = slice(start, start + 64)
            if start:
                longer = hs[48:ROWS].astype(F32)
            else:
                net.recv("h", hr)
                before = jnp.where(c == 1, hr[...].astype(F32), 0.0)
                longer = jnp.concatenate([before, hs[:64].astype(F32)], axis=0)
            positions = c * ROWS + start + lax.broadcasted_iota(jnp.int32, (64, 256), 0)
            for g in range(4):
                lanes = slice(256 * g, 256 * g + 256)
                total = longer[:, lanes]
                for k in range(g + 1):
                    total = total + pltpu.roll(total, 2**k, axis=0)
                counts = jnp.minimum(positions + 1, 2 ** (g + 1)).astype(F32)
                diff = (total[16:] / counts - longer[16:, lanes]).astype(BF16)
                mixed = dot(diff, maps[g])
                after = a1[part, lanes].astype(F32) + mixed * mix_scale[:, lanes]
                ob[part, lanes] = after.astype(BF16)
            half = pl.ds(start, 64)
            net.send(
                "a", lambda half=half: (ob.at[half], xq.at[half], dev(zq, y, x, c)), batch="a", total=lambda: ob
            )

    def second_norm():
        n[pl.ds(0, ROWS), :] = normed(ob[...], gain2)

    def second_own_1():
        turn(1, 0, wd2, 0)
        turn(1, 1, wd2, 0)
        gate_up(1, 0, ROWS, put2(0, ROWS, 0))

    def second_peer_1():
        net.recv("a", xq)
        n[pl.ds(ROWS, ROWS), :] = normed(xq[...], gain2)
        gate_up(1, ROWS, ROWS, put2(ROWS, ROWS, 0))
        part1[...] = dot(h2[pl.ds(ROWS, ROWS), :UNIT], wd2[:UNIT])

    def second_near():
        turn(2, c, wd2, UNIT)
        gate_up_half(2, ROWS, ROWS, c)

    def second_peer_2():
        gate_up_half(2, ROWS, ROWS, o, put2(ROWS, ROWS, UNIT))
        turn(2, o, wd2, UNIT)
        for k in range(2):
            lanes = slice(HALF * k, HALF * k + HALF)
            sq[:, lanes] = (part1[:, lanes] + dot(h2[pl.ds(ROWS, ROWS), UNIT:], wd2[UNIT:, lanes])).astype(BF16)
            net.send(
                "b",
                lambda k=k: (sq.at[:, feats(k)], rq.at[c], dev(zq, y, x, k)),
                width=2, shift=c, batch="b", total=lambda: sq,
            )

    def second_own_2():
        gate_up(2, 0, ROWS, put2(0, ROWS, UNIT))
        base[...] = ob[...].astype(F32) + 0.5 * dot(h2[pl.ds(0, ROWS), :], wd2[...])
        net.send("f", lambda: (base.at[:, feats(o)], rx, sibling))

    def last_sum():
        net.recv("f", rx)
        net.recv("b", rq.at[c], c, 2)
        out[rows(c), :] = (base[:, feats(c)] + 0.5 * rq[c].astype(F32)).astype(BF16)
        net.recv("b", rq.at[o], o, 2)
        out[rows(o), :] = (rx[...] + 0.5 * rq[o].astype(F32)).astype(BF16)

    staged(0)
    exchange(0)
    stage_t.wait()
    staged(1)
    exchange(1)
    spread_tokens(0, taker)
    start(0)
    start(1)
    exchange(2)
    net.send("ps", lambda: (pool, pw.at[c, o, y, x], sibling), cond=taker)
    net.send("pz", lambda: (pool, pw.at[c, j, y, x], dev(zp, y, x, j)), width=2, shift=c)
    own_mg.wait()
    own_sc.wait()
    net.send("mg", lambda: (mixg, mg.at[0, c], sibling), batch="mg", total=lambda: mg.at[:, 0])
    net.send("mg", lambda: (scale, mg.at[1, c], sibling), batch="mg", total=lambda: mg.at[:, 0])
    gain1 = g1[...]
    gain2 = g2[...]
    sa[0].two()
    sb[0].two()
    sa[0].pre()
    sb[0].pre()
    spread_tokens(1, keeper)
    sa[0].three()
    sb[0].three()
    relay_tokens()
    sa[0].mid()
    sb[0].mid()
    sa[0].four()
    sb[0].four()
    start_pool()
    start(2)
    norm_own()
    norm_next()
    norm_last()
    sa[0].five()
    sb[0].five()
    first_near()
    sa[1].two()
    sb[1].two()
    spool.second()
    handed(0)
    first_opposite()
    sa[2].two()
    sb[2].two()
    first_neighbours()
    sa[1].pre()
    sb[1].pre()
    first_own()
    sa[1].three()
    sb[1].three()
    sa[1].mid()
    sb[1].mid()
    first_pass_on()
    sa[2].three()
    sb[2].three()
    sa[2].pre()
    sb[2].pre()
    spool.third(pw.at[:, c])
    sa[1].four()
    sb[1].four()
    sa[2].mid()
    sb[2].mid()
    pool_maps()
    first_sum()
    halo()
    mix()
    sa[1].five()
    sb[1].five()
    sa[2].four()
    sb[2].four()
    second_norm()
    handed(1)
    second_own_1()
    sa[2].five()
    sb[2].five()
    second_peer_1()
    second_near()
    handed(2)
    second_peer_2()
    second_own_2()
    last_sum()
    net.finish()


def local(tok, g1, gate1, up1, down1, mixg, pool, scale, g2, gate2, up2, down2):
    hbm = pl.BlockSpec(memory_space=pl.ANY)
    vmem = pl.BlockSpec(memory_space=pltpu.VMEM)
    result = pl.pallas_call(
        kernel,
        out_shape=pltpu.VMEM((256, HALF), BF16),
        in_specs=[hbm, vmem, hbm, hbm, hbm, hbm, hbm, hbm, vmem, hbm, hbm, hbm],
        out_specs=vmem,
        scratch_shapes=[
            pltpu.VMEM((3, 3, 2, 4, 4, 32, UNIT), BF16),
            pltpu.VMEM((2, 2, 4, 4, 16, 256), BF16),
            pltpu.VMEM((4, ROWS, D), BF16),
            pltpu.VMEM((ROWS, D), BF16),
            pltpu.VMEM((4 * ROWS, D), BF16),
            pltpu.VMEM((4 * ROWS, UNIT), BF16),
            pltpu.VMEM((2 * ROWS, 2 * UNIT), BF16),
            pltpu.VMEM((UNIT, D), BF16),
            pltpu.VMEM((2 * UNIT, D), BF16),
            pltpu.VMEM((4, 256, 256), BF16),
            pltpu.VMEM((ROWS, D), F32),
            pltpu.VMEM((ROWS, HALF), F32),
            pltpu.VMEM((ROWS, HALF), F32),
            pltpu.VMEM((ROWS, D), BF16),
            pltpu.VMEM((ROWS, D), BF16),
            pltpu.VMEM((ROWS, D), BF16),
            pltpu.VMEM((2, ROWS, HALF), BF16),
            pltpu.VMEM((2, ROWS, D), BF16),
            pltpu.VMEM((ROWS, D), BF16),
            pltpu.VMEM((ROWS, D), BF16),
            pltpu.VMEM((16, D), BF16),
            pltpu.VMEM((2, 2, 1, HALF), F32),
            pltpu.VMEM((ROWS, D), BF16),
            pltpu.VMEM((ROWS, D), BF16),
            pltpu.VMEM((2, ROWS, HALF), BF16),
            pltpu.VMEM((ROWS, D), F32),
            pltpu.VMEM((ROWS, HALF), F32),
            pltpu.VMEM((2, 3, 32, 1280), BF16),
            pltpu.VMEM((256, HALF), BF16),
            pltpu.VMEM((ROWS, 2 * UNIT), F32),
            pltpu.VMEM((ROWS, D), F32),
            pltpu.SemaphoreType.DMA((N_SEND,)),
            pltpu.SemaphoreType.DMA((N_RECV,)),
            pltpu.SemaphoreType.DMA((N_LOCAL,)),
        ],
        compiler_params=pltpu.CompilerParams(collective_id=0, has_side_effects=True, vmem_limit_bytes=52 * 2**20),
    )(
        *(
            pltpu.with_memory_space_constraint(value, pltpu.HBM)
            for value in (
                tok.reshape(256, HALF), g1.reshape(1, D), gate1, up1, down1.T, mixg.reshape(1, HALF),
                pool.transpose(0, 2, 1).reshape(16, 256), scale.reshape(1, HALF), g2.reshape(1, D), gate2, up2, down2.T,
            )
        )
    )
    return result.reshape(1, 256, HALF)


def solution(mesh):
    placed = (
        P(("rep", "fs"), None, "tp"),
        P(),
        P("fs", "tp"),
        P("fs", "tp"),
        P("tp", "fs"),
        P("tp"),
        P("tp", None, "fs"),
        P("tp"),
        P(),
        P("fs", "tp"),
        P("fs", "tp"),
        P("tp", "fs"),
    )
    return jax.shard_map(
        local, mesh=mesh, in_specs=placed, out_specs=P(("rep", "fs"), None, "tp"), check_vma=False
    )
```

```python
import jax
import jax.numpy as jnp
from jax import lax
from jax.experimental import pallas as pl
from jax.experimental.pallas import tpu as pltpu
from jax.sharding import PartitionSpec as P

MESH = pl.DeviceIdType.MESH
BF16 = jnp.bfloat16
F32 = jnp.float32
EPS = 1e-06
D = 1024
HALF = 512
ROWS = 128
UNIT = 640
DIRECT = False
N_SEND = 23
N_RECV = 81
N_LOCAL = 10


class Net:
    def __init__(self, ss, rs, ls, here):
        self.ss, self.rs, self.ls, self.here = ss, rs, ls, here
        self.names = {}
        self.batches = {}
        self.locals = 0
        self.sends = 0
        self.pending = []

    def name(self, key, width=1):
        if key not in self.names:
            self.names[key] = sum(w for _, w in self.names.values()), width
        return self.names[key][0]

    def send(self, key, make, cond=None, width=1, shift=None, batch=None, total=None):
        base = self.name(key, width)
        first = batch is None or batch not in self.batches
        if first:
            slot = self.sends
            self.sends += 1
            if batch is not None:
                self.batches[batch] = slot
        else:
            slot = self.batches[batch]

        def copy(src, dst, device):
            where = base if shift is None else base + shift
            return pltpu.make_async_remote_copy(
                src, dst, self.ss.at[slot], self.rs.at[where], device_id=device, device_id_type=MESH
            )

        def end():
            ref = make()[0] if total is None else total()
            copy(ref, ref, self.here).wait_send()

        if cond is None:
            copy(*make()).start()
        else:
            pl.when(cond)(lambda: copy(*make()).start())
        if first:
            self.pending.append(end if cond is None else lambda: pl.when(cond)(end))

    def recv(self, key, ref, offset=0, width=1):
        where = self.name(key, width) + offset
        pltpu.make_async_remote_copy(
            ref, ref, self.ss.at[0], self.rs.at[where], device_id=self.here, device_id_type=MESH
        ).wait_recv()

    def slot(self):
        self.locals += 1
        return self.ls.at[self.locals - 1]

    def local(self, src, dst):
        return pltpu.make_async_copy(src, dst, self.slot())

    def finish(self):
        for end in self.pending:
            end()
        assert self.sends == N_SEND and self.locals == N_LOCAL
        assert sum(w for _, w in self.names.values()) == N_RECV


class Stream:
    def __init__(self, net, unit, tag, direct, piece, group, size, size_all, first, second, sibling):
        self.net, self.unit, self.tag, self.direct = net, unit, (unit, tag), direct
        self.piece, self.group, self.size, self.size_all = piece, group, size, size_all
        self.a, self.ap, self.am, self.ao, self.to_ap, self.to_am, self.to_ao = first
        self.b, self.bp, self.bm, self.bo, self.to_bp, self.to_bm, self.to_bo = second
        self.sibling = sibling
        self.flip = unit == 2

    def send(self, what, a, b, device, kind, count):
        self.net.send(
            (self.tag, what),
            lambda: (self.piece(a, b), self.piece(a, b), device),
            batch=kind,
            total=lambda: self.size_all(count),
        )

    def recv(self, what, a, b):
        self.net.recv((self.tag, what), self.piece(a, b))

    def both(self, k, a):
        late_m, late_p = ("2x" if k >= 2 else f"2m{k}"), ("2x" if k < 2 else f"2p{k}")
        self.send(late_m, a, self.b, self.to_bp, "both", 8)
        self.send(late_p, a, self.b, self.to_bm, "both", 8)

    def hand(self, b):
        self.net.send(
            (self.unit, "d"),
            lambda: (self.group(b), self.group(b), self.sibling),
            batch="hand",
            total=lambda: self.size_all(16),
        )

    def one(self):
        self.send("1m", self.a, self.b, self.to_ap, "ring", 2)
        self.send("1p", self.a, self.b, self.to_am, "ring", 2)
        if self.direct:
            self.send("1o", self.a, self.b, self.to_ao, "far", 1)

    def then(self):
        self.both(0, self.a)

    def two(self):
        for key, k, a, to in (("1p", 2, self.ap, self.to_am), ("1m", 1, self.am, self.to_ap))[:: -1 if self.flip else 1]:
            self.recv(key, a, self.b)
            if key == ("1m" if self.flip else "1p") and not self.direct:
                self.send("1o", a, self.b, to, "far", 1)
            self.both(k, a)

    def three(self):
        self.recv("1o", self.ao, self.b)
        self.both(3, self.ao)
        self.hand(self.b)

    def pre(self):
        self.recv("2m0", self.a, self.bm)
        self.send("2o", self.a, self.bm, self.to_bp, "on", 4)

    def mid(self):
        self.recv("2m1", self.am, self.bm)
        self.send("2o", self.am, self.bm, self.to_bp, "on", 4)
        self.recv("2p2", self.ap, self.bp)
        self.send("2o", self.ap, self.bp, self.to_bm, "on", 4)

    def four(self):
        self.recv("2p3", self.ao, self.bp)
        self.send("2o", self.ao, self.bp, self.to_bm, "on", 4)
        self.net.recv((self.tag, "2x"), self.size(4))
        self.hand(self.bp)
        self.hand(self.bm)

    def five(self):
        self.net.recv((self.tag, "2o"), self.size(4))
        self.hand(self.bo)


class Coarse:
    def __init__(self, net, piece, some, first, second, sibling):
        self.net, self.piece, self.some, self.first_axis, self.second_axis = net, piece, some, first, second
        self.sibling = sibling

    def send(self, key, a, device, total):
        self.net.send(
            key, lambda: (self.piece(a, self.second_axis[0]), self.piece(a, self.second_axis[0]), device),
            batch=key, total=lambda: total,
        )

    def first(self):
        for device in self.first_axis[4:]:
            self.send("p1", self.first_axis[0], device, self.some(1, 3))

    def second(self):
        self.net.recv("p1", self.some(1, 3))
        for device in self.second_axis[4:]:
            for a in self.first_axis[:4]:
                self.send("p2", a, device, self.some(3, 4))

    def third(self, mine):
        self.net.recv("p2", self.some(3, 4))
        self.net.send("p3", lambda: (mine, mine, self.sibling))

    def last(self, theirs):
        self.net.recv("p3", theirs)


def normed(values, gain):
    floats = values.astype(F32)
    mean = jnp.mean(floats * floats, axis=-1, keepdims=True)
    return (floats * lax.rsqrt(mean + EPS) * gain).astype(BF16)


def kernel(
    tok, g1, gate1, up1, down1, mixg, pool, scale, g2, gate2, up2, down2, out,
    w, pw, xt, xq, n, h1, h2, wd1, wd2, maps, own1, pm, pp, so, sm, sp, ra, rb, a1, hs, hr, mg, ob, sq, rq, base, rx, st, tokv, gu, part1,
    ss, rs, ls,
):
    rep = lax.axis_index("rep")
    fs = lax.axis_index("fs")
    c = lax.axis_index("tp")
    o = 1 - c
    j = lax.div(fs, 16)
    z = rep * 2 + j
    y = lax.rem(lax.div(fs, 4), 4)
    x = lax.rem(fs, 4)
    zp, zo, zm = (lax.rem(z + k, 4) for k in (1, 2, 3))
    yp, yo, ym = (lax.rem(y + k, 4) for k in (1, 2, 3))
    xp, xo, xm = (lax.rem(x + k, 4) for k in (1, 2, 3))

    def dev(z_, y_, x_, c_):
        return (lax.div(z_, 2), lax.rem(z_, 2) * 16 + y_ * 4 + x_, c_)

    sibling = dev(z, y, x, o)
    net = Net(ss, rs, ls, sibling)
    keeper = c == j
    taker = c != j
    zq = lax.rem(z + 1 + 2 * lax.rem(z + c, 2), 4)

    def cols(k):
        return pl.ds(pl.multiple_of(k * UNIT, 128), UNIT)

    def feats(k):
        return pl.ds(pl.multiple_of(k * HALF, 128), HALF)

    def rows(k):
        return pl.ds(pl.multiple_of(k * ROWS, 128), ROWS)

    mats = ((gate1, up1, down1), (gate2, up2, down2), (gate2, up2, down2))
    subs = (lax.div(z, 2), 0, 1)

    own_tok = net.local(tok.at[rows(c), :], xt.at[z, :, feats(c)])
    own_tok.start()
    own_w = [net.slot() for u in range(3)]
    own_p = net.slot()

    def own_pool():
        return pltpu.make_async_copy(pool, pw.at[c, c, y, x], own_p)

    stage_t = net.local(tok, tokv)
    stage_t.start()
    stage_w = [net.slot(), net.slot()]

    @pl.when(taker)
    def _():
        for k in range(2):
            for m in range(3):
                pltpu.make_async_copy(mats[k][m], st.at[k, m], stage_w[k]).start()

    @pl.when(keeper)
    def _():
        for u in range(3):
            for m in range(3):
                pltpu.make_async_copy(mats[u][m].at[:, cols(subs[u])], w.at[u, m, c, y, x], own_w[u]).start()
        own_pool().start()

    own_mg = net.local(mixg, mg.at[0, c])
    own_sc = net.local(scale, mg.at[1, c])
    own_mg.start()
    own_sc.start()

    barrier = pltpu.get_barrier_semaphore()
    friends = [dev(z, y, x_, c) for x_ in (xp, xm, xo)] + [dev(z, y_, x, c) for y_ in (yp, ym, yo)] + [sibling]
    friends += [dev(z_, y, x, k) for z_ in (zp, zm) for k in range(2)]
    for friend in friends:
        pl.semaphore_signal(barrier, inc=1, device_id=friend, device_id_type=MESH)
    pl.semaphore_wait(barrier, len(friends))

    def staged(k):
        @pl.when(taker)
        def _():
            pltpu.make_async_copy(st.at[k], st.at[k], stage_w[k]).wait()

    def exchange(u):
        for ab, z_ in ((0, zp), (1, zm)):
            sub = (lax.div(z_, 2), 0, 1)[u]
            part = pl.ds(16 * ab, 16)
            for m in range(3):
                net.send(
                    ("z", u),
                    lambda m=m, part=part, sub=sub, z_=z_: (
                        st.at[min(u, 1), m, part, cols(sub)],
                        w.at[u, m, o, y, x, part, :],
                        dev(z_, y, x, o),
                    ),
                    cond=taker,
                    batch="z",
                    total=lambda: w.at[:, :, 0, 0, 0],
                )

    def own(u):
        ref = w.at[u, :, c, y, x]

        @pl.when(keeper)
        def _():
            pltpu.make_async_copy(ref, ref, own_w[u]).wait()

        @pl.when(taker)
        def _():
            net.recv(("z", u), ref)

    in_x = (x, xp, xm, xo, dev(z, y, xp, c), dev(z, y, xm, c), dev(z, y, xo, c))
    in_y = (y, yp, ym, yo, dev(z, yp, x, c), dev(z, ym, x, c), dev(z, yo, x, c))
    two, top, low = pl.ds(0, 2), pl.ds(0, 16), pl.ds(16, 16)

    def size_w(k):
        return {2: w.at[0, :, 0, two, 0, top], 4: w.at[0, :, 0, :, 0, top]}[k]

    def size_all(k):
        return {
            1: w.at[:, :, 0, two, 0, top],
            2: w.at[:, :, 0, :, 0, top],
            4: w.at[:, :, 0, two, :, top],
            8: w.at[:, :, 0, :, :, top],
            16: w.at[:, :, 0],
        }[k]

    def stream_a(u):
        return Stream(
            net, u, "a", DIRECT and u == 0,
            lambda a, b: w.at[u, :, c, b, a, top, :],
            lambda b: w.at[u, :, c, b, :, top, :],
            size_w, size_all, in_x, in_y, sibling,
        )

    def stream_b(u):
        return Stream(
            net, u, "b", DIRECT and u == 0,
            lambda a, b: w.at[u, :, c, a, b, low, :],
            lambda b: w.at[u, :, c, :, b, low, :],
            size_w, size_all, in_y, in_x, sibling,
        )

    sa = [stream_a(u) for u in range(3)]
    sb = [stream_b(u) for u in range(3)]
    def pick(k, l):
        return k * o + l * c

    xs, ys = (x, xp, xm, xo), (y, yp, ym, yo)
    first = [pick(k, l) for k, l in zip(xs, ys)]
    second = [pick(l, k) for k, l in zip(xs, ys)]
    first += [dev(z, pick(y, l), pick(k, x), c) for k, l in zip(xs[1:], ys[1:])]
    second += [dev(z, pick(l, y), pick(x, k), c) for k, l in zip(xs[1:], ys[1:])]
    spool = Coarse(
        net, lambda a, b: pw.at[:, c, pick(b, a), pick(a, b)], lambda k, l: pw.at[:, 0, pl.ds(0, k), pl.ds(0, l)],
        first, second, sibling,
    )

    def start(u):
        own(u)
        sa[u].one()
        sb[u].one()
        sa[u].then()
        sb[u].then()

    def handed(u):
        net.recv((u, "d"), w.at[u, :, o])

    def spread_tokens(tag, cond):
        for k in range(2):
            for key, z_ in (("tm", zp), ("tp", zm)):
                net.send(
                    key,
                    lambda k=k, z_=z_: (tokv.at[rows(k), :], xt.at[z, :, feats(c)], dev(z_, y, x, k)),
                    cond=cond, width=2, shift=c, batch=("t4", tag), total=lambda: xt.at[pl.ds(0, 2)],
                )
        net.send("ts", lambda: (tokv.at[rows(o), :], xt.at[z, :, feats(c)], sibling), cond=cond)

    def relay_tokens():
        for key, who, half, to in (("tm", zm, 0, zp), ("tp", zp, 1, zm)):
            net.recv(key, xt.at[who, :, feats(half)], half, 2)
            net.send(
                "to",
                lambda who=who, half=half, to=to: (
                    xt.at[who, :, feats(half)], xt.at[who, :, feats(half)], dev(to, y, x, c)
                ),
                batch="t2", total=lambda: xt.at[0],
            )
        net.recv("tm", xt.at[zm, :, feats(1)], 1, 2)
        net.recv("tp", xt.at[zp, :, feats(0)], 0, 2)

    def dot(lhs, rhs):
        return jnp.dot(lhs, rhs, preferred_element_type=F32)

    def gate_up(u, at, count, put):
        for k in range(UNIT // 128):
            part = pl.ds(k * 128, 128)
            wg = w[u, 0, :, :, :, :, part].reshape(D, 128)
            wu = w[u, 1, :, :, :, :, part].reshape(D, 128)
            both = jnp.dot(
                n[pl.ds(at, count), :], jnp.concatenate([wg, wu], axis=1), preferred_element_type=F32
            )
            gate, up = both[:, :128], both[:, 128:]
            put(k * 128, (gate * jax.nn.sigmoid(gate) * up).astype(BF16))

    def put1(at, count):
        def put(k, value):
            h1[pl.ds(at, count), pl.ds(k, 128)] = value

        return put

    def put2(at, count, first):
        def put(k, value):
            h2[pl.ds(at, count), pl.ds(first + k, 128)] = value

        return put

    def gate_up_half(u, at, count, part, put=None):
        lanes = feats(part)
        for k in range(UNIT // 128):
            hid = pl.ds(k * 128, 128)
            wg = w[u, 0, part, :, :, :, hid].reshape(HALF, 128)
            wu = w[u, 1, part, :, :, :, hid].reshape(HALF, 128)
            both = dot(n[pl.ds(at, count), lanes], jnp.concatenate([wg, wu], axis=1))
            if put is None:
                gu[:, pl.ds(k * 256, 256)] = both
            else:
                both = both + gu[:, pl.ds(k * 256, 256)]
                gate, up = both[:, :128], both[:, 128:]
                put(k * 128, (gate * jax.nn.sigmoid(gate) * up).astype(BF16))

    def turn(u, part, wide, at):
        for k in range(2):
            block = w[u, 2, part, 2 * k : 2 * k + 2].reshape(256, UNIT)
            wide[pl.ds(at, UNIT), pl.ds(pl.multiple_of(part * HALF + 256 * k, 128), 256)] = block.T

    def start_pool():
        @pl.when(keeper)
        def _():
            own_pool().wait()
            net.recv("ps", pw.at[o, c, y, x])

        @pl.when(taker)
        def _():
            net.recv("pz", pw.at[0, c, y, x], 0, 2)
            net.recv("pz", pw.at[1, c, y, x], 1, 2)

        spool.first()

    def norm_own():
        own_tok.wait()
        net.recv("ts", xt.at[z, :, feats(o)])
        n[pl.ds(0, ROWS), :] = normed(xt[z], gain1)

    def norm_next():
        n[pl.ds(ROWS, ROWS), :] = normed(xt[zm], gain1)
        n[pl.ds(2 * ROWS, ROWS), :] = normed(xt[zp], gain1)

    def norm_last():
        net.recv("to", xt.at[zo])
        n[pl.ds(3 * ROWS, ROWS), :] = normed(xt[zo], gain1)

    def first_near():
        turn(0, c, wd1, 0)
        gate_up_half(0, 3 * ROWS, ROWS, c)

    def first_opposite():
        gate_up_half(0, 3 * ROWS, ROWS, o, put1(3 * ROWS, ROWS))
        turn(0, o, wd1, 0)
        for k, z_ in ((0, zp), (1, zm)):
            lanes = slice(HALF * k, HALF * k + HALF)
            so[:, lanes] = dot(h1[pl.ds(3 * ROWS, ROWS), :], wd1[:, lanes]).astype(BF16)
            net.send(
                f"r{k}", lambda k=k, z_=z_: (so.at[:, feats(k)], ra.at[k], dev(z_, y, x, c)), batch="r", total=lambda: so
            )

    def pass_on(buf, k, half, z_):
        net.send(
            "q",
            lambda: (buf.at[:, feats(half)], rb.at[k, :, feats(half)], dev(z_, y, x, c)),
            batch="q", total=lambda: xt.at[two],
        )

    def first_neighbours():
        gate_up(0, ROWS, 2 * ROWS, put1(ROWS, 2 * ROWS))
        sums = dot(h1[pl.ds(ROWS, 2 * ROWS), :], wd1[...])
        sm[:, :HALF] = sums[:ROWS, :HALF].astype(BF16)
        sp[:, HALF:] = sums[ROWS:, HALF:].astype(BF16)
        pm[...] = sums[:ROWS, HALF:]
        pp[...] = sums[ROWS:, :HALF]
        pass_on(sp, 0, 1, zp)
        pass_on(sm, 1, 0, zm)

    def first_own():
        gate_up(0, 0, ROWS, put1(0, ROWS))
        own1[...] = dot(h1[pl.ds(0, ROWS), :], wd1[...])

    def first_pass_on():
        net.recv("r0", ra.at[0])
        sp[:, :HALF] = (pp[...] + ra[0].astype(F32)).astype(BF16)
        pass_on(sp, 0, 0, zp)
        net.recv("r1", ra.at[1])
        sm[:, HALF:] = (pm[...] + ra[1].astype(F32)).astype(BF16)
        pass_on(sm, 1, 1, zm)

    def pool_maps():
        spool.last(pw.at[:, o])
        for g in range(4):
            wide = pw[g // 2].reshape(32, 16, 256).astype(F32)
            maps[g] = wide[:, 8 * (g % 2) : 8 * (g % 2) + 8, :].reshape(256, 256).astype(BF16).T

    def joined(k):
        return jnp.concatenate([mg[k, 0], mg[k, 1]], axis=1)

    def first_sum():
        net.recv("q", rb)
        net.recv("mg", mg.at[:, o])

    def halo():
        for part in (slice(ROWS - 16, ROWS), slice(0, ROWS - 16)):
            block = own1[part] + rb[0, part].astype(F32) + rb[1, part].astype(F32)
            value = (xt[z, part].astype(F32) + 0.5 * block).astype(BF16)
            a1[part] = value
            hs[part] = normed(value, joined(0))
            if part.start:
                net.send("h", lambda: (hs.at[pl.ds(112, 16), :], hr, sibling))

    def mix():
        mix_scale = joined(1)
        for start in (64, 0):
            part = slice(start, start + 64)
            if start:
                longer = hs[48:ROWS].astype(F32)
            else:
                net.recv("h", hr)
                before = jnp.where(c == 1, hr[...].astype(F32), 0.0)
                longer = jnp.concatenate([before, hs[:64].astype(F32)], axis=0)
            positions = c * ROWS + start + lax.broadcasted_iota(jnp.int32, (64, 256), 0)
            for g in range(4):
                lanes = slice(256 * g, 256 * g + 256)
                total = longer[:, lanes]
                for k in range(g + 1):
                    total = total + pltpu.roll(total, 2**k, axis=0)
                counts = jnp.minimum(positions + 1, 2 ** (g + 1)).astype(F32)
                diff = (total[16:] / counts - longer[16:, lanes]).astype(BF16)
                mixed = dot(diff, maps[g])
                after = a1[part, lanes].astype(F32) + mixed * mix_scale[:, lanes]
                ob[part, lanes] = after.astype(BF16)
            half = pl.ds(start, 64)
            net.send(
                "a", lambda half=half: (ob.at[half], xq.at[half], dev(zq, y, x, c)), batch="a", total=lambda: ob
            )

    def second_norm():
        n[pl.ds(0, ROWS), :] = normed(ob[...], gain2)

    def second_own_1():
        turn(1, 0, wd2, 0)
        turn(1, 1, wd2, 0)
        gate_up(1, 0, ROWS, put2(0, ROWS, 0))

    def second_peer_1():
        net.recv("a", xq)
        n[pl.ds(ROWS, ROWS), :] = normed(xq[...], gain2)
        gate_up(1, ROWS, ROWS, put2(ROWS, ROWS, 0))
        part1[...] = dot(h2[pl.ds(ROWS, ROWS), :UNIT], wd2[:UNIT])

    def second_near():
        turn(2, c, wd2, UNIT)
        gate_up_half(2, ROWS, ROWS, c)

    def second_peer_2():
        gate_up_half(2, ROWS, ROWS, o, put2(ROWS, ROWS, UNIT))
        turn(2, o, wd2, UNIT)
        for k in range(2):
            lanes = slice(HALF * k, HALF * k + HALF)
            sq[:, lanes] = (part1[:, lanes] + dot(h2[pl.ds(ROWS, ROWS), UNIT:], wd2[UNIT:, lanes])).astype(BF16)
            net.send(
                "b",
                lambda k=k: (sq.at[:, feats(k)], rq.at[c], dev(zq, y, x, k)),
                width=2, shift=c, batch="b", total=lambda: sq,
            )

    def second_own_2():
        gate_up(2, 0, ROWS, put2(0, ROWS, UNIT))
        base[...] = ob[...].astype(F32) + 0.5 * dot(h2[pl.ds(0, ROWS), :], wd2[...])
        net.send("f", lambda: (base.at[:, feats(o)], rx, sibling))

    def last_sum():
        net.recv("f", rx)
        net.recv("b", rq.at[c], c, 2)
        out[rows(c), :] = (base[:, feats(c)] + 0.5 * rq[c].astype(F32)).astype(BF16)
        net.recv("b", rq.at[o], o, 2)
        out[rows(o), :] = (rx[...] + 0.5 * rq[o].astype(F32)).astype(BF16)

    staged(0)
    exchange(0)
    stage_t.wait()
    staged(1)
    exchange(1)
    spread_tokens(0, taker)
    start(0)
    start(1)
    exchange(2)
    net.send("ps", lambda: (pool, pw.at[c, o, y, x], sibling), cond=taker)
    net.send("pz", lambda: (pool, pw.at[c, j, y, x], dev(zp, y, x, j)), width=2, shift=c)
    own_mg.wait()
    own_sc.wait()
    net.send("mg", lambda: (mixg, mg.at[0, c], sibling), batch="mg", total=lambda: mg.at[:, 0])
    net.send("mg", lambda: (scale, mg.at[1, c], sibling), batch="mg", total=lambda: mg.at[:, 0])
    gain1 = g1[...]
    gain2 = g2[...]
    sa[0].two()
    sb[0].two()
    sa[0].pre()
    sb[0].pre()
    spread_tokens(1, keeper)
    sa[0].three()
    sb[0].three()
    relay_tokens()
    sa[0].mid()
    sb[0].mid()
    sa[0].four()
    sb[0].four()
    start_pool()
    start(2)
    norm_own()
    norm_next()
    norm_last()
    sa[0].five()
    sb[0].five()
    first_near()
    sa[1].two()
    sb[1].two()
    spool.second()
    handed(0)
    first_opposite()
    sa[2].two()
    sb[2].two()
    first_neighbours()
    sa[1].pre()
    sb[1].pre()
    first_own()
    sa[1].three()
    sb[1].three()
    sa[1].mid()
    sb[1].mid()
    first_pass_on()
    sa[2].three()
    sb[2].three()
    sa[2].pre()
    sb[2].pre()
    spool.third(pw.at[:, c])
    sa[1].four()
    sb[1].four()
    sa[2].mid()
    sb[2].mid()
    pool_maps()
    first_sum()
    halo()
    mix()
    sa[1].five()
    sb[1].five()
    sa[2].four()
    sb[2].four()
    second_norm()
    handed(1)
    second_own_1()
    sa[2].five()
    sb[2].five()
    second_peer_1()
    second_near()
    handed(2)
    second_peer_2()
    second_own_2()
    last_sum()
    net.finish()


def local(tok, g1, gate1, up1, down1, mixg, pool, scale, g2, gate2, up2, down2):
    hbm = pl.BlockSpec(memory_space=pl.ANY)
    vmem = pl.BlockSpec(memory_space=pltpu.VMEM)
    result = pl.pallas_call(
        kernel,
        out_shape=pltpu.VMEM((256, HALF), BF16),
        in_specs=[hbm, vmem, hbm, hbm, hbm, hbm, hbm, hbm, vmem, hbm, hbm, hbm],
        out_specs=vmem,
        scratch_shapes=[
            pltpu.VMEM((3, 3, 2, 4, 4, 32, UNIT), BF16),
            pltpu.VMEM((2, 2, 4, 4, 16, 256), BF16),
            pltpu.VMEM((4, ROWS, D), BF16),
            pltpu.VMEM((ROWS, D), BF16),
            pltpu.VMEM((4 * ROWS, D), BF16),
            pltpu.VMEM((4 * ROWS, UNIT), BF16),
            pltpu.VMEM((2 * ROWS, 2 * UNIT), BF16),
            pltpu.VMEM((UNIT, D), BF16),
            pltpu.VMEM((2 * UNIT, D), BF16),
            pltpu.VMEM((4, 256, 256), BF16),
            pltpu.VMEM((ROWS, D), F32),
            pltpu.VMEM((ROWS, HALF), F32),
            pltpu.VMEM((ROWS, HALF), F32),
            pltpu.VMEM((ROWS, D), BF16),
            pltpu.VMEM((ROWS, D), BF16),
            pltpu.VMEM((ROWS, D), BF16),
            pltpu.VMEM((2, ROWS, HALF), BF16),
            pltpu.VMEM((2, ROWS, D), BF16),
            pltpu.VMEM((ROWS, D), BF16),
            pltpu.VMEM((ROWS, D), BF16),
            pltpu.VMEM((16, D), BF16),
            pltpu.VMEM((2, 2, 1, HALF), F32),
            pltpu.VMEM((ROWS, D), BF16),
            pltpu.VMEM((ROWS, D), BF16),
            pltpu.VMEM((2, ROWS, HALF), BF16),
            pltpu.VMEM((ROWS, D), F32),
            pltpu.VMEM((ROWS, HALF), F32),
            pltpu.VMEM((2, 3, 32, 1280), BF16),
            pltpu.VMEM((256, HALF), BF16),
            pltpu.VMEM((ROWS, 2 * UNIT), F32),
            pltpu.VMEM((ROWS, D), F32),
            pltpu.SemaphoreType.DMA((N_SEND,)),
            pltpu.SemaphoreType.DMA((N_RECV,)),
            pltpu.SemaphoreType.DMA((N_LOCAL,)),
        ],
        compiler_params=pltpu.CompilerParams(collective_id=0, has_side_effects=True, vmem_limit_bytes=52 * 2**20),
    )(
        *(
            pltpu.with_memory_space_constraint(value, pltpu.HBM)
            for value in (
                tok.reshape(256, HALF), g1.reshape(1, D), gate1, up1, down1.T, mixg.reshape(1, HALF),
                pool.transpose(0, 2, 1).reshape(16, 256), scale.reshape(1, HALF), g2.reshape(1, D), gate2, up2, down2.T,
            )
        )
    )
    return result.reshape(1, 256, HALF)


def solution(mesh):
    placed = (
        P(("rep", "fs"), None, "tp"),
        P(),
        P("fs", "tp"),
        P("fs", "tp"),
        P("tp", "fs"),
        P("tp"),
        P("tp", None, "fs"),
        P("tp"),
        P(),
        P("fs", "tp"),
        P("fs", "tp"),
        P("tp", "fs"),
    )
    return jax.shard_map(
        local, mesh=mesh, in_specs=placed, out_specs=P(("rep", "fs"), None, "tp"), check_vma=False
    )
```
